128 devices in a mesh: rep: 2 (over z_hi), fs: 32 (over z_lo, y, x), tp: 2 (over core).
Axes of the slice: x: 4, y: 4, z: 4 (z_hi: 2, z_lo: 2; z = z_hi * 2 + z_lo), core: 2. Of those that a mesh axis runs over, the one named last changes fastest.
Arguments:
- tokens: bfloat16 [64, 1024, 2048], P(('rep', 'fs'), 'tp'), may hold values from -6 to 6
- mix_gain: float32 [2048], replicated, may hold values from 0.1 to 1.9
- out_gate_w: float32 [2048, 1024], P('fs', 'tp'), may hold values from -0.125 to 0.125
- in_gate_w: float32 [2048, 1024], P('fs', 'tp'), may hold values from -0.125 to 0.125
- value_w: float32 [2048, 1024], P('fs', 'tp'), may hold values from -0.125 to 0.125
- out_gate_scale: float32 [1024], P(('tp', 'fs')), may hold values from 0.28 to 3.5
- in_gate_scale: float32 [1024], P(('tp', 'fs')), may hold values from 0.5 to 2
- value_scale: float32 [1024], P(('tp', 'fs')), may hold values from 0.5 to 2
- mix_taps: float32 [3, 1024], P(None, 'tp'), may hold values from -3.5 to 3.5
- conv_gain: float32 [1024], P('tp'), may hold values from 0.1 to 1.9
- out_proj_w: float32 [1024, 2048], P('tp', 'fs'), may hold values from -0.1875 to 0.1875
- proj_scale: float32 [2048], P('fs'), may hold values from 0.5 to 2
- ffn_gain: float32 [2048], replicated, may hold values from 0.1 to 1.9
- gate_w: float32 [2048, 2816], P('fs', 'tp'), may hold values from -0.125 to 0.125
- up_w: float32 [2048, 2816], P('fs', 'tp'), may hold values from -0.125 to 0.125
- gate_scale: float32 [2816], P(('tp', 'fs')), may hold values from 0.5 to 2
- up_scale: float32 [2816], P(('tp', 'fs')), may hold values from 0.5 to 2
- gate_taps: float32 [3, 2816], P(None, 'tp'), may hold values from -3.5 to 3.5
- up_taps: float32 [3, 2816], P(None, 'tp'), may hold values from -3.5 to 3.5
- gate_bias: float32 [2816], P('tp'), may hold values from -3 to 3
- up_bias: float32 [2816], P('tp'), may hold values from -3 to 3
- down_w: float32 [2816, 2048], P('tp', 'fs'), may hold values from -0.109375 to 0.109375
- down_scale: float32 [2048], P('fs'), may hold values from 0.5 to 2
Outputs:
- layer_out: bfloat16 [64, 1024, 2048], P(('rep', 'fs'), 'tp')
The draws below stay inside these ranges and needn't reach their ends.
All inputs are finite; a program needn't handle non-finite values.
Results may differ from the reference program's by a relative error of at most 0.02.
Values may be sent and summed in bfloat16 or wider, within the bound.
A program may use at most 128 MiB of HBM per device.

```python
import math
import jax
import jax.numpy as jnp
from jax import lax

D = 2048
CONV = 1024
FF = 2816
KW = 3
SEQ = 1024
SEQS = 64


def draw_out_gate_scale(key, part):
    ramp = jnp.exp(jnp.linspace(math.log(0.4), math.log(2.5), CONV)).astype(jnp.float32)
    noise = jax.random.uniform(key, (CONV,), jnp.float32, 0.7, 1.4)
    return ramp * noise


def block_scale(rng, dims, pieces, low, top_value):
    loudness, own = 1.0, jax.random.fold_in(rng, 6)
    for dim, blocks in pieces:
        steps = jnp.exp(jax.random.uniform(jax.random.fold_in(own, dim), (blocks,), jnp.float32, low / len(pieces), top_value / len(pieces)))
        loudness = loudness * jnp.repeat(steps, dims[dim] // blocks).reshape([-1 if axis == dim else 1 for axis in range(len(dims))])
    return loudness


def bell_draw(key, extent, width, limit, cuts=(), held_as=jnp.bfloat16):
    result = jax.random.normal(key, extent, jnp.float32) * width
    if len(cuts) > 0:
        result = block_scale(key, extent, cuts, -0.22, 0.18) * result
    return jnp.clip(result, min=-limit, max=limit).astype(held_as)


def setup_inputs(seed: int = 0) -> dict:
    streams_of = jax.random.split(jax.random.key(seed), 24)
    tokens = bell_draw(streams_of[0], (SEQS, SEQ, D), 1.0, 6.0, ((0, 64), (1, 2)))
    mix_gain = jnp.clip(1.0 + 0.18 * jax.random.normal(streams_of[1], (D,), jnp.float32), 0.1, 1.9)
    out_gate_w = bell_draw(streams_of[2], (D, CONV), D ** -0.5, 0.125, ((0, 32), (1, 2)), jnp.float32)
    in_gate_w = bell_draw(streams_of[3], (D, CONV), D ** -0.5, 0.125, ((0, 32), (1, 2)), jnp.float32)
    value_w = bell_draw(streams_of[4], (D, CONV), D ** -0.5, 0.125, ((0, 32), (1, 2)), jnp.float32)
    out_gate_scale = draw_out_gate_scale(jax.random.fold_in(streams_of[23], 71), 0)
    in_gate_scale = jnp.clip(jnp.exp(math.log(2.0) - 1.3862944 * jax.random.uniform(streams_of[6], (CONV,), jnp.float32) ** block_scale(streams_of[6], (CONV,), ((0, 64),), -0.2, 0.2)), 0.5, 2.0)
    value_scale = jnp.clip(jnp.exp(math.log(2.0) - 1.3862944 * jax.random.uniform(streams_of[7], (CONV,), jnp.float32) ** block_scale(streams_of[7], (CONV,), ((0, 64),), -0.2, 0.2)), 0.5, 2.0)
    mix_taps = bell_draw(streams_of[8], (KW, CONV), KW ** -0.5, 3.5, ((1, 2),), jnp.float32)
    conv_gain = jnp.clip(1.0 + 0.18 * jax.random.normal(streams_of[9], (CONV,), jnp.float32), 0.1, 1.9)
    out_proj_w = bell_draw(streams_of[10], (CONV, D), CONV ** -0.5, 0.1875, ((0, 2), (1, 32)), jnp.float32)
    proj_scale = jnp.clip(jnp.exp(math.log(2.0) - 1.3862944 * jax.random.uniform(streams_of[11], (D,), jnp.float32) ** block_scale(streams_of[11], (D,), ((0, 32),), -0.2, 0.2)), 0.5, 2.0)
    ffn_gain = jnp.clip(1.0 + 0.18 * jax.random.normal(streams_of[12], (D,), jnp.float32), 0.1, 1.9)
    gate_w = bell_draw(streams_of[13], (D, FF), D ** -0.5, 0.125, ((0, 32), (1, 2)), jnp.float32)
    up_w = bell_draw(streams_of[14], (D, FF), D ** -0.5, 0.125, ((0, 32), (1, 2)), jnp.float32)
    gate_scale = jnp.clip(jnp.exp(math.log(2.0) - 1.3862944 * jax.random.uniform(streams_of[15], (FF,), jnp.float32) ** block_scale(streams_of[15], (FF,), ((0, 64),), -0.2, 0.2)), 0.5, 2.0)
    up_scale = jnp.clip(jnp.exp(math.log(2.0) - 1.3862944 * jax.random.uniform(streams_of[16], (FF,), jnp.float32) ** block_scale(streams_of[16], (FF,), ((0, 64),), -0.2, 0.2)), 0.5, 2.0)
    gate_taps = bell_draw(streams_of[17], (KW, FF), KW ** -0.5, 3.5, ((1, 2),), jnp.float32)
    up_taps = bell_draw(streams_of[18], (KW, FF), KW ** -0.5, 3.5, ((1, 2),), jnp.float32)
    gate_bias = bell_draw(streams_of[19], (FF,), 0.5, 3.0, ((0, 2),), jnp.float32)
    up_bias = bell_draw(streams_of[20], (FF,), 0.5, 3.0, ((0, 2),), jnp.float32)
    down_w = bell_draw(streams_of[21], (FF, D), FF ** -0.5, 0.109375, ((0, 2), (1, 32)), jnp.float32)
    down_scale = jnp.clip(jnp.exp(math.log(2.0) - 1.3862944 * jax.random.uniform(streams_of[22], (D,), jnp.float32) ** block_scale(streams_of[22], (D,), ((0, 32),), -0.2, 0.2)), 0.5, 2.0)
    return {"tokens": tokens, "mix_gain": mix_gain, "out_gate_w": out_gate_w, "in_gate_w": in_gate_w, "value_w": value_w, "out_gate_scale": out_gate_scale, "in_gate_scale": in_gate_scale, "value_scale": value_scale, "mix_taps": mix_taps, "conv_gain": conv_gain, "out_proj_w": out_proj_w, "proj_scale": proj_scale, "ffn_gain": ffn_gain, "gate_w": gate_w, "up_w": up_w, "gate_scale": gate_scale, "up_scale": up_scale, "gate_taps": gate_taps, "up_taps": up_taps, "gate_bias": gate_bias, "up_bias": up_bias, "down_w": down_w, "down_scale": down_scale}


epsilon = 1e-06

def norm_rows(values, gain):
    return values * lax.rsqrt(lax.optimization_barrier(jnp.mean(values * values, axis=-1, keepdims=True)) + epsilon) * gain

def causal_taps(values, taps):
    kernel = taps.shape[0]
    length = values.shape[0]
    padded = jnp.pad(values, ((kernel - 1, 0), (0, 0)))
    total = jnp.zeros(values.shape, jnp.float32)
    for offset in range(kernel):
        total = total + taps[offset] * padded[offset:offset + length]
    return total

def reference(tokens, mix_gain, out_gate_w, in_gate_w, value_w, out_gate_scale, in_gate_scale, value_scale, mix_taps, conv_gain, out_proj_w, proj_scale, ffn_gain, gate_w, up_w, gate_scale, up_scale, gate_taps, up_taps, gate_bias, up_bias, down_w, down_scale):

    def project(left, weight, scale):
        return jnp.dot(left, weight.astype(jnp.bfloat16), preferred_element_type=jnp.float32) * scale

    def layer_one(sequence):
        resid = sequence.astype(jnp.float32)
        normed_in = norm_rows(resid, mix_gain).astype(jnp.bfloat16)
        out_gate = project(normed_in, out_gate_w, out_gate_scale).astype(jnp.bfloat16)
        in_gate = project(normed_in, in_gate_w, in_gate_scale).astype(jnp.bfloat16)
        value_in = project(normed_in, value_w, value_scale).astype(jnp.bfloat16)
        mixed_in = in_gate.astype(jnp.float32) * value_in.astype(jnp.float32)
        conv_out = (out_gate.astype(jnp.float32) * causal_taps(mixed_in, mix_taps)).astype(jnp.bfloat16)
        mixed = norm_rows(conv_out.astype(jnp.float32), conv_gain).astype(jnp.bfloat16)
        first = (resid + project(mixed, out_proj_w, proj_scale)).astype(jnp.bfloat16)
        resid_two = first.astype(jnp.float32)
        normed_ffn = norm_rows(resid_two, ffn_gain).astype(jnp.bfloat16)
        gate_pre = project(normed_ffn, gate_w, gate_scale).astype(jnp.bfloat16)
        up_pre = project(normed_ffn, up_w, up_scale).astype(jnp.bfloat16)
        gate_act = causal_taps(gate_pre.astype(jnp.float32), gate_taps) + gate_bias
        up_act = causal_taps(up_pre.astype(jnp.float32), up_taps) + up_bias
        hidden = (jax.nn.silu(gate_act) * up_act).astype(jnp.bfloat16)
        return (resid_two + project(hidden, down_w, down_scale)).astype(jnp.bfloat16)
    return lax.map(layer_one, tokens)
```

```python
import jax
import jax.numpy as jnp
from jax import lax
from jax.experimental import pallas as pl
from jax.experimental.pallas import tpu as pltpu
from jax.sharding import PartitionSpec as P

epsilon = 1e-06
MESH = pl.DeviceIdType.MESH
UNIT = 256
TURNED = "so"

TREES = {
    "A": (
        ((), "x+", 1),
        ((), "x-", 1),
        ("s01", "xs", 1),
        ((0, 1, 2), "y+", 4),
        ((0, 1, 2), "y-", 4),
        ((0, 1, 2), "zs", 4),
        ("s34", "ys", 4),
        ("s34", "zo", 4),
        ("o34", "zo", 4),
        ((6,), "zs", 4),
    ),
    "D": (
        ((), "zs", 1),
        ((0,), "y+", 2),
        ((0,), "y-", 2),
        ("s12", "ys", 2),
        ((1, 2, 3), "x+", 8),
        ((1, 2, 3), "x-", 8),
        ((4,), "x+", 4),
        ((5,), "x-", 4),
    ),
}


def needs_of(kind, m, turn):
    need = TREES[kind][m][0]
    if isinstance(need, str):
        first, second = int(need[1]), int(need[2])
        return (first if (turn > 0) == (need[0] == "s") else second,)
    return need


def link_of(kind, m, turn):
    name = TREES[kind][m][1]
    sign = {"+": 1, "-": -1, "s": turn, "o": -turn}[name[1]]
    return name[0], sign


def plan(chunks, comps, rate=44.0, hop=2.2, issue=0.04, ahead=4.0):
    links = {(a, s): 0.0 for a in "xyz" for s in (1, -1)}
    arrive, waited, sent, ops, done, t = {}, set(), set(), [], set(), 0.0
    every = [(c, m) for c in range(len(chunks)) for m in range(len(TREES[chunks[c][0]]))]

    def wait(pairs):
        for pair in pairs:
            if pair not in waited:
                waited.add(pair)
                ops.append(("wait", *pair))

    while True:
        best = None
        for c, m in every:
            kind, turn, size = chunks[c]
            if (c, m) in sent:
                continue
            needs = [(c, k) for k in needs_of(kind, m, turn)]
            link = link_of(kind, m, turn)
            if all(arrive.get(k, 1e9) <= t for k in needs) and links[link] <= t + ahead:
                best = (c, m, needs, link, size * TREES[kind][m][2])
                break
        if best is not None:
            c, m, needs, link, size = best
            wait(needs)
            ops.append(("send", c, m))
            sent.add((c, m))
            t += issue
            links[link] = max(t, links[link]) + size / rate / 1000.0
            arrive[c, m] = links[link] + hop
            continue
        for k, (us, of_chunks, of_comps) in enumerate(comps):
            pairs = [(c, m) for c, m in every if c in of_chunks]
            if k not in done and done.issuperset(of_comps) and all(arrive.get(q, 1e9) <= t for q in pairs):
                wait(pairs)
                ops.append(("comp", k))
                done.add(k)
                t += us
                break
        else:
            later = [a for a in arrive.values() if a > t] + [b - ahead for b in links.values() if b - ahead > t]
            if not later:
                break
            t = min(later) + 1e-6
    wait(every)
    return ops, t


def list_of_chunks(n_mix, n_pj, n_gu, n_dn):
    item = 64 * UNIT * 2
    chunks, where, count = [("A", 1, 4096)], [("sc", 0, 128)], {"A": 0, "D": 0}

    def add(name, kinds, units):
        for i, kind in enumerate(kinds):
            width = min(1.0, units - i)
            turn = 1 if count[kind] % 2 == 0 else -1
            count[kind] += 1
            chunks.append((kind, turn, int(item * width)))
            where.append((name, i, int(UNIT * width)))

    add("mix", "ADAADA", n_mix)
    add("pj", "AD", n_pj)
    add("gu", "ADAADAADAAD", n_gu)
    add("dn", "ADADAA", n_dn)
    return chunks, where


CHUNKS, WHERE = list_of_chunks(6, 2, 11, 5.5)


def place():
    rep, fs = lax.axis_index("rep"), lax.axis_index("fs")
    tp = lax.axis_index("tp")
    x, y, zl = lax.rem(fs, 4), lax.rem(fs // 4, 4), fs // 16
    z = rep * 2 + zl
    near = {}
    for sign in (1, -1):
        near["x", sign] = (rep, zl * 16 + y * 4 + lax.rem(x + 4 + sign, 4), tp)
        near["y", sign] = (rep, zl * 16 + lax.rem(y + 4 + sign, 4) * 4 + x, tp)
        zn = lax.rem(z + 4 + sign, 4)
        near["z", sign] = (zn // 2, lax.rem(zn, 2) * 16 + y * 4 + x, tp)
    return x, y, zl, near, (rep, fs, 1 - tp)


def carried(kind, m, turn, x, y, z, arriving):
    link, sign = link_of(kind, m, turn)
    if arriving:
        if link == "x":
            x = lax.rem(x + 4 - sign, 4)
        elif link == "y":
            y = lax.rem(y + 4 - sign, 4)
        else:
            z = 1 - z

    def step(v, n):
        return lax.rem(v + 4 + n, 4)

    if kind == "A":
        return {
            0: (z, y, x),
            1: (z, y, x),
            2: (z, y, step(x, -turn)),
            3: (z, y, None),
            4: (z, y, None),
            5: (z, y, None),
            6: (z, step(y, -turn), None),
            7: (z, step(y, -turn), None),
            8: (z, step(y, turn), None),
            9: (z, step(y, 2), None),
        }[m]
    return {
        0: (z, y, x),
        1: (None, y, x),
        2: (None, y, x),
        3: (None, step(y, -turn), x),
        4: (None, None, x),
        5: (None, None, x),
        6: (0, None, step(x, -1)),
        7: (1, None, step(x, 1)),
    }[m]


def part(bufs, c, z, y, x):
    name, i, width = WHERE[c]
    at = tuple(slice(None) if v is None else v for v in (z, y, x))
    ref = bufs[name]
    if name in ("mix", "gu"):
        return ref.at[(i, *at)]
    if name == "sc":
        return ref.at[at]
    return ref.at[(*at, slice(None), slice(i * UNIT, i * UNIT + width))]


def gather_kernel(ops, mix_in, pj_in, gu_in, dn_in, sc_in, mix, pj, gu, dn, sc, own_sem, send_sem, recv_sem):
    x, y, zl, near, other = place()
    bufs = {"mix": mix, "pj": pj, "gu": gu, "dn": dn, "sc": sc}
    own = [
        pltpu.make_async_copy(mix_in, mix.at[:, zl, y, x], own_sem.at[0]),
        pltpu.make_async_copy(pj_in, pj.at[zl, y, x], own_sem.at[1]),
        pltpu.make_async_copy(gu_in, gu.at[:, zl, y, x], own_sem.at[2]),
        pltpu.make_async_copy(dn_in, dn.at[zl, y, x], own_sem.at[3]),
        pltpu.make_async_copy(sc_in, sc.at[zl, y, x], own_sem.at[4]),
    ]
    for copy in own:
        copy.start()
    barrier = pltpu.get_barrier_semaphore()
    for device in near.values():
        pl.semaphore_signal(barrier, inc=1, device_id=device, device_id_type=MESH)
    pl.semaphore_wait(barrier, 6)
    for copy in own:
        copy.wait()

    def copy_of(c, m, arriving):
        kind, turn, _ = CHUNKS[c]
        ref = part(bufs, c, *carried(kind, m, turn, x, y, zl, arriving))
        return pltpu.make_async_remote_copy(
            src_ref=ref,
            dst_ref=ref,
            send_sem=send_sem.at[c],
            recv_sem=recv_sem.at[c, m],
            device_id=near[link_of(kind, m, turn)],
            device_id_type=MESH,
        )

    for op in ops:
        if op[0] == "send":
            copy_of(op[1], op[2], False).start()
        elif op[0] == "wait":
            copy_of(op[1], op[2], True).wait_recv()
    for c, (kind, turn, _) in enumerate(CHUNKS):
        for m in range(len(TREES[kind])):
            copy_of(c, m, False).wait_send()


def gather(mix, pj, gu, dn, sc):
    ops, _ = plan(CHUNKS, [])
    f32, bf16 = jnp.float32, jnp.bfloat16
    shapes = [
        ((6, 2, 4, 4, 64, 256), bf16),
        ((2, 4, 4, 64, 512), bf16),
        ((11, 2, 4, 4, 64, 256), bf16),
        ((2, 4, 4, 64, 1408), bf16),
        ((2, 4, 4, 8, 128), f32),
    ]
    return pl.pallas_call(
        lambda *refs: gather_kernel(ops, *refs),
        out_shape=[jax.ShapeDtypeStruct(*s) for s in shapes],
        in_specs=[pl.BlockSpec(memory_space=pl.ANY)] * 5,
        out_specs=[pl.BlockSpec(memory_space=pltpu.VMEM)] * 5,
        scratch_shapes=[
            pltpu.SemaphoreType.DMA((5,)),
            pltpu.SemaphoreType.DMA((len(CHUNKS),)),
            pltpu.SemaphoreType.DMA((len(CHUNKS), 10)),
        ],
        compiler_params=pltpu.CompilerParams(collective_id=0, has_side_effects=True, vmem_limit_bytes=60 * 1024 * 1024),
    )(mix, pj, gu, dn, sc)


def norm_rows(values, gain):
    return values * lax.rsqrt(jnp.mean(values * values, axis=-1, keepdims=True) + epsilon) * gain


def causal_taps(values, taps):
    kernel = taps.shape[0]
    length = values.shape[0]
    padded = jnp.pad(values, ((kernel - 1, 0), (0, 0)))
    total = jnp.zeros(values.shape, jnp.float32)
    for offset in range(kernel):
        total = total + taps[offset] * padded[offset : offset + length]
    return total


def summed_on_arrival(shard, axis, dim):
    size = lax.axis_size(axis)
    parts = shard.reshape(size, -1, shard.shape[1])
    parts = lax.all_to_all(parts, axis, 0, 0, tiled=True)
    return jnp.sum(parts.astype(jnp.float32), axis=0)


def local(
    tokens, mix_gain, out_gate_w, in_gate_w, value_w, out_gate_scale, in_gate_scale, value_scale, mix_taps, conv_gain,
    out_proj_w, proj_scale, ffn_gain, gate_w, up_w, gate_scale, up_scale, gate_taps, up_taps, gate_bias, up_bias, down_w,
    down_scale,
):
    f32, bf16 = jnp.float32, jnp.bfloat16
    resid = tokens[0].astype(f32)
    mix_own = jnp.stack(
        [w.astype(bf16)[:, 256 * g : 256 * g + 256] for g in (0, 1) for w in (in_gate_w, value_w, out_gate_w)]
    )
    gu_own = jnp.stack(
        [
            jnp.concatenate([w[:, 128 * k : 128 * k + 128] for w in (gate_w, up_w)], axis=1).astype(bf16)
            for k in range(11)
        ]
    )
    pj_own = out_proj_w.astype(bf16).T
    dn_own = down_w.astype(bf16).T
    sc_own = jnp.stack(
        [
            jnp.pad(s, (0, 128 - s.shape[0]))
            for s in (in_gate_scale, value_scale, out_gate_scale, gate_scale, up_scale, proj_scale, down_scale)
        ]
        + [jnp.zeros(128, f32)]
    )
    mix, pj, gu, dn, sc = gather(mix_own, pj_own, gu_own, dn_own, sc_own)
    mix = mix.reshape(6, 2048, 256)
    gu = gu.reshape(11, 2048, 256)
    pj, dn = pj.reshape(2048, 512), dn.reshape(2048, 1408)
    sc = sc.reshape(32, 8, 128)
    s_in, s_val, s_out = (sc[:, k, :16].reshape(-1) for k in range(3))
    s_gate, s_up = (sc[:, k, :44].reshape(-1) for k in (3, 4))
    s_pj, s_dn = (sc[:, k, :64].reshape(-1) for k in (5, 6))

    normed_in = norm_rows(resid, mix_gain).astype(bf16)
    rows = lax.all_gather(normed_in, "tp", axis=0, tiled=True)

    def product(left, right):
        return jnp.dot(left, right, preferred_element_type=f32)

    def pair(a, b, scale):
        both = jnp.concatenate([product(rows, mix[a]), product(rows, mix[b])], axis=1)
        return (both * scale).astype(bf16).astype(f32)

    in_gate, value_in, out_gate = pair(0, 3, s_in), pair(1, 4, s_val), pair(2, 5, s_out)
    conv = (out_gate * causal_taps(in_gate * value_in, mix_taps)).astype(bf16).astype(f32)
    sumsq = lax.psum(jnp.sum(conv * conv, axis=1), "tp")
    mixed = (conv * lax.rsqrt(sumsq / 1024 + epsilon)[:, None] * conv_gain).astype(bf16)
    partial = lax.dot_general(mixed, pj, (((1,), (1,)), ((), ())), preferred_element_type=f32) * s_pj
    first = (resid + summed_on_arrival(partial.astype(bf16), "tp", 0)).astype(bf16).astype(f32)
    normed = norm_rows(first, ffn_gain).astype(bf16)
    rows_two = lax.all_gather(normed, "tp", axis=0, tiled=True)
    pre = [product(rows_two, gu[k]) for k in range(11)]
    gate_pre = (jnp.concatenate([p[:, :128] for p in pre], axis=1) * s_gate).astype(bf16).astype(f32)
    up_pre = (jnp.concatenate([p[:, 128:] for p in pre], axis=1) * s_up).astype(bf16).astype(f32)
    hidden = (jax.nn.silu(causal_taps(gate_pre, gate_taps) + gate_bias) * (causal_taps(up_pre, up_taps) + up_bias)).astype(bf16)
    partial = lax.dot_general(hidden, dn, (((1,), (1,)), ((), ())), preferred_element_type=f32) * s_dn
    return (first + summed_on_arrival(partial.astype(bf16), "tp", 0)).astype(bf16)[None]


def solution(mesh):
    placed = (
        P(("rep", "fs"), "tp", None), P(), P("fs", "tp"), P("fs", "tp"), P("fs", "tp"), P(("tp", "fs")), P(("tp", "fs")),
        P(("tp", "fs")), P(None, "tp"), P("tp"), P("tp", "fs"), P("fs"), P(), P("fs", "tp"), P("fs", "tp"), P(("tp", "fs")),
        P(("tp", "fs")), P(None, "tp"), P(None, "tp"), P("tp"), P("tp"), P("tp", "fs"), P("fs"),
    )
    return jax.shard_map(
        local, mesh=mesh, in_specs=placed, out_specs=P(("rep", "fs"), "tp", None), check_vma=False
    )
```

```python
import jax
import jax.numpy as jnp
from jax import lax
from jax.experimental import pallas as pl
from jax.experimental.pallas import tpu as pltpu
from jax.sharding import PartitionSpec as P

epsilon = 1e-06
MESH = pl.DeviceIdType.MESH
UNIT = 256
TURNED = "so"

TREES = {
    "A": (
        ((), "x+", 1),
        ((), "x-", 1),
        ("s01", "xs", 1),
        ((0, 1, 2), "y+", 4),
        ((0, 1, 2), "y-", 4),
        ((0, 1, 2), "zs", 4),
        ("s34", "ys", 4),
        ("s34", "zo", 4),
        ("o34", "zo", 4),
        ((6,), "zs", 4),
    ),
    "D": (
        ((), "zs", 1),
        ((0,), "y+", 2),
        ((0,), "y-", 2),
        ("s12", "ys", 2),
        ((1, 2, 3), "x+", 8),
        ((1, 2, 3), "x-", 8),
        ((4,), "x+", 4),
        ((5,), "x-", 4),
    ),
}


def needs_of(kind, m, turn):
    need = TREES[kind][m][0]
    if isinstance(need, str):
        first, second = int(need[1]), int(need[2])
        return (first if (turn > 0) == (need[0] == "s") else second,)
    return need


def link_of(kind, m, turn):
    name = TREES[kind][m][1]
    sign = {"+": 1, "-": -1, "s": turn, "o": -turn}[name[1]]
    return name[0], sign


def plan(chunks, comps, rate=44.0, hop=2.2, issue=0.04, ahead=4.0):
    links = {(a, s): 0.0 for a in "xyz" for s in (1, -1)}
    arrive, waited, sent, ops, done, t = {}, set(), set(), [], {}, 0.0
    every = [(c, m) for c in range(len(chunks)) for m in range(len(TREES[chunks[c][0]]))]
    log = []

    def wait(pairs):
        for pair in pairs:
            if pair not in waited:
                waited.add(pair)
                ops.append(("wait", *pair))

    while True:
        best = None
        for c, m in every:
            kind, turn, size = chunks[c]
            if (c, m) in sent:
                continue
            needs = [(c, k) for k in needs_of(kind, m, turn)]
            link = link_of(kind, m, turn)
            if all(arrive.get(k, 1e9) <= t for k in needs) and links[link] <= t + ahead:
                best = (c, m, needs, link, size * TREES[kind][m][2])
                break
        if best is not None:
            c, m, needs, link, size = best
            wait(needs)
            ops.append(("send", c, m))
            sent.add((c, m))
            t += issue
            links[link] = max(t, links[link]) + size / rate / 1000.0
            arrive[c, m] = links[link] + hop
            continue
        soon = []
        for k, (us, of_chunks, of_comps) in enumerate(comps):
            if k in done:
                continue
            pairs = [(c, m) for c, m in every if c in of_chunks]
            ready = max([arrive.get(q, 1e9) for q in pairs] + [done.get(b, 1e9) + lag for b, lag in of_comps] + [0.0])
            if ready <= t:
                wait(pairs)
                ops.append(("comp", k))
                log.append((round(t, 1), k))
                t += us
                done[k] = t
                break
            if ready < 1e8:
                soon.append(ready)
        else:
            later = [a for a in arrive.values() if a > t] + [b - ahead for b in links.values() if b - ahead > t] + soon
            if not later:
                break
            t = min(later) + 1e-6
    wait(every)
    return ops, t, log, arrive


def list_of_chunks(n_mix, n_pj, n_gu, n_dn):
    item = 64 * UNIT * 2
    chunks, where, count = [("A", 1, 4096)], [("sc", 0, 128)], {"A": 0, "D": 0}

    def add(name, kinds, units):
        for i, kind in enumerate(kinds):
            width = min(1.0, units - i)
            turn = 1 if count[kind] % 2 == 0 else -1
            count[kind] += 1
            chunks.append((kind, turn, int(item * width)))
            where.append((name, i, int(UNIT * width)))

    add("mix", "ADAADA", n_mix)
    add("pj", "AD", n_pj)
    add("gu", "ADAADAADAAD", n_gu)
    add("dn", "ADADAA", n_dn)
    return chunks, where


CHUNKS, WHERE = list_of_chunks(6, 2, 11, 5.5)
CHUNK_OF = {(name, i): c for c, (name, i, _) in enumerate(WHERE)}
ROWS = 256


def list_of_blocks():
    names, comps, number = [], [], {}

    def add(name, us, chunks=(), after=()):
        number[name] = len(names)
        names.append(name)
        comps.append((us, {CHUNK_OF[c] for c in chunks}, [(number[b], lag) for b, lag in after]))

    add(("norm",), 2.5)
    add(("scales",), 1.0, [("sc", 0)])
    for k in range(6):
        add(("mix", k), 1.5, [("mix", k)], [(("norm",), 4.0), (("scales",), 0.0)])
    for g in range(2):
        add(("conv", g), 1.2, [], [(("mix", 3 * g + i), 0.0) for i in range(3)] + [(("conv", 0), 0.0)] * g)
    add(("proj", 0), 1.3, [("pj", 0), ("pj", 1)], [(("conv", 0), 0.0), (("conv", 1), 0.0)])
    add(("proj", 1), 1.3, [], [(("proj", 0), 0.0)])
    add(("first",), 2.5, [], [(("proj", 1), 3.0)])
    for k in range(11):
        add(("gu", k), 2.2, [("gu", k)], [(("first",), 4.0)])
    for j in range(6):
        add(("down", j), 1.5, [("dn", j)], [(("gu", k), 0.0) for k in (2 * j, 2 * j + 1) if k < 11] + ([(("down", j - 1), 0.0)] if j else []))
    add(("last",), 3.0, [], [(("down", 5), 3.0)])
    return names, comps


def place():
    rep, fs = lax.axis_index("rep"), lax.axis_index("fs")
    tp = lax.axis_index("tp")
    x, y, zl = lax.rem(fs, 4), lax.rem(fs // 4, 4), fs // 16
    z = rep * 2 + zl
    xs = {n: lax.rem(x + 4 + n, 4) for n in (-1, 1, 2)} | {0: x}
    ys = {n: lax.rem(y + 4 + n, 4) for n in (-1, 1, 2)} | {0: y}
    near = {}
    for sign in (1, -1):
        near["x", sign] = (rep, zl * 16 + y * 4 + xs[sign], tp)
        near["y", sign] = (rep, zl * 16 + ys[sign] * 4 + x, tp)
        zn = lax.rem(z + 4 + sign, 4)
        near["z", sign] = (zn // 2, lax.rem(zn, 2) * 16 + y * 4 + x, tp)
    return xs, ys, {0: zl, 1: 1 - zl}, near, (rep, fs, 1 - tp), tp


def carried(kind, m, turn, arriving):
    sent = {
        "A": (
            (0, 0, 0),
            (0, 0, 0),
            (0, 0, -turn),
            (0, 0, None),
            (0, 0, None),
            (0, 0, None),
            (0, -turn, None),
            (0, -turn, None),
            (0, turn, None),
            (0, 2, None),
        ),
        "D": (
            (0, 0, 0),
            (None, 0, 0),
            (None, 0, 0),
            (None, -turn, 0),
            (None, None, 0),
            (None, None, 0),
            ("plane0", None, -1),
            ("plane1", None, 1),
        ),
    }[kind][m]
    if not arriving:
        return sent
    link, sign = link_of(kind, m, turn)
    z, y, x = sent

    def back(v, n):
        v = v - n
        return v + 4 if v < -1 else v - 4 if v > 2 else v

    if link == "x":
        x = back(x, sign)
    elif link == "y":
        y = back(y, sign)
    else:
        z = 1 - z
    return z, y, x


def mega_kernel(
    ops, names, tokens, mix_in, pj_in, gu_in, dn_in, sc_in, mix_gain, ffn_gain, mix_taps, conv_gain, gate_taps, up_taps,
    gate_bias, up_bias, out, mix, pj, gu, dn, sc, tok, rows, gates, conv, square, acc, hidden, psend, precv, sqrecv, sv_mix,
    sv_gu, sv_pj, sv_dn, own_sem, send_sem, recv_sem, side_send, side_recv, out_sem,
):
    f32, bf16 = jnp.float32, jnp.bfloat16
    xs, ys, zs, near, other, tp = place()
    bufs = {"mix": mix, "pj": pj, "gu": gu, "dn": dn, "sc": sc}
    x, y, zl = xs[0], ys[0], zs[0]
    mine = pl.multiple_of(tp * 512, 512)
    yours = pl.multiple_of((1 - tp) * 512, 512)
    own = [
        pltpu.make_async_copy(sc_in, sc.at[zl, y, x], own_sem.at[0]),
        pltpu.make_async_copy(mix_in, mix.at[:, zl, y, x], own_sem.at[1]),
        pltpu.make_async_copy(pj_in, pj.at[zl, y, x], own_sem.at[2]),
        pltpu.make_async_copy(tokens, tok, own_sem.at[3]),
        pltpu.make_async_copy(gu_in, gu.at[:, zl, y, x], own_sem.at[4]),
        pltpu.make_async_copy(dn_in, dn.at[zl, y, x], own_sem.at[5]),
    ]
    for copy in own:
        copy.start()
    barrier = pltpu.get_barrier_semaphore()
    for device in [*near.values(), other]:
        pl.semaphore_signal(barrier, inc=1, device_id=device, device_id_type=MESH)
    pl.semaphore_wait(barrier, 7)
    for copy in own:
        copy.wait()

    def part(c, at):
        name, i, width = WHERE[c]
        z, y, x = at
        z = slice(None) if z is None else int(z[-1]) if isinstance(z, str) else zs[z]
        y = slice(None) if y is None else ys[y]
        x = slice(None) if x is None else xs[x]
        ref = bufs[name]
        if name in ("mix", "gu"):
            return ref.at[i, z, y, x]
        if name == "sc":
            return ref.at[z, y, x]
        return ref.at[z, y, x, :, i * UNIT : i * UNIT + width]

    def copy_of(c, m, arriving):
        kind, turn, _ = CHUNKS[c]
        ref = part(c, carried(kind, m, turn, arriving))
        return pltpu.make_async_remote_copy(
            src_ref=ref,
            dst_ref=ref,
            send_sem=send_sem.at[c],
            recv_sem=recv_sem.at[c, m],
            device_id=near[link_of(kind, m, turn)],
            device_id_type=MESH,
        )

    def to_other(src, dst, i):
        return pltpu.make_async_remote_copy(
            src_ref=src, dst_ref=dst, send_sem=side_send.at[i], recv_sem=side_recv.at[i], device_id=other, device_id_type=MESH
        )

    def normed(values, gain):
        return (values * lax.rsqrt(jnp.mean(values * values, axis=1, keepdims=True) + epsilon) * gain[...]).astype(bf16)

    def shifted(values, before):
        both = jnp.concatenate([before, values], axis=0)
        return pltpu.roll(both, 1, 0)[8:], pltpu.roll(both, 2, 0)[8:]

    def dot_nt(left, right):
        return lax.dot_general(left, right, (((1,), (1,)), ((), ())), preferred_element_type=f32)

    def spread(row, width, group):
        total = jnp.zeros((1, 128), f32)
        lane = lax.broadcasted_iota(jnp.int32, (1, 128), 1)
        for s in range(group * 128 // width, min(31, (group * 128 + 127) // width) + 1):
            at = s * width - group * 128
            line = sc[s // 16, s // 4 % 4, s % 4, row : row + 1, :]
            if at % 128:
                line = pltpu.roll(line, at % 128, 1)
            total = jnp.where((lane >= at) & (lane < at + width), line, total)
        return total

    send_rows = [to_other(rows.at[pl.ds(mine, 512)], rows.at[pl.ds(mine, 512)], i) for i in (0, 3)]
    recv_rows = [to_other(rows.at[pl.ds(yours, 512)], rows.at[pl.ds(yours, 512)], i) for i in (0, 3)]
    send_sums = [to_other(psend, precv, i) for i in (1, 4)]
    send_square = to_other(square.at[pl.ds(yours, 512)], sqrecv, 2)
    seen = set()

    def block_norm():
        @pl.loop(0, 512, step=64)
        def _(r):
            at = pl.multiple_of(r, 64)
            rows[pl.ds(mine + at, 64), :] = normed(tok[pl.ds(at, 64), :].astype(f32), mix_gain)

        send_rows[0].start()

    def block_scales():
        for k in range(6):
            for i in range(2):
                sv_mix[k, :, 128 * i : 128 * i + 128] = spread(k % 3, 16, k // 3 * 2 + i)
        for k in range(11):
            sv_gu[k, :, :128] = spread(3, 44, k)
            sv_gu[k, :, 128:] = spread(4, 44, k)
        for k in range(16):
            sv_pj[k // 4, :, 128 * (k % 4) : 128 * (k % 4) + 128] = spread(5, 64, k)
            sv_dn[k // 4, :, 128 * (k % 4) : 128 * (k % 4) + 128] = spread(6, 64, k)

    def block_mix(k):
        if "rows" not in seen:
            seen.add("rows")
            recv_rows[0].wait_recv()

        @pl.loop(0, 1024, step=ROWS)
        def _(r):
            at = pl.ds(pl.multiple_of(r, ROWS), ROWS)
            weight = mix[k].reshape(2048, 256)
            gates[k, at, :] = (jnp.dot(rows[at, :], weight, preferred_element_type=f32) * sv_mix[k]).astype(bf16)

    def block_conv(g):
        cols = slice(256 * g, 256 * g + 256)
        taps, gain = mix_taps[:, cols], conv_gain[:, cols]

        def body(i, before):
            at = pl.ds(pl.multiple_of(i * 128, 128), 128)
            value = gates[3 * g, at, :].astype(f32) * gates[3 * g + 1, at, :].astype(f32)
            one, two = shifted(value, before)
            total = taps[0:1] * two + taps[1:2] * one + taps[2:3] * value
            done = (gates[3 * g + 2, at, :].astype(f32) * total).astype(bf16).astype(f32)
            conv[at, cols] = (done * gain).astype(bf16)
            squares = jnp.broadcast_to(jnp.sum(done * done, axis=1, keepdims=True), (128, 128))
            square[at, :] = squares if g == 0 else square[at, :] + squares
            return value[-8:]

        lax.fori_loop(0, 8, body, jnp.zeros((8, 256), f32))
        if g == 1:
            send_square.start()

    def block_proj(half):
        start = yours if half == 0 else mine

        @pl.loop(0, 8)
        def _(i):
            r, n = pl.multiple_of(i // 4 * ROWS, ROWS), i % 4
            weight = pj[n // 2, pl.ds(n % 2 * 2, 2)].reshape(512, 512)
            part_sum = dot_nt(conv[pl.ds(start + r, ROWS), :], weight) * sv_pj[n]
            cols = pl.ds(pl.multiple_of(n * 512, 512), 512)
            if half == 0:
                psend[pl.ds(r, ROWS), cols] = part_sum.astype(bf16)
            else:
                acc[pl.ds(start + r, ROWS), cols] = part_sum

        if half == 0:
            send_sums[0].start()

    def block_first():
        send_sums[0].wait_recv()
        send_square.wait_recv()
        send_rows[0].wait_send()

        @pl.loop(0, 512, step=64)
        def _(r):
            at = pl.ds(pl.multiple_of(r, 64), 64)
            there = pl.ds(pl.multiple_of(mine + r, 64), 64)
            squares = square[there, :1] + sqrecv[at, :1]
            summed = (acc[there, :] + precv[at, :].astype(f32)) * lax.rsqrt(squares / 1024 + epsilon)
            first = (tok[at, :].astype(f32) + summed).astype(bf16)
            tok[at, :] = first
            rows[there, :] = normed(first.astype(f32), ffn_gain)

        send_rows[1].start()

    def block_gu(k):
        if "rows2" not in seen:
            seen.add("rows2")
            recv_rows[1].wait_recv()
        cols = slice(128 * k, 128 * k + 128)

        def body(i, before):
            at = pl.ds(pl.multiple_of(i * ROWS, ROWS), ROWS)
            weight = gu[k].reshape(2048, 256)
            pre = (jnp.dot(rows[at, :], weight, preferred_element_type=f32) * sv_gu[k]).astype(bf16).astype(f32)
            one, two = shifted(pre, before)
            acts = []
            for j, (taps, bias) in enumerate(((gate_taps, gate_bias), (up_taps, up_bias))):
                half, t = slice(128 * j, 128 * j + 128), taps[:, cols]
                acts.append(t[0:1] * two[:, half] + t[1:2] * one[:, half] + t[2:3] * pre[:, half] + bias[:, cols])
            hidden[at, cols] = (acts[0] / (1.0 + jnp.exp(-acts[0])) * acts[1]).astype(bf16)
            return pre[-8:]

        lax.fori_loop(0, 1024 // ROWS, body, jnp.zeros((8, 256), f32))

    def block_down(j):
        width = WHERE[CHUNK_OF["dn", j]][2]
        lanes = slice(UNIT * j, UNIT * j + width)

        def product(r, n):
            weight = dn[n // 2, pl.ds(n % 2 * 2, 2), :, :, lanes].reshape(512, width)
            return dot_nt(hidden[pl.ds(r, ROWS), lanes], weight)

        def sweep(first, count, store):
            @pl.loop(0, count * 4)
            def _(i):
                r, n = pl.multiple_of(first + i // 4 * ROWS, ROWS), i % 4
                cols = pl.ds(pl.multiple_of(n * 512, 512), 512)
                store(i // 4 * ROWS, r, n, cols)

        if j < 5:

            def store(_, r, n, cols):
                value = product(r, n)
                acc[pl.ds(r, ROWS), cols] = value if j == 0 else acc[pl.ds(r, ROWS), cols] + value

            sweep(0, 4, store)
            return
        send_sums[0].wait_send()

        def give(here, r, n, cols):
            value = (acc[pl.ds(r, ROWS), cols] + product(r, n)) * sv_dn[n]
            psend[pl.ds(pl.multiple_of(here, ROWS), ROWS), cols] = value.astype(bf16)

        sweep(yours, 2, give)
        send_sums[1].start()

        def keep(_, r, n, cols):
            acc[pl.ds(r, ROWS), cols] = (acc[pl.ds(r, ROWS), cols] + product(r, n)) * sv_dn[n]

        sweep(mine, 2, keep)

    def block_last():
        send_sums[1].wait_recv()
        send_rows[1].wait_send()
        outs = []
        for q in range(4):

            @pl.loop(0, 128, step=64)
            def _(r):
                at = pl.ds(pl.multiple_of(q * 128 + r, 64), 64)
                there = pl.ds(pl.multiple_of(mine + q * 128 + r, 64), 64)
                summed = acc[there, :] + precv[at, :].astype(f32)
                rows[there, :] = (tok[at, :].astype(f32) + summed).astype(bf16)

            outs.append(
                pltpu.make_async_copy(rows.at[pl.ds(mine + q * 128, 128)], out.at[pl.ds(q * 128, 128)], out_sem.at[q])
            )
            outs[-1].start()
        for copy in outs:
            copy.wait()

    blocks = {
        "norm": block_norm, "scales": block_scales, "mix": block_mix, "conv": block_conv, "proj": block_proj,
        "first": block_first, "gu": block_gu, "down": block_down, "last": block_last,
    }
    for op in ops:
        if op[0] == "send":
            copy_of(op[1], op[2], False).start()
        elif op[0] == "wait":
            copy_of(op[1], op[2], True).wait_recv()
        else:
            name, *index = names[op[1]]
            blocks[name](*index)
    for c, (kind, turn, _) in enumerate(CHUNKS):
        for m in range(len(TREES[kind])):
            copy_of(c, m, False).wait_send()
    send_square.wait_send()
    send_sums[1].wait_send()


def mega(*args):
    names, comps = list_of_blocks()
    ops, _, _, _ = plan(CHUNKS, comps)
    f32, bf16 = jnp.float32, jnp.bfloat16
    hbm, vmem = pl.BlockSpec(memory_space=pl.ANY), pl.BlockSpec(memory_space=pltpu.VMEM)
    dma = pltpu.SemaphoreType.DMA
    return pl.pallas_call(
        lambda *refs: mega_kernel(ops, names, *refs),
        out_shape=jax.ShapeDtypeStruct((512, 2048), bf16),
        in_specs=[hbm] * 6 + [vmem] * 8,
        out_specs=hbm,
        scratch_shapes=[
            pltpu.VMEM((6, 2, 4, 4, 64, 256), bf16),
            pltpu.VMEM((2, 4, 4, 64, 512), bf16),
            pltpu.VMEM((11, 2, 4, 4, 64, 256), bf16),
            pltpu.VMEM((2, 4, 4, 64, 1408), bf16),
            pltpu.VMEM((2, 4, 4, 8, 128), f32),
            pltpu.VMEM((512, 2048), bf16),
            pltpu.VMEM((1024, 2048), bf16),
            pltpu.VMEM((6, 1024, 256), bf16),
            pltpu.VMEM((1024, 512), bf16),
            pltpu.VMEM((1024, 128), f32),
            pltpu.VMEM((1024, 2048), f32),
            pltpu.VMEM((1024, 1408), bf16),
            pltpu.VMEM((512, 2048), bf16),
            pltpu.VMEM((512, 2048), bf16),
            pltpu.VMEM((512, 128), f32),
            pltpu.VMEM((6, 1, 256), f32),
            pltpu.VMEM((11, 1, 256), f32),
            pltpu.VMEM((4, 1, 512), f32),
            pltpu.VMEM((4, 1, 512), f32),
            dma((6,)),
            dma((len(CHUNKS),)),
            dma((len(CHUNKS), 10)),
            dma((5,)),
            dma((5,)),
            dma((4,)),
        ],
        compiler_params=pltpu.CompilerParams(collective_id=0, has_side_effects=True, vmem_limit_bytes=62 * 1024 * 1024),
    )(*args)


def local(
    tokens, mix_gain, out_gate_w, in_gate_w, value_w, out_gate_scale, in_gate_scale, value_scale, mix_taps, conv_gain,
    out_proj_w, proj_scale, ffn_gain, gate_w, up_w, gate_scale, up_scale, gate_taps, up_taps, gate_bias, up_bias, down_w,
    down_scale,
):
    f32, bf16 = jnp.float32, jnp.bfloat16
    mix_own = jnp.stack(
        [w.astype(bf16)[:, 256 * g : 256 * g + 256] for g in (0, 1) for w in (in_gate_w, value_w, out_gate_w)]
    )
    gu_own = jnp.stack(
        [
            jnp.concatenate([w[:, 128 * k : 128 * k + 128] for w in (gate_w, up_w)], axis=1).astype(bf16)
            for k in range(11)
        ]
    )
    pj_own = out_proj_w.astype(bf16).T
    dn_own = down_w.astype(bf16).T
    sc_own = jnp.stack(
        [
            jnp.pad(s, (0, 128 - s.shape[0]))
            for s in (in_gate_scale, value_scale, out_gate_scale, gate_scale, up_scale, proj_scale, down_scale)
        ]
        + [jnp.zeros(128, f32)]
    )
    line = lambda v: v.reshape(1, -1)
    return mega(
        tokens[0], mix_own, pj_own, gu_own, dn_own, sc_own, line(mix_gain), line(ffn_gain), mix_taps, line(conv_gain),
        gate_taps, up_taps, line(gate_bias), line(up_bias),
    )[None]


def solution(mesh):
    placed = (
        P(("rep", "fs"), "tp", None), P(), P("fs", "tp"), P("fs", "tp"), P("fs", "tp"), P(("tp", "fs")), P(("tp", "fs")),
        P(("tp", "fs")), P(None, "tp"), P("tp"), P("tp", "fs"), P("fs"), P(), P("fs", "tp"), P("fs", "tp"), P(("tp", "fs")),
        P(("tp", "fs")), P(None, "tp"), P(None, "tp"), P("tp"), P("tp"), P("tp", "fs"), P("fs"),
    )
    return jax.shard_map(
        local, mesh=mesh, in_specs=placed, out_specs=P(("rep", "fs"), "tp", None), check_vma=False
    )
```

```python
import jax
import jax.numpy as jnp
from jax import lax
from jax.experimental import pallas as pl
from jax.experimental.pallas import tpu as pltpu
from jax.sharding import PartitionSpec as P

epsilon = 1e-06
MESH = pl.DeviceIdType.MESH
UNIT = 256
TURNED = "so"

TREES = {
    "A": (
        ((), "x+", 1),
        ((), "x-", 1),
        ("s01", "xs", 1),
        ((0, 1, 2), "y+", 4),
        ((0, 1, 2), "y-", 4),
        ((0, 1, 2), "zs", 4),
        ("s34", "ys", 4),
        ("s34", "zo", 4),
        ("o34", "zo", 4),
        ((6,), "zs", 4),
    ),
    "D": (
        ((), "zs", 1),
        ((0,), "y+", 2),
        ((0,), "y-", 2),
        ("s12", "ys", 2),
        ((1, 2, 3), "x+", 8),
        ((1, 2, 3), "x-", 8),
        ((4,), "x+", 4),
        ((5,), "x-", 4),
    ),
}


def needs_of(kind, m, turn):
    need = TREES[kind][m][0]
    if isinstance(need, str):
        first, second = int(need[1]), int(need[2])
        return (first if (turn > 0) == (need[0] == "s") else second,)
    return need


def link_of(kind, m, turn):
    name = TREES[kind][m][1]
    sign = {"+": 1, "-": -1, "s": turn, "o": -turn}[name[1]]
    return name[0], sign


RATE, HOP, AHEAD = 45.0, 2.2, 3.0


def plan(chunks, comps, own_after, rate=RATE, hop=HOP, issue=0.04, ahead=AHEAD):
    links = {(a, s): 0.0 for a in "xyz" for s in (1, -1)}
    arrive, waited, sent, ops, done, t = {}, set(), set(), [], {}, 0.0
    every = [(c, m) for c in range(len(chunks)) for m in range(len(TREES[chunks[c][0]]))]
    log = []

    def wait(pairs):
        for pair in pairs:
            if pair not in waited:
                waited.add(pair)
                ops.append(("wait", *pair))

    while True:
        best = None
        for c, m in every:
            kind, turn, size = chunks[c]
            if (c, m) in sent:
                continue
            needs = [(c, k) for k in needs_of(kind, m, turn)]
            link = link_of(kind, m, turn)
            here = bool(needs) or c not in own_after or own_after[c] in done
            if here and all(arrive.get(k, 1e9) <= t for k in needs) and links[link] <= t + ahead:
                best = (c, m, needs, link, size * TREES[kind][m][2])
                break
        if best is not None:
            c, m, needs, link, size = best
            wait(needs)
            ops.append(("send", c, m))
            sent.add((c, m))
            t += issue
            links[link] = max(t, links[link]) + size / rate / 1000.0
            arrive[c, m] = links[link] + hop
            continue
        soon = []
        for k, (us, of_chunks, of_comps) in enumerate(comps):
            if k in done:
                continue
            pairs = [(c, m) for c, m in every if c in of_chunks]
            ready = max([arrive.get(q, 1e9) for q in pairs] + [done.get(b, 1e9) + lag for b, lag in of_comps] + [0.0])
            if ready <= t:
                wait(pairs)
                ops.append(("comp", k))
                log.append((round(t, 1), k))
                t += us
                done[k] = t
                break
            if ready < 1e8:
                soon.append(ready)
        else:
            later = [a for a in arrive.values() if a > t] + [b - ahead for b in links.values() if b - ahead > t] + soon
            if not later:
                break
            t = min(later) + 1e-6
    wait(every)
    return ops, t, log, arrive


def list_of_chunks(n_mix, n_pj, n_gu, n_dn):
    item = 64 * UNIT * 2
    chunks, where, count = [("A", 1, 4096)], [("sc", 0, 128)], {"A": 0, "D": 0}

    def add(name, kinds, units):
        for i, kind in enumerate(kinds):
            width = min(1.0, units - i)
            turn = 1 if count[kind] % 2 == 0 else -1
            count[kind] += 1
            chunks.append((kind, turn, int(item * width)))
            where.append((name, i, int(UNIT * width)))

    add("mix", "ADAADA", n_mix)
    add("pj", "AD", n_pj)
    add("gu", "ADAADAADAAD", n_gu)
    add("dn", "ADADAA", n_dn)
    return chunks, where


CHUNKS, WHERE = list_of_chunks(6, 2, 11, 5.5)
CHUNK_OF = {(name, i): c for c, (name, i, _) in enumerate(WHERE)}
ROWS = 256
DOWN = ((0, 2), (2, 2), (4, 1), (5, 1))


def list_of_blocks():
    names, comps, number = [], [], {}

    def add(name, us, chunks=(), after=()):
        number[name] = len(names)
        names.append(name)
        comps.append((us, {CHUNK_OF[c] for c in chunks}, [(number[b], lag) for b, lag in after]))

    add(("cast", "gu"), 0.6)
    add(("cast", "rest"), 0.4)
    add(("norm",), 2.0)
    add(("scales",), 1.0, [("sc", 0)])
    for k in range(6):
        add(("mix", k), 1.5, [("mix", k)], [(("norm",), 4.0), (("scales",), 0.0)])
    for g in range(2):
        add(("conv", g), 1.2, [], [(("mix", 3 * g + i), 0.0) for i in range(3)] + [(("conv", 0), 0.0)] * g)
    add(("proj", 0), 1.3, [("pj", 0), ("pj", 1)], [(("conv", 0), 0.0), (("conv", 1), 0.0)])
    add(("proj", 1), 1.3, [], [(("proj", 0), 0.0)])
    add(("first",), 2.5, [], [(("proj", 1), 3.0)])
    for k in range(11):
        add(("gu", k), 2.2, [("gu", k)], [(("first",), 4.0)])
    for j, (first, count) in enumerate(DOWN):
        units = range(first, first + count)
        halves = [k for u in units for k in (2 * u, 2 * u + 1) if k < 11]
        add(("down", j), 0.3 + 1.1 * count, [("dn", u) for u in units], [(("gu", k), 0.0) for k in halves] + ([(("down", j - 1), 0.0)] if j else []))
    add(("last",), 3.0, [], [(("down", 3), 3.0)])
    own_after = {}
    for (name, _), c in CHUNK_OF.items():
        if name in ("gu", "pj", "dn"):
            own_after[c] = number["cast", "gu" if name == "gu" else "rest"]
    return names, comps, own_after


def place():
    rep, fs = lax.axis_index("rep"), lax.axis_index("fs")
    tp = lax.axis_index("tp")
    x, y, zl = lax.rem(fs, 4), lax.rem(fs // 4, 4), fs // 16
    z = rep * 2 + zl
    xs = {n: lax.rem(x + 4 + n, 4) for n in (-1, 1, 2)} | {0: x}
    ys = {n: lax.rem(y + 4 + n, 4) for n in (-1, 1, 2)} | {0: y}
    near = {}
    for sign in (1, -1):
        near["x", sign] = (rep, zl * 16 + y * 4 + xs[sign], tp)
        near["y", sign] = (rep, zl * 16 + ys[sign] * 4 + x, tp)
        zn = lax.rem(z + 4 + sign, 4)
        near["z", sign] = (zn // 2, lax.rem(zn, 2) * 16 + y * 4 + x, tp)
    return xs, ys, {0: zl, 1: 1 - zl}, near, (rep, fs, 1 - tp), tp


def carried(kind, m, turn, arriving):
    sent = {
        "A": (
            (0, 0, 0),
            (0, 0, 0),
            (0, 0, -turn),
            (0, 0, None),
            (0, 0, None),
            (0, 0, None),
            (0, -turn, None),
            (0, -turn, None),
            (0, turn, None),
            (0, 2, None),
        ),
        "D": (
            (0, 0, 0),
            (None, 0, 0),
            (None, 0, 0),
            (None, -turn, 0),
            (None, None, 0),
            (None, None, 0),
            ("plane0", None, -1),
            ("plane1", None, 1),
        ),
    }[kind][m]
    if not arriving:
        return sent
    link, sign = link_of(kind, m, turn)
    z, y, x = sent

    def back(v, n):
        v = v - n
        return v + 4 if v < -1 else v - 4 if v > 2 else v

    if link == "x":
        x = back(x, sign)
    elif link == "y":
        y = back(y, sign)
    else:
        z = 1 - z
    return z, y, x


def mega_kernel(
    ops, names, tokens, in_w, val_w, out_w, gate_w, up_w, pj_w, dn_w, in_s, val_s, out_s, gate_s, up_s, pj_s, dn_s, mix_gain,
    ffn_gain, mix_taps, conv_gain, gate_taps, up_taps, gate_bias, up_bias, out, mix, pj, gu, dn, sc, tok, rows, gates, conv, square, acc, hidden, psend, precv, sqrecv, sv_mix,
    sv_gu, sv_pj, sv_dn, own_sem, send_sem, recv_sem, side_send, side_recv,
):
    f32, bf16 = jnp.float32, jnp.bfloat16
    xs, ys, zs, near, other, tp = place()
    bufs = {"mix": mix, "pj": pj, "gu": gu, "dn": dn, "sc": sc}
    x, y, zl = xs[0], ys[0], zs[0]
    mine = pl.multiple_of(tp * 512, 512)
    yours = pl.multiple_of((1 - tp) * 512, 512)
    mix_f32 = [acc.at[64 * i : 64 * i + 64, 0:512] for i in range(3)]
    gu_f32 = [acc.at[192 + 64 * i : 256 + 64 * i, 0:1408] for i in range(2)]
    pj_f32, dn_f32 = acc.at[320:384, 0:512], acc.at[384:448, 0:1408]
    own = [
        pltpu.make_async_copy(src, dst, own_sem.at[i])
        for i, (src, dst) in enumerate(
            zip(
                (in_w, val_w, out_w, gate_w, up_w, pj_w, dn_w, tokens),
                (*mix_f32, *gu_f32, pj_f32, dn_f32, tok),
            )
        )
    ]
    for copy in own:
        copy.start()
    barrier = pltpu.get_barrier_semaphore()
    for device in [*near.values(), other]:
        pl.semaphore_signal(barrier, inc=1, device_id=device, device_id_type=MESH)
    sc[zl, y, x] = jnp.zeros((8, 128), f32)
    for i, ref in enumerate((in_s, val_s, out_s, gate_s, up_s, pj_s, dn_s)):
        sc[zl, y, x, i : i + 1, : ref.shape[0]] = ref[...].reshape(1, -1)
    for i in range(3):
        own[i].wait()
        for g in range(2):
            mix[3 * g + i, zl, y, x] = mix_f32[i][:, 256 * g : 256 * g + 256].astype(bf16)
    pl.semaphore_wait(barrier, 7)

    def block_cast(which):
        if which == "gu":
            for i in range(2):
                own[3 + i].wait()
                for k in range(11):
                    gu[k, zl, y, x, :, 128 * i : 128 * i + 128] = gu_f32[i][:, 128 * k : 128 * k + 128].astype(bf16)
        else:
            own[5].wait()
            pj[zl, y, x] = pj_f32[...].astype(bf16)
            own[6].wait()
            dn[zl, y, x] = dn_f32[...].astype(bf16)

    def part(c, at):
        name, i, width = WHERE[c]
        z, y, x = at
        z = slice(None) if z is None else int(z[-1]) if isinstance(z, str) else zs[z]
        y = slice(None) if y is None else ys[y]
        x = slice(None) if x is None else xs[x]
        ref = bufs[name]
        if name in ("mix", "gu"):
            return ref.at[i, z, y, x]
        if name == "sc":
            return ref.at[z, y, x]
        return ref.at[z, y, x, :, i * UNIT : i * UNIT + width]

    def copy_of(c, m, arriving):
        kind, turn, _ = CHUNKS[c]
        ref = part(c, carried(kind, m, turn, arriving))
        return pltpu.make_async_remote_copy(
            src_ref=ref,
            dst_ref=ref,
            send_sem=send_sem.at[c],
            recv_sem=recv_sem.at[c, m],
            device_id=near[link_of(kind, m, turn)],
            device_id_type=MESH,
        )

    def to_other(src, dst, i):
        return pltpu.make_async_remote_copy(
            src_ref=src, dst_ref=dst, send_sem=side_send.at[i], recv_sem=side_recv.at[i], device_id=other, device_id_type=MESH
        )

    def normed(values, gain):
        return (values * lax.rsqrt(jnp.mean(values * values, axis=1, keepdims=True) + epsilon) * gain[...].reshape(1, -1)).astype(bf16)

    def shifted(values, before):
        both = jnp.concatenate([before, values], axis=0)
        return pltpu.roll(both, 1, 0)[8:], pltpu.roll(both, 2, 0)[8:]

    def dot_nt(left, right):
        return lax.dot_general(left, right, (((1,), (1,)), ((), ())), preferred_element_type=f32)

    def spread(row, width, group):
        total = jnp.zeros((1, 128), f32)
        lane = lax.broadcasted_iota(jnp.int32, (1, 128), 1)
        for s in range(group * 128 // width, min(31, (group * 128 + 127) // width) + 1):
            at = s * width - group * 128
            line = sc[s // 16, s // 4 % 4, s % 4, row : row + 1, :]
            if at % 128:
                line = pltpu.roll(line, at % 128, 1)
            total = jnp.where((lane >= at) & (lane < at + width), line, total)
        return total

    send_rows = [to_other(rows.at[pl.ds(mine, 512)], rows.at[pl.ds(mine, 512)], i) for i in (0, 3)]
    recv_rows = [to_other(rows.at[pl.ds(yours, 512)], rows.at[pl.ds(yours, 512)], i) for i in (0, 3)]
    send_sums = [to_other(psend, precv, i) for i in (1, 4)]
    send_square = to_other(square.at[pl.ds(yours, 512)], sqrecv, 2)
    seen = set()

    def block_norm():
        own[7].wait()

        @pl.loop(0, 512, step=64)
        def _(r):
            at = pl.multiple_of(r, 64)
            rows[pl.ds(mine + at, 64), :] = normed(tok[pl.ds(at, 64), :].astype(f32), mix_gain)

        send_rows[0].start()

    def block_scales():
        for k in range(6):
            for i in range(2):
                sv_mix[k, :, 128 * i : 128 * i + 128] = spread(k % 3, 16, k // 3 * 2 + i)
        for k in range(11):
            sv_gu[k, :, :128] = spread(3, 44, k)
            sv_gu[k, :, 128:] = spread(4, 44, k)
        for k in range(16):
            sv_pj[k // 2, :, 128 * (k % 2) : 128 * (k % 2) + 128] = spread(5, 64, k)
            sv_dn[k // 2, :, 128 * (k % 2) : 128 * (k % 2) + 128] = spread(6, 64, k)

    def block_mix(k):
        if "rows" not in seen:
            seen.add("rows")
            recv_rows[0].wait_recv()

        for r in range(0, 1024, ROWS):
            at = pl.ds(r, ROWS)
            weight = mix[k].reshape(2048, 256)
            gates[k, at, :] = (jnp.dot(rows[at, :], weight, preferred_element_type=f32) * sv_mix[k]).astype(bf16)

    def block_conv(g):
        cols = slice(256 * g, 256 * g + 256)
        taps, gain = mix_taps[:, cols], conv_gain[cols].reshape(1, 256)

        def body(i, before):
            at = pl.ds(pl.multiple_of(i * 128, 128), 128)
            value = gates[3 * g, at, :].astype(f32) * gates[3 * g + 1, at, :].astype(f32)
            one, two = shifted(value, before)
            total = taps[0:1] * two + taps[1:2] * one + taps[2:3] * value
            done = (gates[3 * g + 2, at, :].astype(f32) * total).astype(bf16).astype(f32)
            conv[at, cols] = (done * gain).astype(bf16)
            squares = jnp.broadcast_to(jnp.sum(done * done, axis=1, keepdims=True), (128, 128))
            square[at, :] = squares if g == 0 else square[at, :] + squares
            return value[-8:]

        lax.fori_loop(0, 8, body, jnp.zeros((8, 256), f32))
        if g == 1:
            send_square.start()

    def block_proj(half):
        start = yours if half == 0 else mine

        for n in range(8):
            weight = pj[n // 4, n % 4].reshape(256, 512)
            part_sum = dot_nt(conv[pl.ds(start, 512), :], weight) * sv_pj[n]
            cols = slice(n * 256, n * 256 + 256)
            if half == 0:
                psend[:, cols] = part_sum.astype(bf16)
            else:
                acc[pl.ds(start, 512), cols] = part_sum

        if half == 0:
            send_sums[0].start()

    def block_first():
        send_sums[0].wait_recv()
        send_square.wait_recv()
        send_rows[0].wait_send()

        @pl.loop(0, 512, step=64)
        def _(r):
            at = pl.ds(pl.multiple_of(r, 64), 64)
            there = pl.ds(pl.multiple_of(mine + r, 64), 64)
            squares = square[there, :1] + sqrecv[at, :1]
            summed = (acc[there, :] + precv[at, :].astype(f32)) * lax.rsqrt(squares / 1024 + epsilon)
            first = (tok[at, :].astype(f32) + summed).astype(bf16)
            tok[at, :] = first
            rows[there, :] = normed(first.astype(f32), ffn_gain)

        send_rows[1].start()

    def block_gu(k):
        if "rows2" not in seen:
            seen.add("rows2")
            recv_rows[1].wait_recv()
        cols = slice(128 * k, 128 * k + 128)

        def body(i, before):
            at = pl.ds(i * ROWS, ROWS)
            weight = gu[k].reshape(2048, 256)
            pre = (jnp.dot(rows[at, :], weight, preferred_element_type=f32) * sv_gu[k]).astype(bf16).astype(f32)
            one, two = shifted(pre, before)
            acts = []
            for j, (taps, bias) in enumerate(((gate_taps, gate_bias), (up_taps, up_bias))):
                half, t = slice(128 * j, 128 * j + 128), taps[:, cols]
                acts.append(t[0:1] * two[:, half] + t[1:2] * one[:, half] + t[2:3] * pre[:, half] + bias[cols].reshape(1, 128))
            hidden[at, cols] = (acts[0] / (1.0 + jnp.exp(-acts[0])) * acts[1]).astype(bf16)
            return pre[-8:]

        before = jnp.zeros((8, 256), f32)
        for i in range(1024 // ROWS):
            before = body(i, before)

    def block_down(j):
        first, count = DOWN[j]
        width = sum(WHERE[CHUNK_OF["dn", u]][2] for u in range(first, first + count))
        lanes = slice(UNIT * first, UNIT * first + width)

        def product(start, count, n):
            weight = dn[n // 4, n % 4, :, :, lanes].reshape(256, width)
            return dot_nt(hidden[pl.ds(start, count), lanes], weight)

        def sweep(start, count, store):
            for n in range(8):
                store(n, slice(n * 256, n * 256 + 256), pl.ds(start, count), product(start, count, n))

        if j < len(DOWN) - 1:

            def store(n, cols, at, value):
                acc[at, cols] = value if j == 0 else acc[at, cols] + value

            sweep(0, 1024, store)
            return
        send_sums[0].wait_send()

        def give(n, cols, at, value):
            psend[:, cols] = ((acc[at, cols] + value) * sv_dn[n]).astype(bf16)

        sweep(yours, 512, give)
        send_sums[1].start()

        def keep(n, cols, at, value):
            acc[at, cols] = (acc[at, cols] + value) * sv_dn[n]

        sweep(mine, 512, keep)

    def block_last():
        send_sums[1].wait_recv()
        for q in range(4):

            @pl.loop(0, 128, step=64)
            def _(r):
                at = pl.ds(pl.multiple_of(q * 128 + r, 64), 64)
                there = pl.ds(pl.multiple_of(mine + q * 128 + r, 64), 64)
                summed = acc[there, :] + precv[at, :].astype(f32)
                out[at, :] = (tok[at, :].astype(f32) + summed).astype(bf16)

    blocks = {
        "cast": block_cast,
        "norm": block_norm, "scales": block_scales, "mix": block_mix, "conv": block_conv, "proj": block_proj,
        "first": block_first, "gu": block_gu, "down": block_down, "last": block_last,
    }
    for op in ops:
        if op[0] == "send":
            copy_of(op[1], op[2], False).start()
        elif op[0] == "wait":
            copy_of(op[1], op[2], True).wait_recv()
        else:
            name, *index = names[op[1]]
            blocks[name](*index)
    for c, (kind, turn, _) in enumerate(CHUNKS):
        for m in range(len(TREES[kind])):
            copy_of(c, m, False).wait_send()
    send_square.wait_send()
    send_rows[1].wait_send()
    send_sums[1].wait_send()


def mega(*args):
    names, comps, own_after = list_of_blocks()
    ops, _, _, _ = plan(CHUNKS, comps, own_after)
    f32, bf16 = jnp.float32, jnp.bfloat16
    hbm, vmem = pl.BlockSpec(memory_space=pl.ANY), pl.BlockSpec(memory_space=pltpu.VMEM)
    dma = pltpu.SemaphoreType.DMA
    return pl.pallas_call(
        lambda *refs: mega_kernel(ops, names, *refs),
        out_shape=pltpu.VMEM((512, 2048), bf16),
        in_specs=[hbm] * 8 + [vmem] * 15,
        out_specs=vmem,
        scratch_shapes=[
            pltpu.VMEM((6, 2, 4, 4, 64, 256), bf16),
            pltpu.VMEM((2, 4, 4, 64, 512), bf16),
            pltpu.VMEM((11, 2, 4, 4, 64, 256), bf16),
            pltpu.VMEM((2, 4, 4, 64, 1408), bf16),
            pltpu.VMEM((2, 4, 4, 8, 128), f32),
            pltpu.VMEM((512, 2048), bf16),
            pltpu.VMEM((1024, 2048), bf16),
            pltpu.VMEM((6, 1024, 256), bf16),
            pltpu.VMEM((1024, 512), bf16),
            pltpu.VMEM((1024, 128), f32),
            pltpu.VMEM((1024, 2048), f32),
            pltpu.VMEM((1024, 1408), bf16),
            pltpu.VMEM((512, 2048), bf16),
            pltpu.VMEM((512, 2048), bf16),
            pltpu.VMEM((512, 128), f32),
            pltpu.VMEM((6, 1, 256), f32),
            pltpu.VMEM((11, 1, 256), f32),
            pltpu.VMEM((8, 1, 256), f32),
            pltpu.VMEM((8, 1, 256), f32),
            dma((8,)),
            dma((len(CHUNKS),)),
            dma((len(CHUNKS), 10)),
            dma((5,)),
            dma((5,)),
        ],
        compiler_params=pltpu.CompilerParams(collective_id=0, has_side_effects=True, vmem_limit_bytes=58 * 1024 * 1024),
    )(*args)


def to_hbm(values):
    def kernel(src, dst, sem):
        copies = [
            pltpu.make_async_copy(src.at[128 * q : 128 * q + 128], dst.at[128 * q : 128 * q + 128], sem.at[q])
            for q in range(4)
        ]
        for copy in copies:
            copy.start()
        for copy in copies:
            copy.wait()

    return pl.pallas_call(
        kernel,
        out_shape=jax.ShapeDtypeStruct(values.shape, values.dtype),
        in_specs=[pl.BlockSpec(memory_space=pltpu.VMEM)],
        out_specs=pl.BlockSpec(memory_space=pl.ANY),
        scratch_shapes=[pltpu.SemaphoreType.DMA((4,))],
        compiler_params=pltpu.CompilerParams(vmem_limit_bytes=4 * 1024 * 1024),
    )(values)


def local(
    tokens, mix_gain, out_gate_w, in_gate_w, value_w, out_gate_scale, in_gate_scale, value_scale, mix_taps, conv_gain,
    out_proj_w, proj_scale, ffn_gain, gate_w, up_w, gate_scale, up_scale, gate_taps, up_taps, gate_bias, up_bias, down_w,
    down_scale,
):
    return to_hbm(mega(
        tokens[0], in_gate_w, value_w, out_gate_w, gate_w, up_w, out_proj_w.T, down_w.T, in_gate_scale, value_scale,
        out_gate_scale, gate_scale, up_scale, proj_scale, down_scale, mix_gain, ffn_gain, mix_taps, conv_gain, gate_taps,
        up_taps, gate_bias, up_bias,
    ))[None]


def solution(mesh):
    placed = (
        P(("rep", "fs"), "tp", None), P(), P("fs", "tp"), P("fs", "tp"), P("fs", "tp"), P(("tp", "fs")), P(("tp", "fs")),
        P(("tp", "fs")), P(None, "tp"), P("tp"), P("tp", "fs"), P("fs"), P(), P("fs", "tp"), P("fs", "tp"), P(("tp", "fs")),
        P(("tp", "fs")), P(None, "tp"), P(None, "tp"), P("tp"), P("tp"), P("tp", "fs"), P("fs"),
    )
    return jax.shard_map(
        local, mesh=mesh, in_specs=placed, out_specs=P(("rep", "fs"), "tp", None), check_vma=False
    )
```

```python
import jax
import jax.numpy as jnp
from jax import lax
from jax.experimental import pallas as pl
from jax.experimental.pallas import tpu as pltpu
from jax.sharding import PartitionSpec as P

epsilon = 1e-06
MESH = pl.DeviceIdType.MESH
UNIT = 256
TURNED = "so"

TREES = {
    "A": (
        ((), "x+", 1),
        ((), "x-", 1),
        ("s01", "xs", 1),
        ((0, 1, 2), "y+", 4),
        ((0, 1, 2), "y-", 4),
        ((0, 1, 2), "zs", 4),
        ("s34", "ys", 4),
        ("s34", "zo", 4),
        ("o34", "zo", 4),
        ((6,), "zs", 4),
    ),
    "D": (
        ((), "zs", 1),
        ((0,), "y+", 2),
        ((0,), "y-", 2),
        ("s12", "ys", 2),
        ((1, 2, 3), "x+", 8),
        ((1, 2, 3), "x-", 8),
        ((4,), "x+", 4),
        ((5,), "x-", 4),
    ),
    "C": (
        ((), "zs", 1),
        ((0,), "x+", 2),
        ((0,), "x-", 2),
        ("s12", "xs", 2),
        ((1, 2, 3), "y+", 8),
        ((1, 2, 3), "y-", 8),
        ((4,), "y+", 4),
        ((5,), "y-", 4),
    ),
}


def needs_of(kind, m, turn):
    need = TREES[kind][m][0]
    if isinstance(need, str):
        first, second = int(need[1]), int(need[2])
        return (first if (turn > 0) == (need[0] == "s") else second,)
    return need


def link_of(kind, m, turn):
    name = TREES[kind][m][1]
    sign = {"+": 1, "-": -1, "s": turn, "o": -turn}[name[1]]
    return name[0], sign


RATE, HOP, AHEAD = 46.0, 2.2, 2.5
ORDER = (
    ("mix", 5, "A", 1),
    ("gu", 10, "D", 1),
    ("mix", 0, "A", -1),
    ("mix", 2, "A", 1),
    ("mix", 1, "D", 1),
    ("mix", 4, "D", -1),
    ("gu", 8, "A", -1),
    ("pj", 1, "D", -1),
    ("mix", 3, "A", 1),
    ("pj", 0, "A", 1),
    ("gu", 6, "A", 1),
    ("gu", 2, "A", -1),
    ("gu", 3, "A", -1),
    ("dn", 0, "D", -1),
    ("gu", 1, "D", 1),
    ("gu", 0, "A", 1),
    ("dn", 1, "A", -1),
    ("gu", 4, "D", 1),
    ("gu", 9, "A", 1),
    ("gu", 5, "A", -1),
    ("gu", 7, "D", 1),
    ("dn", 3, "A", 1),
    ("dn", 4, "A", -1),
    ("dn", 2, "D", -1),
    ("dn", 5, "A", 1),
)
LEAD = {("A", 6): 1.0, ("C", 4): 12, ("D", 2): 0.5, ("D", 3): 9.0, ("D", 1): 6.0, ("D", 5): 3.5, ("D", 6): 10, ("A", 0): 0.5, ("D", 7): 8, ("D", 0): 4.0, ("A", 7): 1.5, ("C", 1): 5.0, ("A", 1): -3, ("A", 9): 3.0, ("A", 4): 1.0, ("A", 2): 9.0, ("A", 3): 0.5, ("C", 0): 1.5, ("D", 4): 6.0, ("C", 5): 9.5, ("C", 7): 8.0, ("C", 3): 1.5, ("A", 5): 1, ("C", 2): 8.0, ("A", 8): -0.5}


def plan(chunks, comps, own_after, rate=RATE, hop=HOP, issue=0.04, ahead=AHEAD):
    links = {(a, s): 0.0 for a in "xyz" for s in (1, -1)}
    arrive, waited, sent, ops, done, t = {}, set(), set(), [], {}, 0.0
    every = [(c, m) for c in range(len(chunks)) for m in range(len(TREES[chunks[c][0]]))]
    every.sort(key=lambda e: (e[0] - LEAD.get((chunks[e[0]][0], e[1]), 0.0), e[1]))
    log = []

    def wait(pairs):
        for pair in pairs:
            if pair not in waited:
                waited.add(pair)
                ops.append(("wait", *pair))

    while True:
        best = None
        for c, m in every:
            kind, turn, size = chunks[c]
            if (c, m) in sent:
                continue
            needs = [(c, k) for k in needs_of(kind, m, turn)]
            link = link_of(kind, m, turn)
            here = bool(needs) or c not in own_after or own_after[c] in done
            if here and all(arrive.get(k, 1e9) <= t for k in needs) and links[link] <= t + ahead:
                best = (c, m, needs, link, size * TREES[kind][m][2])
                break
        if best is not None:
            c, m, needs, link, size = best
            wait(needs)
            ops.append(("send", c, m))
            sent.add((c, m))
            t += issue
            links[link] = max(t, links[link]) + size / rate / 1000.0
            arrive[c, m] = links[link] + hop
            continue
        soon = []
        for k, (us, of_chunks, of_comps) in enumerate(comps):
            if k in done:
                continue
            pairs = [(c, m) for c, m in every if c in of_chunks]
            ready = max([arrive.get(q, 1e9) for q in pairs] + [done.get(b, 1e9) + lag for b, lag in of_comps] + [0.0])
            if ready <= t:
                wait(pairs)
                ops.append(("comp", k))
                log.append((round(t, 1), k))
                t += us
                done[k] = t
                break
            if ready < 1e8:
                soon.append(ready)
        else:
            later = [a for a in arrive.values() if a > t] + [b - ahead for b in links.values() if b - ahead > t] + soon
            if not later:
                break
            t = min(later) + 1e-6
    wait(every)
    return ops, t, log, arrive


def list_of_chunks():
    chunks, where = [("A", 1, 4096)], [("sc", 0, 128)]
    for name, i, kind, turn in ORDER:
        width = UNIT // 2 if (name, i) == LAST else UNIT
        chunks.append((kind, turn, 64 * width * 2))
        where.append((name, i, width))
    return chunks, where


LAST = ("dn", 5)
CHUNKS, WHERE = list_of_chunks()
CHUNK_OF = {(name, i): c for c, (name, i, _) in enumerate(WHERE)}
ROWS = 256
DOWN = ((0, 2), (2, 2), (4, 1))


def list_of_blocks():
    names, comps, number = [], [], {}

    def add(name, us, chunks=(), after=()):
        number[name] = len(names)
        names.append(name)
        comps.append((us, {CHUNK_OF[c] for c in chunks}, [(number[b], lag) for b, lag in after]))

    add(("cast", "gu"), 0.5)
    add(("cast", "rest"), 0.4)
    add(("norm",), 1.5)
    add(("scales",), 1.0, [("sc", 0)])
    for k in range(6):
        add(("mix", k), 1.05, [("mix", k)], [(("norm",), 4.0), (("scales",), 0.0)])
    for g in range(2):
        add(("conv", g), 1.0, [], [(("mix", 3 * g + i), 0.0) for i in range(3)] + [(("conv", 0), 0.0)] * g)
    add(("proj", 0), 0.8, [("pj", 0), ("pj", 1)], [(("conv", 0), 0.0), (("conv", 1), 0.0)])
    add(("proj", 1), 0.8, [], [(("proj", 0), 0.0)])
    add(("first",), 2.0, [], [(("proj", 1), 3.2)])
    for k in range(11):
        add(("gu", k), 1.45, [("gu", k)], [(("first",), 4.0)])
    for j, (first, count) in enumerate(DOWN):
        units = range(first, first + count)
        before = [(("gu", k), 0.0) for u in units for k in (2 * u, 2 * u + 1)] + [(("down", j - 1), 0.0)] * (j > 0)
        add(("down", j), 0.1 + 1.15 * count, [("dn", u) for u in units], before)
    add(("give",), 0.5, [], [(("down", len(DOWN) - 1), 0.0), (("gu", 10), 0.0)])
    add(("base",), 1.3, [], [(("give",), 4.2)])
    add(("final",), 2.2, [LAST], [(("base",), 0.0)])
    own_after = {}
    for (name, _), c in CHUNK_OF.items():
        if name in ("gu", "pj", "dn"):
            own_after[c] = number["cast", "gu" if name == "gu" else "rest"]
    return names, comps, own_after


def place():
    rep, fs = lax.axis_index("rep"), lax.axis_index("fs")
    tp = lax.axis_index("tp")
    x, y, zl = lax.rem(fs, 4), lax.rem(fs // 4, 4), fs // 16
    z = rep * 2 + zl
    xs = {n: lax.rem(x + 4 + n, 4) for n in (-1, 1, 2)} | {0: x}
    ys = {n: lax.rem(y + 4 + n, 4) for n in (-1, 1, 2)} | {0: y}
    near = {}
    for sign in (1, -1):
        near["x", sign] = (rep, zl * 16 + y * 4 + xs[sign], tp)
        near["y", sign] = (rep, zl * 16 + ys[sign] * 4 + x, tp)
        zn = lax.rem(z + 4 + sign, 4)
        near["z", sign] = (zn // 2, lax.rem(zn, 2) * 16 + y * 4 + x, tp)
    return xs, ys, {0: zl, 1: 1 - zl}, near, (rep, fs, 1 - tp), tp


def carried(kind, m, turn, arriving):
    sent = {
        "A": (
            (0, 0, 0),
            (0, 0, 0),
            (0, 0, -turn),
            (0, 0, None),
            (0, 0, None),
            (0, 0, None),
            (0, -turn, None),
            (0, -turn, None),
            (0, turn, None),
            (0, 2, None),
        ),
        "D": (
            (0, 0, 0),
            (None, 0, 0),
            (None, 0, 0),
            (None, -turn, 0),
            (None, None, 0),
            (None, None, 0),
            ("plane0", None, -1),
            ("plane1", None, 1),
        ),
        "C": (
            (0, 0, 0),
            (None, 0, 0),
            (None, 0, 0),
            (None, 0, -turn),
            (None, 0, None),
            (None, 0, None),
            ("plane0", -1, None),
            ("plane1", 1, None),
        ),
    }[kind][m]
    if not arriving:
        return sent
    link, sign = link_of(kind, m, turn)
    z, y, x = sent

    def back(v, n):
        v = v - n
        return v + 4 if v < -1 else v - 4 if v > 2 else v

    if link == "x":
        x = back(x, sign)
    elif link == "y":
        y = back(y, sign)
    else:
        z = 1 - z
    return z, y, x


def mega_kernel(
    ops, names, tokens, in_w, val_w, out_w, gate_w, up_w, pj_w, dn_w, in_s, val_s, out_s, gate_s, up_s, pj_s, dn_s, mix_gain,
    ffn_gain, mix_taps, conv_gain, gate_taps, up_taps, gate_bias, up_bias, out, mix, pj, gu, dn, sc, tok, rows, gates, conv, square, acc, hidden, psend, precv, sqrecv, sv_mix,
    sv_gu, sv_pj, sv_dn, hidden_other, dn_other, own_sem, send_sem, recv_sem, side_send, side_recv,
):
    f32, bf16 = jnp.float32, jnp.bfloat16
    xs, ys, zs, near, other, tp = place()
    bufs = {"mix": mix, "pj": pj, "gu": gu, "dn": dn, "sc": sc}
    x, y, zl = xs[0], ys[0], zs[0]
    mine = pl.multiple_of(tp * 512, 512)
    yours = pl.multiple_of((1 - tp) * 512, 512)
    mix_f32 = [acc.at[64 * i : 64 * i + 64, 0:512] for i in range(3)]
    gu_f32 = [acc.at[192 + 64 * i : 256 + 64 * i, 0:1408] for i in range(2)]
    pj_f32, dn_f32 = acc.at[320:384, 0:512], acc.at[384:448, 0:1408]
    own = [
        pltpu.make_async_copy(src, dst, own_sem.at[i])
        for i, (src, dst) in enumerate(
            zip(
                (in_w, val_w, out_w, gate_w, up_w, pj_w, dn_w, tokens),
                (*mix_f32, *gu_f32, pj_f32, dn_f32, tok),
            )
        )
    ]
    for copy in own:
        copy.start()
    barrier = pltpu.get_barrier_semaphore()
    for device in [*near.values(), other]:
        pl.semaphore_signal(barrier, inc=1, device_id=device, device_id_type=MESH)
    sc[zl, y, x] = jnp.zeros((8, 128), f32)
    for i, ref in enumerate((in_s, val_s, out_s, gate_s, up_s, pj_s, dn_s)):
        sc[zl, y, x, i : i + 1, : ref.shape[0]] = ref[...].reshape(1, -1)
    for i in range(3):
        own[i].wait()
        for g in range(2):
            mix[3 * g + i, zl, y, x] = mix_f32[i][:, 256 * g : 256 * g + 256].astype(bf16)
    pl.semaphore_wait(barrier, 7)

    def block_cast(which):
        if which == "gu":
            for i in range(2):
                own[3 + i].wait()
                for k in range(11):
                    gu[k, zl, y, x, :, 128 * i : 128 * i + 128] = gu_f32[i][:, 128 * k : 128 * k + 128].astype(bf16)
        else:
            own[5].wait()
            pj[zl, y, x] = pj_f32[...].astype(bf16)
            own[6].wait()
            dn[zl, y, x] = dn_f32[...].astype(bf16)
            pass_on((0, 0, 0), 10)

    def part(c, at):
        name, i, width = WHERE[c]
        z, y, x = at
        z = slice(None) if z is None else int(z[-1]) if isinstance(z, str) else zs[z]
        y = slice(None) if y is None else ys[y]
        x = slice(None) if x is None else xs[x]
        ref = bufs[name]
        if name in ("mix", "gu"):
            return ref.at[i, z, y, x]
        if name == "sc":
            return ref.at[z, y, x]
        return ref.at[z, y, x, :, i * UNIT : i * UNIT + width]

    def copy_of(c, m, arriving):
        kind, turn, _ = CHUNKS[c]
        ref = part(c, carried(kind, m, turn, arriving))
        return pltpu.make_async_remote_copy(
            src_ref=ref,
            dst_ref=ref,
            send_sem=send_sem.at[c],
            recv_sem=recv_sem.at[c, m],
            device_id=near[link_of(kind, m, turn)],
            device_id_type=MESH,
        )

    def to_other(src, dst, i):
        return pltpu.make_async_remote_copy(
            src_ref=src, dst_ref=dst, send_sem=side_send.at[i], recv_sem=side_recv.at[i], device_id=other, device_id_type=MESH
        )

    def normed(values, gain):
        return (values * lax.rsqrt(jnp.mean(values * values, axis=1, keepdims=True) + epsilon) * gain[...].reshape(1, -1)).astype(bf16)

    def shifted(values, before):
        both = jnp.concatenate([before, values], axis=0)
        return pltpu.roll(both, 1, 0)[8:], pltpu.roll(both, 2, 0)[8:]

    def dot_nt(left, right):
        return lax.dot_general(left, right, (((1,), (1,)), ((), ())), preferred_element_type=f32)

    def spread(row, width, group):
        total = jnp.zeros((1, 128), f32)
        lane = lax.broadcasted_iota(jnp.int32, (1, 128), 1)
        for s in range(group * 128 // width, min(31, (group * 128 + 127) // width) + 1):
            at = s * width - group * 128
            line = sc[s // 16, s // 4 % 4, s % 4, row : row + 1, :]
            if at % 128:
                line = pltpu.roll(line, at % 128, 1)
            total = jnp.where((lane >= at) & (lane < at + width), line, total)
        return total

    send_rows = [to_other(rows.at[pl.ds(mine, 512)], rows.at[pl.ds(mine, 512)], i) for i in (0, 3)]
    recv_rows = [to_other(rows.at[pl.ds(yours, 512)], rows.at[pl.ds(yours, 512)], i) for i in (0, 3)]
    send_sums = [to_other(psend, precv, i) for i in (1, 4)]
    send_square = to_other(square.at[pl.ds(yours, 512)], sqrecv, 2)
    last_lanes = slice(1280, 1408)
    send_hidden = to_other(hidden.at[pl.ds(yours, 512), last_lanes], hidden_other, 5)
    last_chunk = CHUNK_OF[LAST]
    arrived_last = []
    seen = set()

    def pass_on(at, i):
        z, y, x = at
        z = slice(None) if z is None else int(z[-1]) if isinstance(z, str) else zs[z]
        y = slice(None) if y is None else ys[y]
        x = slice(None) if x is None else xs[x]
        copy = to_other(part(last_chunk, at), dn_other.at[z, y, x], 6 + i)
        copy.start()
        arrived_last.append(copy)

    def block_norm():
        own[7].wait()

        @pl.loop(0, 512, step=64)
        def _(r):
            at = pl.multiple_of(r, 64)
            rows[pl.ds(mine + at, 64), :] = normed(tok[pl.ds(at, 64), :].astype(f32), mix_gain)

        send_rows[0].start()

    def block_scales():
        for k in range(6):
            for i in range(2):
                sv_mix[k, :, 128 * i : 128 * i + 128] = spread(k % 3, 16, k // 3 * 2 + i)
        for k in range(11):
            sv_gu[k, :, :128] = spread(3, 44, k)
            sv_gu[k, :, 128:] = spread(4, 44, k)
        for k in range(16):
            sv_pj[k // 2, :, 128 * (k % 2) : 128 * (k % 2) + 128] = spread(5, 64, k)
            sv_dn[k // 2, :, 128 * (k % 2) : 128 * (k % 2) + 128] = spread(6, 64, k)

    def block_mix(k):
        if "rows" not in seen:
            seen.add("rows")
            recv_rows[0].wait_recv()

        for r in range(0, 1024, ROWS):
            at = pl.ds(r, ROWS)
            weight = mix[k].reshape(2048, 256)
            gates[k, at, :] = (jnp.dot(rows[at, :], weight, preferred_element_type=f32) * sv_mix[k]).astype(bf16)

    def block_conv(g):
        cols = slice(256 * g, 256 * g + 256)
        taps, gain = mix_taps[:, cols], conv_gain[cols].reshape(1, 256)

        def body(i, before):
            at = pl.ds(pl.multiple_of(i * 128, 128), 128)
            value = gates[3 * g, at, :].astype(f32) * gates[3 * g + 1, at, :].astype(f32)
            one, two = shifted(value, before)
            total = taps[0:1] * two + taps[1:2] * one + taps[2:3] * value
            done = (gates[3 * g + 2, at, :].astype(f32) * total).astype(bf16).astype(f32)
            conv[at, cols] = (done * gain).astype(bf16)
            squares = jnp.broadcast_to(jnp.sum(done * done, axis=1, keepdims=True), (128, 128))
            square[at, :] = squares if g == 0 else square[at, :] + squares
            return value[-8:]

        lax.fori_loop(0, 8, body, jnp.zeros((8, 256), f32))
        if g == 1:
            send_square.start()

    def block_proj(half):
        start = yours if half == 0 else mine

        for n in range(8):
            weight = pj[n // 4, n % 4].reshape(256, 512)
            part_sum = dot_nt(conv[pl.ds(start, 512), :], weight) * sv_pj[n]
            cols = slice(n * 256, n * 256 + 256)
            if half == 0:
                psend[:, cols] = part_sum.astype(bf16)
            else:
                acc[pl.ds(start, 512), cols] = part_sum

        if half == 0:
            send_sums[0].start()

    def block_first():
        send_sums[0].wait_recv()
        send_square.wait_recv()
        send_rows[0].wait_send()

        @pl.loop(0, 512, step=64)
        def _(r):
            at = pl.ds(pl.multiple_of(r, 64), 64)
            there = pl.ds(pl.multiple_of(mine + r, 64), 64)
            squares = square[there, :1] + sqrecv[at, :1]
            summed = (acc[there, :] + precv[at, :].astype(f32)) * lax.rsqrt(squares / 1024 + epsilon)
            first = (tok[at, :].astype(f32) + summed).astype(bf16)
            tok[at, :] = first
            rows[there, :] = normed(first.astype(f32), ffn_gain)

        send_rows[1].start()

    def block_gu(k):
        if "rows2" not in seen:
            seen.add("rows2")
            recv_rows[1].wait_recv()
        cols = slice(128 * k, 128 * k + 128)

        def body(i, before):
            at = pl.ds(i * ROWS, ROWS)
            weight = gu[k].reshape(2048, 256)
            pre = (jnp.dot(rows[at, :], weight, preferred_element_type=f32) * sv_gu[k]).astype(bf16).astype(f32)
            one, two = shifted(pre, before)
            acts = []
            for j, (taps, bias) in enumerate(((gate_taps, gate_bias), (up_taps, up_bias))):
                half, t = slice(128 * j, 128 * j + 128), taps[:, cols]
                acts.append(t[0:1] * two[:, half] + t[1:2] * one[:, half] + t[2:3] * pre[:, half] + bias[cols].reshape(1, 128))
            hidden[at, cols] = (acts[0] / (1.0 + jnp.exp(-acts[0])) * acts[1]).astype(bf16)
            return pre[-8:]

        before = jnp.zeros((8, 256), f32)
        for i in range(1024 // ROWS):
            before = body(i, before)
        if k == 10:
            send_hidden.start()

    def block_down(j):
        first, count = DOWN[j]
        width = sum(WHERE[CHUNK_OF["dn", u]][2] for u in range(first, first + count))
        lanes = slice(UNIT * first, UNIT * first + width)

        def product(start, count, n):
            weight = dn[n // 4, n % 4, :, :, lanes].reshape(256, width)
            return dot_nt(hidden[pl.ds(start, count), lanes], weight)

        def sweep(start, count, store):
            for n in range(8):
                store(n, slice(n * 256, n * 256 + 256), pl.ds(start, count), product(start, count, n))

        def store(n, cols, at, value):
            acc[at, cols] = value if j == 0 else acc[at, cols] + value

        sweep(0, 1024, store)


    def block_give():
        send_sums[0].wait_send()

        @pl.loop(0, 512, step=64)
        def _(r):
            at, there = pl.ds(pl.multiple_of(r, 64), 64), pl.ds(pl.multiple_of(yours + r, 64), 64)
            for n in range(8):
                cols = slice(256 * n, 256 * n + 256)
                psend[at, cols] = (acc[there, cols] * sv_dn[n]).astype(bf16)

        send_sums[1].start()

    def block_base():
        send_sums[1].wait_recv()

        @pl.loop(0, 512, step=64)
        def _(r):
            at, there = pl.ds(pl.multiple_of(r, 64), 64), pl.ds(pl.multiple_of(mine + r, 64), 64)
            for n in range(8):
                cols = slice(256 * n, 256 * n + 256)
                summed = acc[there, cols] * sv_dn[n] + precv[at, cols].astype(f32)
                acc[there, cols] = tok[at, cols].astype(f32) + summed

    def block_final():
        send_hidden.wait_recv()
        for copy in arrived_last:
            copy.wait_recv()
        at = pl.ds(mine, 512)
        left = jnp.concatenate([hidden[at, last_lanes], hidden_other[...]], axis=1)
        for n in range(8):
            cols = slice(256 * n, 256 * n + 256)
            weights = [dn[n // 4, n % 4, :, :, last_lanes].reshape(256, 128), dn_other[n // 4, n % 4].reshape(256, 128)]
            value = dot_nt(left, jnp.concatenate(weights, axis=1)) * sv_dn[n]
            out[:, cols] = (acc[at, cols] + value).astype(bf16)

    blocks = {
        "cast": block_cast,
        "norm": block_norm, "scales": block_scales, "mix": block_mix, "conv": block_conv, "proj": block_proj,
        "first": block_first, "gu": block_gu, "down": block_down, "give": block_give, "base": block_base,
        "final": block_final,
    }
    gone = set()

    def sent_by(end):
        for c, (kind, _, _) in enumerate(CHUNKS):
            entries = range(len(TREES[kind]))
            if c not in gone and all(("send", c, m) in ops[:end] for m in entries):
                gone.add(c)
                for m in entries:
                    copy_of(c, m, False).wait_send()

    for step, op in enumerate(ops):
        if op[0] == "send":
            copy_of(op[1], op[2], False).start()
        elif op[0] == "wait":
            copy_of(op[1], op[2], True).wait_recv()
            if op[1] == last_chunk:
                pass_on(carried(*CHUNKS[last_chunk][:1], op[2], CHUNKS[last_chunk][1], True), op[2])
        else:
            name, *index = names[op[1]]
            if name == "base":
                sent_by(step - 30)
            blocks[name](*index)
    sent_by(len(ops))
    send_square.wait_send()
    send_rows[1].wait_send()
    send_sums[1].wait_send()
    send_hidden.wait_send()
    for copy in arrived_last:
        copy.wait_send()


def mega(*args):
    names, comps, own_after = list_of_blocks()
    ops, _, _, _ = plan(CHUNKS, comps, own_after)
    f32, bf16 = jnp.float32, jnp.bfloat16
    hbm, vmem = pl.BlockSpec(memory_space=pl.ANY), pl.BlockSpec(memory_space=pltpu.VMEM)
    dma = pltpu.SemaphoreType.DMA
    return pl.pallas_call(
        lambda *refs: mega_kernel(ops, names, *refs),
        out_shape=pltpu.VMEM((512, 2048), bf16),
        in_specs=[hbm] * 8 + [vmem] * 15,
        out_specs=vmem,
        scratch_shapes=[
            pltpu.VMEM((6, 2, 4, 4, 64, 256), bf16),
            pltpu.VMEM((2, 4, 4, 64, 512), bf16),
            pltpu.VMEM((11, 2, 4, 4, 64, 256), bf16),
            pltpu.VMEM((2, 4, 4, 64, 1408), bf16),
            pltpu.VMEM((2, 4, 4, 8, 128), f32),
            pltpu.VMEM((512, 2048), bf16),
            pltpu.VMEM((1024, 2048), bf16),
            pltpu.VMEM((6, 1024, 256), bf16),
            pltpu.VMEM((1024, 512), bf16),
            pltpu.VMEM((1024, 128), f32),
            pltpu.VMEM((1024, 2048), f32),
            pltpu.VMEM((1024, 1408), bf16),
            pltpu.VMEM((512, 2048), bf16),
            pltpu.VMEM((512, 2048), bf16),
            pltpu.VMEM((512, 128), f32),
            pltpu.VMEM((6, 1, 256), f32),
            pltpu.VMEM((11, 1, 256), f32),
            pltpu.VMEM((8, 1, 256), f32),
            pltpu.VMEM((8, 1, 256), f32),
            pltpu.VMEM((512, 128), bf16),
            pltpu.VMEM((2, 4, 4, 64, 128), bf16),
            dma((8,)),
            dma((len(CHUNKS),)),
            dma((len(CHUNKS), 10)),
            dma((17,)),
            dma((17,)),
        ],
        compiler_params=pltpu.CompilerParams(collective_id=0, has_side_effects=True, vmem_limit_bytes=58 * 1024 * 1024),
    )(*args)


def to_hbm(values):
    def kernel(src, dst, sem):
        copies = [
            pltpu.make_async_copy(src.at[128 * q : 128 * q + 128], dst.at[128 * q : 128 * q + 128], sem.at[q])
            for q in range(4)
        ]
        for copy in copies:
            copy.start()
        for copy in copies:
            copy.wait()

    return pl.pallas_call(
        kernel,
        out_shape=jax.ShapeDtypeStruct(values.shape, values.dtype),
        in_specs=[pl.BlockSpec(memory_space=pltpu.VMEM)],
        out_specs=pl.BlockSpec(memory_space=pl.ANY),
        scratch_shapes=[pltpu.SemaphoreType.DMA((4,))],
        compiler_params=pltpu.CompilerParams(vmem_limit_bytes=4 * 1024 * 1024),
    )(values)


def local(
    tokens, mix_gain, out_gate_w, in_gate_w, value_w, out_gate_scale, in_gate_scale, value_scale, mix_taps, conv_gain,
    out_proj_w, proj_scale, ffn_gain, gate_w, up_w, gate_scale, up_scale, gate_taps, up_taps, gate_bias, up_bias, down_w,
    down_scale,
):
    return to_hbm(mega(
        tokens[0], in_gate_w, value_w, out_gate_w, gate_w, up_w, out_proj_w.T, down_w.T, in_gate_scale, value_scale,
        out_gate_scale, gate_scale, up_scale, proj_scale, down_scale, mix_gain, ffn_gain, mix_taps, conv_gain, gate_taps,
        up_taps, gate_bias, up_bias,
    ))[None]


def solution(mesh):
    placed = (
        P(("rep", "fs"), "tp", None), P(), P("fs", "tp"), P("fs", "tp"), P("fs", "tp"), P(("tp", "fs")), P(("tp", "fs")),
        P(("tp", "fs")), P(None, "tp"), P("tp"), P("tp", "fs"), P("fs"), P(), P("fs", "tp"), P("fs", "tp"), P(("tp", "fs")),
        P(("tp", "fs")), P(None, "tp"), P(None, "tp"), P("tp"), P("tp"), P("tp", "fs"), P("fs"),
    )
    return jax.shard_map(
        local, mesh=mesh, in_specs=placed, out_specs=P(("rep", "fs"), "tp", None), check_vma=False
    )
```

```python
import jax
import jax.numpy as jnp
from jax import lax
from jax.experimental import pallas as pl
from jax.experimental.pallas import tpu as pltpu
from jax.sharding import PartitionSpec as P

epsilon = 1e-06
MESH = pl.DeviceIdType.MESH
UNIT = 256
TURNED = "so"

TREES = {
    "A": (
        ((), "x+", 1),
        ((), "x-", 1),
        ("s01", "xs", 1),
        ((0, 1, 2), "y+", 4),
        ((0, 1, 2), "y-", 4),
        ((0, 1, 2), "zs", 4),
        ("s34", "ys", 4),
        ("s34", "zo", 4),
        ("o34", "zo", 4),
        ((6,), "zs", 4),
    ),
    "D": (
        ((), "zs", 1),
        ((0,), "y+", 2),
        ((0,), "y-", 2),
        ("s12", "ys", 2),
        ((1, 2, 3), "x+", 8),
        ((1, 2, 3), "x-", 8),
        ((4,), "x+", 4),
        ((5,), "x-", 4),
    ),
    "E": (
        ((), "x+", 1),
        ((), "x-", 1),
        ("s01", "xs", 1),
        ((0, 1, 2), "y+", 4),
        ((0, 1, 2), "y-", 4),
        ((), "zs", 1),
        ((0,), "zs", 1),
        ((1,), "zs", 1),
        ((2,), "zs", 1),
        ("s34", "ys", 4),
        ("s34", "zo", 4),
        ("o34", "zo", 4),
        ((9,), "zs", 4),
    ),
    "C": (
        ((), "zs", 1),
        ((0,), "x+", 2),
        ((0,), "x-", 2),
        ("s12", "xs", 2),
        ((1, 2, 3), "y+", 8),
        ((1, 2, 3), "y-", 8),
        ((4,), "y+", 4),
        ((5,), "y-", 4),
    ),
}


def needs_of(kind, m, turn):
    need = TREES[kind][m][0]
    if isinstance(need, str):
        first, second = int(need[1]), int(need[2])
        return (first if (turn > 0) == (need[0] == "s") else second,)
    return need


def link_of(kind, m, turn):
    name = TREES[kind][m][1]
    sign = {"+": 1, "-": -1, "s": turn, "o": -turn}[name[1]]
    return name[0], sign


RATE, HOP, AHEAD = 46.0, 2.2, 3
ORDER = (
    ("mix", 0, "A", 1),
    ("mix", 2, "D", 1),
    ("mix", 3, "E", 1),
    ("mix", 5, "A", -1),
    ("mix", 1, "E", -1),
    ("gu", 1, "D", -1),
    ("pj", 0, "D", -1),
    ("mix", 4, "D", 1),
    ("gu", 2, "E", 1),
    ("gu", 8, "A", -1),
    ("pj", 1, "A", -1),
    ("gu", 7, "D", 1),
    ("dn", 3, "A", 1),
    ("gu", 0, "A", -1),
    ("gu", 4, "D", 1),
    ("gu", 3, "E", 1),
    ("gu", 9, "D", -1),
    ("dn", 0, "D", 1),
    ("dn", 1, "A", -1),
    ("gu", 5, "A", -1),
    ("gu", 6, "A", -1),
    ("dn", 2, "E", 1),
    ("dn", 5, "D", -1),
    ("gu", 10, "D", 1),
    ("dn", 4, "A", -1),
)
LEAD = {("A", 6): 12, ("C", 4): 9, ("D", 2): 1.0, ("D", 3): 7.5, ("D", 1): 12, ("D", 5): 1.0, ("D", 6): 1.5, ("D", 7): 9.5, ("D", 0): 12, ("A", 7): 1.5, ("C", 1): 5.5, ("C", 6): 4.0, ("A", 1): 2.0, ("A", 9): 12, ("A", 4): 3.5, ("A", 2): 7.0, ("A", 3): 0.5, ("C", 0): 8.5, ("D", 4): -3, ("C", 5): 6, ("C", 7): 4.5, ("C", 3): 9, ("A", 5): 11.5, ("C", 2): 2.5, ("A", 8): 10, ("E", 7): 11.5, ("E", 10): 7.5, ("E", 8): 1, ("E", 0): -3, ("E", 2): -0.5, ("E", 9): -1.5, ("E", 3): 7.5, ("E", 5): 4.5, ("E", 4): -2.0, ("E", 1): -3, ("E", 12): 10, ("E", 6): 9.0}


def plan(chunks, comps, own_after, rate=RATE, hop=HOP, issue=0.04, ahead=AHEAD):
    links = {(a, s): 0.0 for a in "xyz" for s in (1, -1)}
    arrive, waited, sent, ops, done, t = {}, set(), set(), [], {}, 0.0
    every = [(c, m) for c in range(len(chunks)) for m in range(len(TREES[chunks[c][0]]))]
    every.sort(key=lambda e: (e[0] - LEAD.get((chunks[e[0]][0], e[1]), 0.0), e[1]))
    log = []

    def wait(pairs):
        for pair in pairs:
            if pair not in waited:
                waited.add(pair)
                ops.append(("wait", *pair))

    while True:
        best = None
        for c, m in every:
            kind, turn, size = chunks[c]
            if (c, m) in sent:
                continue
            needs = [(c, k) for k in needs_of(kind, m, turn)]
            link = link_of(kind, m, turn)
            here = bool(needs) or c not in own_after or own_after[c] in done
            if here and all(arrive.get(k, 1e9) <= t for k in needs) and links[link] <= t + ahead:
                best = (c, m, needs, link, size * TREES[kind][m][2])
                break
        if best is not None:
            c, m, needs, link, size = best
            wait(needs)
            ops.append(("send", c, m))
            sent.add((c, m))
            t += issue
            links[link] = max(t, links[link]) + size / rate / 1000.0
            arrive[c, m] = links[link] + hop
            continue
        soon = []
        for k, (us, of_chunks, of_comps) in enumerate(comps):
            if k in done:
                continue
            pairs = [(c, m) for c, m in every if c in of_chunks]
            ready = max([arrive.get(q, 1e9) for q in pairs] + [done.get(b, 1e9) + lag for b, lag in of_comps] + [0.0])
            if ready <= t:
                wait(pairs)
                ops.append(("comp", k))
                log.append((round(t, 1), k))
                t += us
                done[k] = t
                break
            if ready < 1e8:
                soon.append(ready)
        else:
            later = [a for a in arrive.values() if a > t] + [b - ahead for b in links.values() if b - ahead > t] + soon
            if not later:
                break
            t = min(later) + 1e-6
    wait(every)
    return ops, t, log, arrive


def list_of_chunks():
    chunks, where = [("A", 1, 4096)], [("sc", 0, 128)]
    for name, i, kind, turn in ORDER:
        width = UNIT // 2 if (name, i) == LAST else UNIT
        chunks.append((kind, turn, 64 * width * 2))
        where.append((name, i, width))
    return chunks, where


LAST = ("dn", 5)
CHUNKS, WHERE = list_of_chunks()
CHUNK_OF = {(name, i): c for c, (name, i, _) in enumerate(WHERE)}
ROWS = 256
DOWN = ((0, 2), (2, 2))
PASSED = 4


def list_of_blocks():
    names, comps, number = [], [], {}

    def add(name, us, chunks=(), after=()):
        number[name] = len(names)
        names.append(name)
        comps.append((us, {CHUNK_OF[c] for c in chunks}, [(number[b], lag) for b, lag in after]))

    add(("cast", "gu"), 0.5)
    add(("cast", "rest"), 0.4)
    add(("norm",), 1.5)
    add(("scales",), 1.0, [("sc", 0)])
    for k in range(6):
        add(("mix", k), 1.05, [("mix", k)], [(("norm",), 4.0), (("scales",), 0.0)])
    for g in range(2):
        add(("conv", g), 1.0, [], [(("mix", 3 * g + i), 0.0) for i in range(3)] + [(("conv", 0), 0.0)] * g)
    add(("proj", 0), 0.8, [("pj", 0), ("pj", 1)], [(("conv", 0), 0.0), (("conv", 1), 0.0)])
    add(("proj", 1), 0.8, [], [(("proj", 0), 0.0)])
    add(("first",), 2.0, [], [(("proj", 1), 3.2)])
    for k in range(11):
        add(("gu", k), 1.45, [("gu", k)], [(("first",), 4.0)])
    for j, (first, count) in enumerate(DOWN):
        units = range(first, first + count)
        before = [(("gu", k), 0.0) for u in units for k in (2 * u, 2 * u + 1)] + [(("down", j - 1), 0.0)] * (j > 0)
        add(("down", j), 0.1 + 1.15 * count, [("dn", u) for u in units], before)
    add(("give",), 0.5, [], [(("down", len(DOWN) - 1), 0.0)])
    add(("base",), 1.3, [], [(("give",), 4.2)])
    add(("near", 4), 1.3, [("dn", 4)], [(("base",), 0.0), (("gu", 8), 2.0), (("gu", 9), 2.0)])
    add(("near", 5), 1.5, [("dn", 5)], [(("near", 4), 0.0), (("gu", 10), 2.0)])
    own_after = {}
    for (name, _), c in CHUNK_OF.items():
        if name in ("gu", "pj", "dn"):
            own_after[c] = number["cast", "gu" if name == "gu" else "rest"]
    return names, comps, own_after


def place():
    rep, fs = lax.axis_index("rep"), lax.axis_index("fs")
    tp = lax.axis_index("tp")
    x, y, zl = lax.rem(fs, 4), lax.rem(fs // 4, 4), fs // 16
    z = rep * 2 + zl
    xs = {n: lax.rem(x + 4 + n, 4) for n in (-1, 1, 2)} | {0: x}
    ys = {n: lax.rem(y + 4 + n, 4) for n in (-1, 1, 2)} | {0: y}
    near = {}
    for sign in (1, -1):
        near["x", sign] = (rep, zl * 16 + y * 4 + xs[sign], tp)
        near["y", sign] = (rep, zl * 16 + ys[sign] * 4 + x, tp)
        zn = lax.rem(z + 4 + sign, 4)
        near["z", sign] = (zn // 2, lax.rem(zn, 2) * 16 + y * 4 + x, tp)
    return xs, ys, {0: zl, 1: 1 - zl}, near, (rep, fs, 1 - tp), tp


def carried(kind, m, turn, arriving):
    sent = {
        "A": (
            (0, 0, 0),
            (0, 0, 0),
            (0, 0, -turn),
            (0, 0, None),
            (0, 0, None),
            (0, 0, None),
            (0, -turn, None),
            (0, -turn, None),
            (0, turn, None),
            (0, 2, None),
        ),
        "D": (
            (0, 0, 0),
            (None, 0, 0),
            (None, 0, 0),
            (None, -turn, 0),
            (None, None, 0),
            (None, None, 0),
            ("plane0", None, -1),
            ("plane1", None, 1),
        ),
        "E": (
            (0, 0, 0),
            (0, 0, 0),
            (0, 0, -turn),
            (0, 0, None),
            (0, 0, None),
            (0, 0, 0),
            (0, 0, -1),
            (0, 0, 1),
            (0, 0, 2),
            (0, -turn, None),
            (0, -turn, None),
            (0, turn, None),
            (0, 2, None),
        ),
        "C": (
            (0, 0, 0),
            (None, 0, 0),
            (None, 0, 0),
            (None, 0, -turn),
            (None, 0, None),
            (None, 0, None),
            ("plane0", -1, None),
            ("plane1", 1, None),
        ),
    }[kind][m]
    if not arriving:
        return sent
    link, sign = link_of(kind, m, turn)
    z, y, x = sent

    def back(v, n):
        v = v - n
        return v + 4 if v < -1 else v - 4 if v > 2 else v

    if link == "x":
        x = back(x, sign)
    elif link == "y":
        y = back(y, sign)
    else:
        z = 1 - z
    return z, y, x


def mega_kernel(
    ops, names, tokens, in_w, val_w, out_w, gate_w, up_w, pj_w, dn_w, *rest,
):
    small_in, out, small = rest[:15], rest[15], rest[16:31]
    run_kernel(ops, names, tokens, in_w, val_w, out_w, gate_w, up_w, pj_w, dn_w, small_in, small, out, *rest[31:])


def run_kernel(
    ops, names, tokens, in_w, val_w, out_w, gate_w, up_w, pj_w, dn_w, small_in, small, out, mix, pj, gu, dn, sc, tok, rows, gates, conv, square, acc, hidden, psend, precv, sqrecv, sv_mix,
    sv_gu, sv_pj, sv_dn, hidden_other, dn_other, own_sem, send_sem, recv_sem, side_send, side_recv,
):
    f32, bf16 = jnp.float32, jnp.bfloat16
    (in_s, val_s, out_s, gate_s, up_s, pj_s, dn_s, mix_gain, ffn_gain, mix_taps, conv_gain, gate_taps, up_taps, gate_bias,
     up_bias) = small
    xs, ys, zs, near, other, tp = place()
    bufs = {"mix": mix, "pj": pj, "gu": gu, "dn": dn, "sc": sc}
    x, y, zl = xs[0], ys[0], zs[0]
    mine = pl.multiple_of(tp * 512, 512)
    yours = pl.multiple_of((1 - tp) * 512, 512)
    mix_f32 = [acc.at[64 * i : 64 * i + 64, 0:512] for i in range(3)]
    gu_f32 = [acc.at[192 + 64 * i : 256 + 64 * i, 0:1408] for i in range(2)]
    pj_f32, dn_f32 = acc.at[320:384, 0:512], acc.at[384:448, 0:1408]
    own = [
        pltpu.make_async_copy(src, dst, own_sem.at[i])
        for i, (src, dst) in enumerate(
            zip(
                (in_w, val_w, out_w, gate_w, up_w, pj_w, dn_w, tokens),
                (*mix_f32, *gu_f32, pj_f32, dn_f32, tok),
            )
        )
    ]
    small_copies = [pltpu.make_async_copy(src, dst, own_sem.at[8 + i]) for i, (src, dst) in enumerate(zip(small_in, small))]
    for copy in own[:3] + small_copies[:7] + own[3:] + small_copies[7:]:
        copy.start()
    barrier = pltpu.get_barrier_semaphore()
    for device in [*near.values(), other]:
        pl.semaphore_signal(barrier, inc=1, device_id=device, device_id_type=MESH)
    sc[zl, y, x] = jnp.zeros((8, 128), f32)
    for copy in small_copies[:7]:
        copy.wait()
    for i, ref in enumerate((in_s, val_s, out_s, gate_s, up_s, pj_s, dn_s)):
        sc[zl, y, x, i : i + 1, : ref.shape[0]] = ref[...].reshape(1, -1)
    for i in range(3):
        own[i].wait()
        for g in range(2):
            mix[3 * g + i, zl, y, x] = mix_f32[i][:, 256 * g : 256 * g + 256].astype(bf16)
    pl.semaphore_wait(barrier, 7)

    def block_cast(which):
        if which == "gu":
            for i in range(2):
                own[3 + i].wait()
                for k in range(11):
                    gu[k, zl, y, x, :, 128 * i : 128 * i + 128] = gu_f32[i][:, 128 * k : 128 * k + 128].astype(bf16)
        else:
            own[5].wait()
            pj[zl, y, x] = pj_f32[...].astype(bf16)
            own[6].wait()
            dn[zl, y, x] = dn_f32[...].astype(bf16)
            for unit in passed:
                pass_on(unit, (0, 0, 0), 13)

    def part(c, at):
        name, i, width = WHERE[c]
        z, y, x = at
        z = slice(None) if z is None else int(z[-1]) if isinstance(z, str) else zs[z]
        y = slice(None) if y is None else ys[y]
        x = slice(None) if x is None else xs[x]
        ref = bufs[name]
        if name in ("mix", "gu"):
            return ref.at[i, z, y, x]
        if name == "sc":
            return ref.at[z, y, x]
        return ref.at[z, y, x, :, i * UNIT : i * UNIT + width]

    def copy_of(c, m, arriving):
        kind, turn, _ = CHUNKS[c]
        ref = part(c, carried(kind, m, turn, arriving))
        return pltpu.make_async_remote_copy(
            src_ref=ref,
            dst_ref=ref,
            send_sem=send_sem.at[c],
            recv_sem=recv_sem.at[c, m],
            device_id=near[link_of(kind, m, turn)],
            device_id_type=MESH,
        )

    def to_other(src, dst, i):
        return pltpu.make_async_remote_copy(
            src_ref=src, dst_ref=dst, send_sem=side_send.at[i], recv_sem=side_recv.at[i], device_id=other, device_id_type=MESH
        )

    def normed(values, gain):
        return (values * lax.rsqrt(jnp.mean(values * values, axis=1, keepdims=True) + epsilon) * gain[...].reshape(1, -1)).astype(bf16)

    def shifted(values, before):
        both = jnp.concatenate([before, values], axis=0)
        return pltpu.roll(both, 1, 0)[8:], pltpu.roll(both, 2, 0)[8:]

    def dot_nt(left, right):
        return lax.dot_general(left, right, (((1,), (1,)), ((), ())), preferred_element_type=f32)

    def spread(row, width, group):
        total = jnp.zeros((1, 128), f32)
        lane = lax.broadcasted_iota(jnp.int32, (1, 128), 1)
        for s in range(group * 128 // width, min(31, (group * 128 + 127) // width) + 1):
            at = s * width - group * 128
            line = sc[s // 16, s // 4 % 4, s % 4, row : row + 1, :]
            if at % 128:
                line = pltpu.roll(line, at % 128, 1)
            total = jnp.where((lane >= at) & (lane < at + width), line, total)
        return total

    send_rows = [to_other(rows.at[pl.ds(mine, 512)], rows.at[pl.ds(mine, 512)], i) for i in (0, 3)]
    recv_rows = [to_other(rows.at[pl.ds(yours, 512)], rows.at[pl.ds(yours, 512)], i) for i in (0, 3)]
    send_sums = [to_other(psend, precv, i) for i in (1, 4)]
    send_square = to_other(square.at[pl.ds(yours, 512)], sqrecv, 2)
    def lanes_of(unit):
        return slice(UNIT * unit, min(UNIT * unit + UNIT, 1408)), slice(UNIT * (unit - PASSED), min(UNIT * unit + UNIT, 1408) - UNIT * PASSED)

    send_hidden = {}
    for unit in (4, 5):
        here, there = lanes_of(unit)
        send_hidden[unit] = to_other(hidden.at[pl.ds(yours, 512), here], hidden_other.at[:, there], 1 + unit)
    passed = {4: [], 5: []}
    seen = set()

    def pass_on(unit, at, i):
        z, y, x = at
        z = slice(None) if z is None else int(z[-1]) if isinstance(z, str) else zs[z]
        y = slice(None) if y is None else ys[y]
        x = slice(None) if x is None else xs[x]
        ref = dn_other.at[z, y, x, :, lanes_of(unit)[1]]
        copy = to_other(part(CHUNK_OF["dn", unit], at), ref, 7 + 14 * (unit - PASSED) + i)
        copy.start()
        passed[unit].append(copy)

    def block_norm():
        own[7].wait()
        for copy in small_copies[7:]:
            copy.wait()

        @pl.loop(0, 512, step=64)
        def _(r):
            at = pl.multiple_of(r, 64)
            rows[pl.ds(mine + at, 64), :] = normed(tok[pl.ds(at, 64), :].astype(f32), mix_gain)

        send_rows[0].start()

    def block_scales():
        for k in range(6):
            for i in range(2):
                sv_mix[k, :, 128 * i : 128 * i + 128] = spread(k % 3, 16, k // 3 * 2 + i)
        for k in range(11):
            sv_gu[k, :, :128] = spread(3, 44, k)
            sv_gu[k, :, 128:] = spread(4, 44, k)
        for k in range(16):
            sv_pj[k // 2, :, 128 * (k % 2) : 128 * (k % 2) + 128] = spread(5, 64, k)
            sv_dn[k // 2, :, 128 * (k % 2) : 128 * (k % 2) + 128] = spread(6, 64, k)

    def block_mix(k):
        if "rows" not in seen:
            seen.add("rows")
            recv_rows[0].wait_recv()

        for r in range(0, 1024, ROWS):
            at = pl.ds(r, ROWS)
            weight = mix[k].reshape(2048, 256)
            gates[k, at, :] = (jnp.dot(rows[at, :], weight, preferred_element_type=f32) * sv_mix[k]).astype(bf16)

    def block_conv(g):
        cols = slice(256 * g, 256 * g + 256)
        taps, gain = mix_taps[:, cols], conv_gain[cols].reshape(1, 256)

        def body(i, before):
            at = pl.ds(pl.multiple_of(i * 128, 128), 128)
            value = gates[3 * g, at, :].astype(f32) * gates[3 * g + 1, at, :].astype(f32)
            one, two = shifted(value, before)
            total = taps[0:1] * two + taps[1:2] * one + taps[2:3] * value
            done = (gates[3 * g + 2, at, :].astype(f32) * total).astype(bf16).astype(f32)
            conv[at, cols] = (done * gain).astype(bf16)
            squares = jnp.broadcast_to(jnp.sum(done * done, axis=1, keepdims=True), (128, 128))
            square[at, :] = squares if g == 0 else square[at, :] + squares
            return value[-8:]

        lax.fori_loop(0, 8, body, jnp.zeros((8, 256), f32))
        if g == 1:
            send_square.start()

    def block_proj(half):
        start = yours if half == 0 else mine

        for n in range(8):
            weight = pj[n // 4, n % 4].reshape(256, 512)
            part_sum = dot_nt(conv[pl.ds(start, 512), :], weight) * sv_pj[n]
            cols = slice(n * 256, n * 256 + 256)
            if half == 0:
                psend[:, cols] = part_sum.astype(bf16)
            else:
                acc[pl.ds(start, 512), cols] = part_sum

        if half == 0:
            send_sums[0].start()

    def block_first():
        send_sums[0].wait_recv()
        send_square.wait_recv()
        send_rows[0].wait_send()

        @pl.loop(0, 512, step=64)
        def _(r):
            at = pl.ds(pl.multiple_of(r, 64), 64)
            there = pl.ds(pl.multiple_of(mine + r, 64), 64)
            squares = square[there, :1] + sqrecv[at, :1]
            summed = (acc[there, :] + precv[at, :].astype(f32)) * lax.rsqrt(squares / 1024 + epsilon)
            first = (tok[at, :].astype(f32) + summed).astype(bf16)
            tok[at, :] = first
            rows[there, :] = normed(first.astype(f32), ffn_gain)

        send_rows[1].start()

    def block_gu(k):
        if "rows2" not in seen:
            seen.add("rows2")
            recv_rows[1].wait_recv()
        cols = slice(128 * k, 128 * k + 128)

        def body(i, before):
            at = pl.ds(i * ROWS, ROWS)
            weight = gu[k].reshape(2048, 256)
            pre = (jnp.dot(rows[at, :], weight, preferred_element_type=f32) * sv_gu[k]).astype(bf16).astype(f32)
            one, two = shifted(pre, before)
            acts = []
            for j, (taps, bias) in enumerate(((gate_taps, gate_bias), (up_taps, up_bias))):
                half, t = slice(128 * j, 128 * j + 128), taps[:, cols]
                acts.append(t[0:1] * two[:, half] + t[1:2] * one[:, half] + t[2:3] * pre[:, half] + bias[cols].reshape(1, 128))
            hidden[at, cols] = (acts[0] / (1.0 + jnp.exp(-acts[0])) * acts[1]).astype(bf16)
            return pre[-8:]

        before = jnp.zeros((8, 256), f32)
        for i in range(1024 // ROWS):
            before = body(i, before)
        seen.add(k)
        if k == 10:
            send_hidden[5].start()
        elif k in (8, 9) and {8, 9} <= seen:
            send_hidden[4].start()

    def block_down(j):
        first, count = DOWN[j]
        width = sum(WHERE[CHUNK_OF["dn", u]][2] for u in range(first, first + count))
        lanes = slice(UNIT * first, UNIT * first + width)

        def product(start, count, n):
            weight = dn[n // 4, n % 4, :, :, lanes].reshape(256, width)
            return dot_nt(hidden[pl.ds(start, count), lanes], weight)

        def sweep(start, count, store):
            for n in range(8):
                store(n, slice(n * 256, n * 256 + 256), pl.ds(start, count), product(start, count, n))

        def store(n, cols, at, value):
            acc[at, cols] = value if j == 0 else acc[at, cols] + value

        sweep(0, 1024, store)


    def block_give():
        send_sums[0].wait_send()

        @pl.loop(0, 512, step=64)
        def _(r):
            at, there = pl.ds(pl.multiple_of(r, 64), 64), pl.ds(pl.multiple_of(yours + r, 64), 64)
            for n in range(8):
                cols = slice(256 * n, 256 * n + 256)
                psend[at, cols] = (acc[there, cols] * sv_dn[n]).astype(bf16)

        send_sums[1].start()

    def block_base():
        send_sums[1].wait_recv()

        @pl.loop(0, 512, step=64)
        def _(r):
            at, there = pl.ds(pl.multiple_of(r, 64), 64), pl.ds(pl.multiple_of(mine + r, 64), 64)
            for n in range(8):
                cols = slice(256 * n, 256 * n + 256)
                summed = acc[there, cols] * sv_dn[n] + precv[at, cols].astype(f32)
                acc[there, cols] = tok[at, cols].astype(f32) + summed

    def block_near(unit):
        send_hidden[unit].wait_recv()
        for copy in passed[unit]:
            copy.wait_recv()
        here, there = lanes_of(unit)
        width = here.stop - here.start
        at = pl.ds(mine, 512)
        left = jnp.concatenate([hidden[at, here], hidden_other[:, there]], axis=1)
        for n in range(8):
            cols = slice(256 * n, 256 * n + 256)
            weights = [ref[n // 4, n % 4, :, :, lanes].reshape(256, width) for ref, lanes in ((dn, here), (dn_other, there))]
            value = acc[at, cols] + dot_nt(left, jnp.concatenate(weights, axis=1)) * sv_dn[n]
            if unit == 5:
                out[:, cols] = value.astype(bf16)
            else:
                acc[at, cols] = value

    blocks = {
        "cast": block_cast,
        "norm": block_norm, "scales": block_scales, "mix": block_mix, "conv": block_conv, "proj": block_proj,
        "first": block_first, "gu": block_gu, "down": block_down, "give": block_give, "base": block_base,
        "near": block_near,
    }
    gone = set()

    def sent_by(end):
        for c, (kind, _, _) in enumerate(CHUNKS):
            entries = range(len(TREES[kind]))
            if c not in gone and all(("send", c, m) in ops[:end] for m in entries):
                gone.add(c)
                for m in entries:
                    copy_of(c, m, False).wait_send()

    for step, op in enumerate(ops):
        if op[0] == "send":
            copy_of(op[1], op[2], False).start()
        elif op[0] == "wait":
            copy_of(op[1], op[2], True).wait_recv()
            name, unit, _ = WHERE[op[1]]
            if name == "dn" and unit in passed:
                pass_on(unit, carried(CHUNKS[op[1]][0], op[2], CHUNKS[op[1]][1], True), op[2])
        else:
            name, *index = names[op[1]]
            if name == "base":
                sent_by(step - 30)
            blocks[name](*index)
    sent_by(len(ops))
    send_square.wait_send()
    send_rows[1].wait_send()
    send_sums[1].wait_send()
    for unit in passed:
        for copy in [send_hidden[unit], *passed[unit]]:
            copy.wait_send()


def mega(*args):
    names, comps, own_after = list_of_blocks()
    ops, _, _, _ = plan(CHUNKS, comps, own_after)
    f32, bf16 = jnp.float32, jnp.bfloat16
    hbm, vmem = pl.BlockSpec(memory_space=pl.ANY), pl.BlockSpec(memory_space=pltpu.VMEM)
    dma = pltpu.SemaphoreType.DMA
    return pl.pallas_call(
        lambda *refs: mega_kernel(ops, names, *refs),
        out_shape=pltpu.VMEM((512, 2048), bf16),
        in_specs=[hbm] * 23,
        out_specs=vmem,
        scratch_shapes=[pltpu.VMEM(a.shape, f32) for a in args[8:]] + [
            pltpu.VMEM((6, 2, 4, 4, 64, 256), bf16),
            pltpu.VMEM((2, 4, 4, 64, 512), bf16),
            pltpu.VMEM((11, 2, 4, 4, 64, 256), bf16),
            pltpu.VMEM((2, 4, 4, 64, 1408), bf16),
            pltpu.VMEM((2, 4, 4, 8, 128), f32),
            pltpu.VMEM((512, 2048), bf16),
            pltpu.VMEM((1024, 2048), bf16),
            pltpu.VMEM((6, 1024, 256), bf16),
            pltpu.VMEM((1024, 512), bf16),
            pltpu.VMEM((1024, 128), f32),
            pltpu.VMEM((1024, 2048), f32),
            pltpu.VMEM((1024, 1408), bf16),
            pltpu.VMEM((512, 2048), bf16),
            pltpu.VMEM((512, 2048), bf16),
            pltpu.VMEM((512, 128), f32),
            pltpu.VMEM((6, 1, 256), f32),
            pltpu.VMEM((11, 1, 256), f32),
            pltpu.VMEM((8, 1, 256), f32),
            pltpu.VMEM((8, 1, 256), f32),
            pltpu.VMEM((512, 384), bf16),
            pltpu.VMEM((2, 4, 4, 64, 384), bf16),
            dma((23,)),
            dma((len(CHUNKS),)),
            dma((len(CHUNKS), 13)),
            dma((35,)),
            dma((35,)),
        ],
        compiler_params=pltpu.CompilerParams(collective_id=0, has_side_effects=True, vmem_limit_bytes=58 * 1024 * 1024),
    )(*args)


def to_hbm(values):
    def kernel(src, dst, sem):
        copies = [
            pltpu.make_async_copy(src.at[128 * q : 128 * q + 128], dst.at[128 * q : 128 * q + 128], sem.at[q])
            for q in range(4)
        ]
        for copy in copies:
            copy.start()
        for copy in copies:
            copy.wait()

    return pl.pallas_call(
        kernel,
        out_shape=jax.ShapeDtypeStruct(values.shape, values.dtype),
        in_specs=[pl.BlockSpec(memory_space=pltpu.VMEM)],
        out_specs=pl.BlockSpec(memory_space=pl.ANY),
        scratch_shapes=[pltpu.SemaphoreType.DMA((4,))],
        compiler_params=pltpu.CompilerParams(vmem_limit_bytes=4 * 1024 * 1024),
    )(values)


def local(
    tokens, mix_gain, out_gate_w, in_gate_w, value_w, out_gate_scale, in_gate_scale, value_scale, mix_taps, conv_gain,
    out_proj_w, proj_scale, ffn_gain, gate_w, up_w, gate_scale, up_scale, gate_taps, up_taps, gate_bias, up_bias, down_w,
    down_scale,
):
    return to_hbm(mega(
        tokens[0], in_gate_w, value_w, out_gate_w, gate_w, up_w, out_proj_w.T, down_w.T, in_gate_scale, value_scale,
        out_gate_scale, gate_scale, up_scale, proj_scale, down_scale, mix_gain, ffn_gain, mix_taps, conv_gain, gate_taps,
        up_taps, gate_bias, up_bias,
    ))[None]


def solution(mesh):
    placed = (
        P(("rep", "fs"), "tp", None), P(), P("fs", "tp"), P("fs", "tp"), P("fs", "tp"), P(("tp", "fs")), P(("tp", "fs")),
        P(("tp", "fs")), P(None, "tp"), P("tp"), P("tp", "fs"), P("fs"), P(), P("fs", "tp"), P("fs", "tp"), P(("tp", "fs")),
        P(("tp", "fs")), P(None, "tp"), P(None, "tp"), P("tp"), P("tp"), P("tp", "fs"), P("fs"),
    )
    return jax.shard_map(
        local, mesh=mesh, in_specs=placed, out_specs=P(("rep", "fs"), "tp", None), check_vma=False
    )
```

```python
import jax
import jax.numpy as jnp
from jax import lax
from jax.experimental import pallas as pl
from jax.experimental.pallas import tpu as pltpu
from jax.sharding import PartitionSpec as P

epsilon = 1e-06
MESH = pl.DeviceIdType.MESH
UNIT = 256
TURNED = "so"

TREES = {
    "A": (
        ((), "x+", 1),
        ((), "x-", 1),
        ("s01", "xs", 1),
        ((0, 1, 2), "y+", 4),
        ((0, 1, 2), "y-", 4),
        ((0, 1, 2), "zs", 4),
        ("s34", "ys", 4),
        ("s34", "zo", 4),
        ("o34", "zo", 4),
        ((6,), "zs", 4),
    ),
    "D": (
        ((), "zs", 1),
        ((0,), "y+", 2),
        ((0,), "y-", 2),
        ("s12", "ys", 2),
        ((1, 2, 3), "x+", 8),
        ((1, 2, 3), "x-", 8),
        ((4,), "x+", 4),
        ((5,), "x-", 4),
    ),
    "E": (
        ((), "x+", 1),
        ((), "x-", 1),
        ("s01", "xs", 1),
        ((0, 1, 2), "y+", 4),
        ((0, 1, 2), "y-", 4),
        ((), "zs", 1),
        ((0,), "zs", 1),
        ((1,), "zs", 1),
        ((2,), "zs", 1),
        ("s34", "ys", 4),
        ("s34", "zo", 4),
        ("o34", "zo", 4),
        ((9,), "zs", 4),
    ),
    "C": (
        ((), "zs", 1),
        ((0,), "x+", 2),
        ((0,), "x-", 2),
        ("s12", "xs", 2),
        ((1, 2, 3), "y+", 8),
        ((1, 2, 3), "y-", 8),
        ((4,), "y+", 4),
        ((5,), "y-", 4),
    ),
}


def needs_of(kind, m, turn):
    need = TREES[kind][m][0]
    if isinstance(need, str):
        first, second = int(need[1]), int(need[2])
        return (first if (turn > 0) == (need[0] == "s") else second,)
    return need


def link_of(kind, m, turn):
    name = TREES[kind][m][1]
    sign = {"+": 1, "-": -1, "s": turn, "o": -turn}[name[1]]
    return name[0], sign


RATE, HOP, AHEAD = 46.5, 2.2, 1.5
ORDER = (
    ("mix", 4, "D", -1),
    ("pj", 1, "D", -1),
    ("mix", 0, "A", 1),
    ("gu", 8, "E", -1),
    ("dn", 3, "A", 1),
    ("mix", 2, "D", 1),
    ("mix", 3, "A", 1),
    ("mix", 1, "E", -1),
    ("mix", 5, "A", -1),
    ("pj", 0, "D", 1),
    ("gu", 5, "A", -1),
    ("gu", 1, "D", 1),
    ("gu", 4, "A", 1),
    ("gu", 7, "D", 1),
    ("gu", 3, "E", -1),
    ("gu", 2, "A", -1),
    ("gu", 9, "D", -1),
    ("dn", 1, "E", 1),
    ("gu", 6, "E", -1),
    ("dn", 0, "D", 1),
    ("gu", 0, "A", -1),
    ("dn", 2, "E", 1),
    ("gu", 10, "E", 1),
    ("dn", 5, "D", -1),
    ("dn", 4, "E", 1),
)
LEAD = {("A", 6): 7.5, ("C", 4): 2.5, ("D", 2): 0.5, ("D", 3): 8.0, ("D", 1): 9.5, ("D", 5): 3, ("D", 6): 12, ("A", 0): 2.5, ("D", 7): 10.0, ("D", 0): 4.0, ("A", 7): 12, ("C", 1): 6.0, ("C", 6): 0.5, ("A", 1): -1.0, ("A", 9): -2.5, ("A", 4): 1.5, ("A", 2): 12, ("A", 3): 6.0, ("C", 0): 7.5, ("D", 4): 6.0, ("C", 5): 8.5, ("C", 7): -2.0, ("C", 3): -2.5, ("A", 5): 1, ("C", 2): 5.0, ("A", 8): 12, ("E", 7): 8, ("E", 11): -2, ("E", 8): -1.5, ("E", 0): -0.5, ("E", 2): -2.5, ("E", 9): 3.0, ("E", 3): 12, ("E", 5): 0.5, ("E", 4): -3, ("E", 1): -3, ("E", 12): 2.5, ("E", 6): 12}


def plan(chunks, comps, own_after, rate=RATE, hop=HOP, issue=0.04, ahead=AHEAD):
    links = {(a, s): 0.0 for a in "xyz" for s in (1, -1)}
    arrive, waited, sent, ops, done, t = {}, set(), set(), [], {}, 0.0
    every = [(c, m) for c in range(len(chunks)) for m in range(len(TREES[chunks[c][0]]))]
    every.sort(key=lambda e: (e[0] - LEAD.get((chunks[e[0]][0], e[1]), 0.0), e[1]))
    log = []

    def wait(pairs):
        for pair in pairs:
            if pair not in waited:
                waited.add(pair)
                ops.append(("wait", *pair))

    while True:
        best = None
        for c, m in every:
            kind, turn, size = chunks[c]
            if (c, m) in sent:
                continue
            needs = [(c, k) for k in needs_of(kind, m, turn)]
            link = link_of(kind, m, turn)
            here = bool(needs) or c not in own_after or own_after[c] in done
            if here and all(arrive.get(k, 1e9) <= t for k in needs) and links[link] <= t + ahead:
                best = (c, m, needs, link, size * TREES[kind][m][2])
                break
        if best is not None:
            c, m, needs, link, size = best
            wait(needs)
            ops.append(("send", c, m))
            sent.add((c, m))
            t += issue
            links[link] = max(t, links[link]) + size / rate / 1000.0
            arrive[c, m] = links[link] + hop
            continue
        soon = []
        for k, (us, of_chunks, of_comps) in enumerate(comps):
            if k in done:
                continue
            pairs = [(c, m) for c, m in every if c in of_chunks]
            ready = max([arrive.get(q, 1e9) for q in pairs] + [done.get(b, 1e9) + lag for b, lag in of_comps] + [0.0])
            if ready <= t:
                wait(pairs)
                ops.append(("comp", k))
                log.append((round(t, 1), k))
                t += us
                done[k] = t
                break
            if ready < 1e8:
                soon.append(ready)
        else:
            later = [a for a in arrive.values() if a > t] + [b - ahead for b in links.values() if b - ahead > t] + soon
            if not later:
                break
            t = min(later) + 1e-6
    wait(every)
    return ops, t, log, arrive


def list_of_chunks():
    chunks, where = [("A", 1, 4096)], [("sc", 0, 128)]
    for name, i, kind, turn in ORDER:
        width = UNIT // 2 if (name, i) == LAST else UNIT
        chunks.append((kind, turn, 64 * width * 2))
        where.append((name, i, width))
    return chunks, where


LAST = ("dn", 5)
CHUNKS, WHERE = list_of_chunks()
CHUNK_OF = {(name, i): c for c, (name, i, _) in enumerate(WHERE)}
ROWS = 256
DOWN = ((0, 2), (2, 2))
PASSED = 4


def list_of_blocks():
    names, comps, number = [], [], {}

    def add(name, us, chunks=(), after=()):
        number[name] = len(names)
        names.append(name)
        comps.append((us, {CHUNK_OF[c] for c in chunks}, [(number[b], lag) for b, lag in after]))

    add(("cast", "gu"), 0.5)
    add(("cast", "rest"), 0.4)
    add(("norm",), 1.3)
    add(("scales",), 0.3, [("sc", 0)])
    for k in range(6):
        add(("mix", k), 1.25, [("mix", k)], [(("norm",), 4.0), (("scales",), 0.0)])
    for g in range(2):
        add(("conv", g), 1.3, [], [(("mix", 3 * g + i), 0.0) for i in range(3)] + [(("conv", 0), 0.0)] * g)
    add(("proj", 0), 1.3, [("pj", 0), ("pj", 1)], [(("conv", 0), 0.0), (("conv", 1), 0.0)])
    add(("proj", 1), 1.3, [], [(("proj", 0), 0.0)])
    add(("first",), 2.8, [], [(("proj", 1), 0.0), (("proj", 0), 2.0)])
    for k in range(11):
        add(("gu", k), 1.75, [("gu", k)], [(("first",), 2.2)])
    for j, (first, count) in enumerate(DOWN):
        units = range(first, first + count)
        before = [(("gu", k), 0.0) for u in units for k in (2 * u, 2 * u + 1)] + [(("down", j - 1), 0.0)] * (j > 0)
        add(("down", j), 2.4, [("dn", u) for u in units], before)
    add(("give",), 0.3, [], [(("down", len(DOWN) - 1), 0.0)])
    add(("base",), 0.9, [], [(("give",), 4.2)])
    add(("near", 4), 1.7, [("dn", 4)], [(("base",), 0.0), (("gu", 8), 2.0), (("gu", 9), 2.0)])
    add(("near", 5), 1.9, [("dn", 5)], [(("near", 4), 0.0), (("gu", 10), 2.0)])
    own_after = {}
    for (name, _), c in CHUNK_OF.items():
        if name in ("gu", "pj", "dn"):
            own_after[c] = number["cast", "gu" if name == "gu" else "rest"]
    return names, comps, own_after


def place():
    rep, fs = lax.axis_index("rep"), lax.axis_index("fs")
    tp = lax.axis_index("tp")
    x, y, zl = lax.rem(fs, 4), lax.rem(fs // 4, 4), fs // 16
    z = rep * 2 + zl
    xs = {n: lax.rem(x + 4 + n, 4) for n in (-1, 1, 2)} | {0: x}
    ys = {n: lax.rem(y + 4 + n, 4) for n in (-1, 1, 2)} | {0: y}
    near = {}
    for sign in (1, -1):
        near["x", sign] = (rep, zl * 16 + y * 4 + xs[sign], tp)
        near["y", sign] = (rep, zl * 16 + ys[sign] * 4 + x, tp)
        zn = lax.rem(z + 4 + sign, 4)
        near["z", sign] = (zn // 2, lax.rem(zn, 2) * 16 + y * 4 + x, tp)
    return xs, ys, {0: zl, 1: 1 - zl}, near, (rep, fs, 1 - tp), tp


def carried(kind, m, turn, arriving):
    sent = {
        "A": (
            (0, 0, 0),
            (0, 0, 0),
            (0, 0, -turn),
            (0, 0, None),
            (0, 0, None),
            (0, 0, None),
            (0, -turn, None),
            (0, -turn, None),
            (0, turn, None),
            (0, 2, None),
        ),
        "D": (
            (0, 0, 0),
            (None, 0, 0),
            (None, 0, 0),
            (None, -turn, 0),
            (None, None, 0),
            (None, None, 0),
            ("plane0", None, -1),
            ("plane1", None, 1),
        ),
        "E": (
            (0, 0, 0),
            (0, 0, 0),
            (0, 0, -turn),
            (0, 0, None),
            (0, 0, None),
            (0, 0, 0),
            (0, 0, -1),
            (0, 0, 1),
            (0, 0, 2),
            (0, -turn, None),
            (0, -turn, None),
            (0, turn, None),
            (0, 2, None),
        ),
        "C": (
            (0, 0, 0),
            (None, 0, 0),
            (None, 0, 0),
            (None, 0, -turn),
            (None, 0, None),
            (None, 0, None),
            ("plane0", -1, None),
            ("plane1", 1, None),
        ),
    }[kind][m]
    if not arriving:
        return sent
    link, sign = link_of(kind, m, turn)
    z, y, x = sent

    def back(v, n):
        v = v - n
        return v + 4 if v < -1 else v - 4 if v > 2 else v

    if link == "x":
        x = back(x, sign)
    elif link == "y":
        y = back(y, sign)
    else:
        z = 1 - z
    return z, y, x


def mega_kernel(
    ops, names, tokens, in_w, val_w, out_w, gate_w, up_w, pj_w, dn_w, *rest,
):
    small_in, out, small = rest[:15], rest[15], rest[16:31]
    run_kernel(ops, names, tokens, in_w, val_w, out_w, gate_w, up_w, pj_w, dn_w, small_in, small, out, *rest[31:])


def run_kernel(
    ops, names, tokens, in_w, val_w, out_w, gate_w, up_w, pj_w, dn_w, small_in, small, out, mix, pj, gu, dn, sc, tok, rows, gates, conv, square, acc, hidden, psend, precv, sqrecv, sv_mix,
    sv_gu, sv_pj, sv_dn, hidden_other, dn_other, own_sem, send_sem, recv_sem, side_send, side_recv,
):
    f32, bf16 = jnp.float32, jnp.bfloat16
    (in_s, val_s, out_s, gate_s, up_s, pj_s, dn_s, mix_gain, ffn_gain, mix_taps, conv_gain, gate_taps, up_taps, gate_bias,
     up_bias) = small
    xs, ys, zs, near, other, tp = place()
    bufs = {"mix": mix, "pj": pj, "gu": gu, "dn": dn, "sc": sc}
    x, y, zl = xs[0], ys[0], zs[0]
    mine = pl.multiple_of(tp * 512, 512)
    yours = pl.multiple_of((1 - tp) * 512, 512)
    mix_f32 = [acc.at[64 * i : 64 * i + 64, 0:512] for i in range(3)]
    gu_f32 = [acc.at[192 + 64 * i : 256 + 64 * i, 0:1408] for i in range(2)]
    pj_f32, dn_f32 = acc.at[320:384, 0:512], acc.at[384:448, 0:1408]
    own = [
        pltpu.make_async_copy(src, dst, own_sem.at[i])
        for i, (src, dst) in enumerate(
            zip(
                (in_w, val_w, out_w, gate_w, up_w, pj_w, dn_w, tokens),
                (*mix_f32, *gu_f32, pj_f32, dn_f32, tok),
            )
        )
    ]
    small_copies = [pltpu.make_async_copy(src, dst, own_sem.at[8 + i]) for i, (src, dst) in enumerate(zip(small_in, small))]
    for copy in own[:3] + small_copies[:7] + own[3:] + small_copies[7:]:
        copy.start()
    barrier = pltpu.get_barrier_semaphore()
    for device in [*near.values(), other]:
        pl.semaphore_signal(barrier, inc=1, device_id=device, device_id_type=MESH)
    sc[zl, y, x] = jnp.zeros((8, 128), f32)
    for copy in small_copies[:7]:
        copy.wait()
    for i, ref in enumerate((in_s, val_s, out_s, gate_s, up_s, pj_s, dn_s)):
        sc[zl, y, x, i : i + 1, : ref.shape[0]] = ref[...].reshape(1, -1)
    for i in range(3):
        own[i].wait()
        for g in range(2):
            mix[3 * g + i, zl, y, x] = mix_f32[i][:, 256 * g : 256 * g + 256].astype(bf16)
    pl.semaphore_wait(barrier, 7)

    def block_cast(which):
        if which == "gu":
            for i in range(2):
                own[3 + i].wait()
                for k in range(11):
                    gu[k, zl, y, x, :, 128 * i : 128 * i + 128] = gu_f32[i][:, 128 * k : 128 * k + 128].astype(bf16)
        else:
            own[5].wait()
            pj[zl, y, x] = pj_f32[...].astype(bf16)
            own[6].wait()
            dn[zl, y, x] = dn_f32[...].astype(bf16)
            for unit in passed:
                pass_on(unit, (0, 0, 0), 13)

    def part(c, at):
        name, i, width = WHERE[c]
        z, y, x = at
        z = slice(None) if z is None else int(z[-1]) if isinstance(z, str) else zs[z]
        y = slice(None) if y is None else ys[y]
        x = slice(None) if x is None else xs[x]
        ref = bufs[name]
        if name in ("mix", "gu"):
            return ref.at[i, z, y, x]
        if name == "sc":
            return ref.at[z, y, x]
        return ref.at[z, y, x, :, i * UNIT : i * UNIT + width]

    def copy_of(c, m, arriving):
        kind, turn, _ = CHUNKS[c]
        ref = part(c, carried(kind, m, turn, arriving))
        return pltpu.make_async_remote_copy(
            src_ref=ref,
            dst_ref=ref,
            send_sem=send_sem.at[c],
            recv_sem=recv_sem.at[c, m],
            device_id=near[link_of(kind, m, turn)],
            device_id_type=MESH,
        )

    def to_other(src, dst, i):
        return pltpu.make_async_remote_copy(
            src_ref=src, dst_ref=dst, send_sem=side_send.at[i], recv_sem=side_recv.at[i], device_id=other, device_id_type=MESH
        )

    def normed(values, gain):
        return (values * lax.rsqrt(jnp.mean(values * values, axis=1, keepdims=True) + epsilon) * gain[...].reshape(1, -1)).astype(bf16)

    def shifted(values, before):
        both = jnp.concatenate([before, values], axis=0)
        return pltpu.roll(both, 1, 0)[8:], pltpu.roll(both, 2, 0)[8:]

    def dot_nt(left, right):
        return lax.dot_general(left, right, (((1,), (1,)), ((), ())), preferred_element_type=f32)

    def spread(row, width, group):
        total = jnp.zeros((1, 128), f32)
        lane = lax.broadcasted_iota(jnp.int32, (1, 128), 1)
        for s in range(group * 128 // width, min(31, (group * 128 + 127) // width) + 1):
            at = s * width - group * 128
            line = sc[s // 16, s // 4 % 4, s % 4, row : row + 1, :]
            if at % 128:
                line = pltpu.roll(line, at % 128, 1)
            total = jnp.where((lane >= at) & (lane < at + width), line, total)
        return total

    def rows_copy(to_send, first, count, i):
        at = pl.ds((mine if to_send else yours) + first, count)
        return to_other(rows.at[at], rows.at[at], i)

    send_rows, recv_rows = (rows_copy(b, 0, 512, 0) for b in (True, False))
    send_again, recv_again = ([rows_copy(b, 128 * q, 128, 35 + q) for q in range(4)] for b in (True, False))
    send_parts = [to_other(psend.at[pl.ds(256 * q, 256)], precv.at[pl.ds(256 * q, 256)], (1, 3)[q]) for q in range(2)]
    send_sums = to_other(psend, precv, 4)
    send_square = to_other(square.at[pl.ds(yours, 512)], sqrecv, 2)
    def lanes_of(unit):
        return slice(UNIT * unit, min(UNIT * unit + UNIT, 1408)), slice(UNIT * (unit - PASSED), min(UNIT * unit + UNIT, 1408) - UNIT * PASSED)

    send_hidden = {}
    for unit in (4, 5):
        here, there = lanes_of(unit)
        send_hidden[unit] = to_other(hidden.at[pl.ds(yours, 512), here], hidden_other.at[:, there], 1 + unit)
    passed = {4: [], 5: []}
    seen = set()

    def pass_on(unit, at, i):
        z, y, x = at
        z = slice(None) if z is None else int(z[-1]) if isinstance(z, str) else zs[z]
        y = slice(None) if y is None else ys[y]
        x = slice(None) if x is None else xs[x]
        ref = dn_other.at[z, y, x, :, lanes_of(unit)[1]]
        copy = to_other(part(CHUNK_OF["dn", unit], at), ref, 7 + 14 * (unit - PASSED) + i)
        copy.start()
        passed[unit].append(copy)

    def block_norm():
        own[7].wait()
        for copy in small_copies[7:]:
            copy.wait()

        @pl.loop(0, 512, step=64)
        def _(r):
            at = pl.multiple_of(r, 64)
            rows[pl.ds(mine + at, 64), :] = normed(tok[pl.ds(at, 64), :].astype(f32), mix_gain)

        send_rows.start()

    def block_scales():
        for k in range(6):
            for i in range(2):
                sv_mix[k, :, 128 * i : 128 * i + 128] = spread(k % 3, 16, k // 3 * 2 + i)
        for k in range(11):
            sv_gu[k, :, :128] = spread(3, 44, k)
            sv_gu[k, :, 128:] = spread(4, 44, k)
        for k in range(16):
            sv_pj[k // 2, :, 128 * (k % 2) : 128 * (k % 2) + 128] = spread(5, 64, k)
            sv_dn[k // 2, :, 128 * (k % 2) : 128 * (k % 2) + 128] = spread(6, 64, k)

    def block_mix(k):
        if "rows" not in seen:
            seen.add("rows")
            recv_rows.wait_recv()

        for r in range(0, 1024, ROWS):
            at = pl.ds(r, ROWS)
            weight = mix[k].reshape(2048, 256)
            gates[k, at, :] = (jnp.dot(rows[at, :], weight, preferred_element_type=f32) * sv_mix[k]).astype(bf16)

    def block_conv(g):
        cols = slice(256 * g, 256 * g + 256)
        taps, gain = mix_taps[:, cols], conv_gain[cols].reshape(1, 256)

        def body(i, before):
            at = pl.ds(pl.multiple_of(i * 128, 128), 128)
            value = gates[3 * g, at, :].astype(f32) * gates[3 * g + 1, at, :].astype(f32)
            one, two = shifted(value, before)
            total = taps[0:1] * two + taps[1:2] * one + taps[2:3] * value
            done = (gates[3 * g + 2, at, :].astype(f32) * total).astype(bf16).astype(f32)
            conv[at, cols] = (done * gain).astype(bf16)
            squares = jnp.broadcast_to(jnp.sum(done * done, axis=1, keepdims=True), (128, 128))
            square[at, :] = squares if g == 0 else square[at, :] + squares
            return value[-8:]

        lax.fori_loop(0, 8, body, jnp.zeros((8, 256), f32))
        if g == 1:
            send_square.start()

    def block_proj(half):
        for q in range(2):
            here = pl.ds(256 * q, 256)
            rows_at = pl.ds((yours if half == 0 else mine) + 256 * q, 256)
            for n in range(8):
                weight = pj[n // 4, n % 4].reshape(256, 512)
                part_sum = dot_nt(conv[rows_at, :], weight) * sv_pj[n]
                cols = slice(n * 256, n * 256 + 256)
                if half == 0:
                    psend[here, cols] = part_sum.astype(bf16)
                else:
                    acc[rows_at, cols] = part_sum
            if half == 0:
                send_parts[q].start()

    def block_first():
        send_square.wait_recv()
        send_rows.wait_send()
        for q in range(4):
            if q % 2 == 0:
                send_parts[q // 2].wait_recv()

            @pl.loop(128 * q, 128 * q + 128, step=64)
            def _(r):
                at = pl.ds(pl.multiple_of(r, 64), 64)
                there = pl.ds(pl.multiple_of(mine + r, 64), 64)
                squares = square[there, :1] + sqrecv[at, :1]
                summed = (acc[there, :] + precv[at, :].astype(f32)) * lax.rsqrt(squares / 1024 + epsilon)
                first = (tok[at, :].astype(f32) + summed).astype(bf16)
                tok[at, :] = first
                rows[there, :] = normed(first.astype(f32), ffn_gain)

            send_again[q].start()

    def block_gu(k):
        if "rows2" not in seen:
            seen.add("rows2")
            for copy in recv_again:
                copy.wait_recv()
        cols = slice(128 * k, 128 * k + 128)

        def body(i, before):
            at = pl.ds(i * ROWS, ROWS)
            weight = gu[k].reshape(2048, 256)
            pre = (jnp.dot(rows[at, :], weight, preferred_element_type=f32) * sv_gu[k]).astype(bf16).astype(f32)
            one, two = shifted(pre, before)
            acts = []
            for j, (taps, bias) in enumerate(((gate_taps, gate_bias), (up_taps, up_bias))):
                half, t = slice(128 * j, 128 * j + 128), taps[:, cols]
                acts.append(t[0:1] * two[:, half] + t[1:2] * one[:, half] + t[2:3] * pre[:, half] + bias[cols].reshape(1, 128))
            half = 0.5 * acts[0]
            hidden[at, cols] = ((half + half * jnp.tanh(half)) * acts[1]).astype(bf16)
            return pre[-8:]

        before = jnp.zeros((8, 256), f32)
        for i in range(1024 // ROWS):
            before = body(i, before)
        seen.add(k)
        if k == 10:
            send_hidden[5].start()
        elif k in (8, 9) and {8, 9} <= seen:
            send_hidden[4].start()

    def block_down(j):
        first, count = DOWN[j]
        width = sum(WHERE[CHUNK_OF["dn", u]][2] for u in range(first, first + count))
        lanes = slice(UNIT * first, UNIT * first + width)

        def product(start, count, n):
            weight = dn[n // 4, n % 4, :, :, lanes].reshape(256, width)
            return dot_nt(hidden[pl.ds(start, count), lanes], weight)

        def sweep(start, count, store):
            for n in range(8):
                store(n, slice(n * 256, n * 256 + 256), pl.ds(start, count), product(start, count, n))

        def store(n, cols, at, value):
            acc[at, cols] = value if j == 0 else acc[at, cols] + value

        sweep(0, 1024, store)


    def block_give():
        for copy in send_parts:
            copy.wait_send()

        @pl.loop(0, 512, step=64)
        def _(r):
            at, there = pl.ds(pl.multiple_of(r, 64), 64), pl.ds(pl.multiple_of(yours + r, 64), 64)
            for n in range(8):
                cols = slice(256 * n, 256 * n + 256)
                psend[at, cols] = (acc[there, cols] * sv_dn[n]).astype(bf16)

        send_sums.start()

    def block_base():
        send_sums.wait_recv()

        @pl.loop(0, 512, step=64)
        def _(r):
            at, there = pl.ds(pl.multiple_of(r, 64), 64), pl.ds(pl.multiple_of(mine + r, 64), 64)
            for n in range(8):
                cols = slice(256 * n, 256 * n + 256)
                summed = acc[there, cols] * sv_dn[n] + precv[at, cols].astype(f32)
                acc[there, cols] = tok[at, cols].astype(f32) + summed

    def block_near(unit):
        send_hidden[unit].wait_recv()
        for copy in passed[unit]:
            copy.wait_recv()
        here, there = lanes_of(unit)
        width = here.stop - here.start
        at = pl.ds(mine, 512)
        left = jnp.concatenate([hidden[at, here], hidden_other[:, there]], axis=1)
        for n in range(8):
            cols = slice(256 * n, 256 * n + 256)
            weights = [ref[n // 4, n % 4, :, :, lanes].reshape(256, width) for ref, lanes in ((dn, here), (dn_other, there))]
            value = acc[at, cols] + dot_nt(left, jnp.concatenate(weights, axis=1)) * sv_dn[n]
            if unit == 5:
                out[:, cols] = value.astype(bf16)
            else:
                acc[at, cols] = value

    blocks = {
        "cast": block_cast,
        "norm": block_norm, "scales": block_scales, "mix": block_mix, "conv": block_conv, "proj": block_proj,
        "first": block_first, "gu": block_gu, "down": block_down, "give": block_give, "base": block_base,
        "near": block_near,
    }
    gone = set()

    def sent_by(end):
        for c, (kind, _, _) in enumerate(CHUNKS):
            entries = range(len(TREES[kind]))
            if c not in gone and all(("send", c, m) in ops[:end] for m in entries):
                gone.add(c)
                for m in entries:
                    copy_of(c, m, False).wait_send()

    for step, op in enumerate(ops):
        if op[0] == "send":
            copy_of(op[1], op[2], False).start()
        elif op[0] == "wait":
            copy_of(op[1], op[2], True).wait_recv()
            name, unit, _ = WHERE[op[1]]
            if name == "dn" and unit in passed:
                pass_on(unit, carried(CHUNKS[op[1]][0], op[2], CHUNKS[op[1]][1], True), op[2])
        else:
            name, *index = names[op[1]]
            if name == "base":
                sent_by(step - 30)
            blocks[name](*index)
    sent_by(len(ops))
    send_square.wait_send()
    send_sums.wait_send()
    for copy in send_again:
        copy.wait_send()
    for unit in passed:
        for copy in [send_hidden[unit], *passed[unit]]:
            copy.wait_send()


def mega(*args):
    names, comps, own_after = list_of_blocks()
    ops, _, _, _ = plan(CHUNKS, comps, own_after)
    f32, bf16 = jnp.float32, jnp.bfloat16
    hbm, vmem = pl.BlockSpec(memory_space=pl.ANY), pl.BlockSpec(memory_space=pltpu.VMEM)
    dma = pltpu.SemaphoreType.DMA
    return pl.pallas_call(
        lambda *refs: mega_kernel(ops, names, *refs),
        out_shape=pltpu.VMEM((512, 2048), bf16),
        in_specs=[hbm] * 23,
        out_specs=vmem,
        scratch_shapes=[pltpu.VMEM(a.shape, f32) for a in args[8:]] + [
            pltpu.VMEM((6, 2, 4, 4, 64, 256), bf16),
            pltpu.VMEM((2, 4, 4, 64, 512), bf16),
            pltpu.VMEM((11, 2, 4, 4, 64, 256), bf16),
            pltpu.VMEM((2, 4, 4, 64, 1408), bf16),
            pltpu.VMEM((2, 4, 4, 8, 128), f32),
            pltpu.VMEM((512, 2048), bf16),
            pltpu.VMEM((1024, 2048), bf16),
            pltpu.VMEM((6, 1024, 256), bf16),
            pltpu.VMEM((1024, 512), bf16),
            pltpu.VMEM((1024, 128), f32),
            pltpu.VMEM((1024, 2048), f32),
            pltpu.VMEM((1024, 1408), bf16),
            pltpu.VMEM((512, 2048), bf16),
            pltpu.VMEM((512, 2048), bf16),
            pltpu.VMEM((512, 128), f32),
            pltpu.VMEM((6, 1, 256), f32),
            pltpu.VMEM((11, 1, 256), f32),
            pltpu.VMEM((8, 1, 256), f32),
            pltpu.VMEM((8, 1, 256), f32),
            pltpu.VMEM((512, 384), bf16),
            pltpu.VMEM((2, 4, 4, 64, 384), bf16),
            dma((23,)),
            dma((len(CHUNKS),)),
            dma((len(CHUNKS), 13)),
            dma((39,)),
            dma((39,)),
        ],
        compiler_params=pltpu.CompilerParams(collective_id=0, has_side_effects=True, vmem_limit_bytes=58 * 1024 * 1024),
    )(*args)


def to_hbm(values):
    def kernel(src, dst, sem):
        copies = [
            pltpu.make_async_copy(src.at[128 * q : 128 * q + 128], dst.at[128 * q : 128 * q + 128], sem.at[q])
            for q in range(4)
        ]
        for copy in copies:
            copy.start()
        for copy in copies:
            copy.wait()

    return pl.pallas_call(
        kernel,
        out_shape=jax.ShapeDtypeStruct(values.shape, values.dtype),
        in_specs=[pl.BlockSpec(memory_space=pltpu.VMEM)],
        out_specs=pl.BlockSpec(memory_space=pl.ANY),
        scratch_shapes=[pltpu.SemaphoreType.DMA((4,))],
        compiler_params=pltpu.CompilerParams(vmem_limit_bytes=4 * 1024 * 1024),
    )(values)


def local(
    tokens, mix_gain, out_gate_w, in_gate_w, value_w, out_gate_scale, in_gate_scale, value_scale, mix_taps, conv_gain,
    out_proj_w, proj_scale, ffn_gain, gate_w, up_w, gate_scale, up_scale, gate_taps, up_taps, gate_bias, up_bias, down_w,
    down_scale,
):
    return to_hbm(mega(
        tokens[0], in_gate_w, value_w, out_gate_w, gate_w, up_w, out_proj_w.T, down_w.T, in_gate_scale, value_scale,
        out_gate_scale, gate_scale, up_scale, proj_scale, down_scale, mix_gain, ffn_gain, mix_taps, conv_gain, gate_taps,
        up_taps, gate_bias, up_bias,
    ))[None]


def solution(mesh):
    placed = (
        P(("rep", "fs"), "tp", None), P(), P("fs", "tp"), P("fs", "tp"), P("fs", "tp"), P(("tp", "fs")), P(("tp", "fs")),
        P(("tp", "fs")), P(None, "tp"), P("tp"), P("tp", "fs"), P("fs"), P(), P("fs", "tp"), P("fs", "tp"), P(("tp", "fs")),
        P(("tp", "fs")), P(None, "tp"), P(None, "tp"), P("tp"), P("tp"), P("tp", "fs"), P("fs"),
    )
    return jax.shard_map(
        local, mesh=mesh, in_specs=placed, out_specs=P(("rep", "fs"), "tp", None), check_vma=False
    )
```

```python
import jax
import jax.numpy as jnp
from jax import lax
from jax.experimental import pallas as pl
from jax.experimental.pallas import tpu as pltpu
from jax.sharding import PartitionSpec as P

epsilon = 1e-06
MESH = pl.DeviceIdType.MESH
UNIT = 256
TURNED = "so"

TREES = {
    "A": (
        ((), "x+", 1),
        ((), "x-", 1),
        ("s01", "xs", 1),
        ((0, 1, 2), "y+", 4),
        ((0, 1, 2), "y-", 4),
        ((0, 1, 2), "zs", 4),
        ("s34", "ys", 4),
        ("s34", "zo", 4),
        ("o34", "zo", 4),
        ((6,), "zs", 4),
    ),
    "D": (
        ((), "zs", 1),
        ((0,), "y+", 2),
        ((0,), "y-", 2),
        ("s12", "ys", 2),
        ((1, 2, 3), "x+", 8),
        ((1, 2, 3), "x-", 8),
        ((4,), "x+", 4),
        ((5,), "x-", 4),
    ),
    "E": (
        ((), "x+", 1),
        ((), "x-", 1),
        ("s01", "xs", 1),
        ((0, 1, 2), "y+", 4),
        ((0, 1, 2), "y-", 4),
        ((), "zs", 1),
        ((0,), "zs", 1),
        ((1,), "zs", 1),
        ((2,), "zs", 1),
        ("s34", "ys", 4),
        ("s34", "zo", 4),
        ("o34", "zo", 4),
        ((9,), "zs", 4),
    ),
    "C": (
        ((), "zs", 1),
        ((0,), "x+", 2),
        ((0,), "x-", 2),
        ("s12", "xs", 2),
        ((1, 2, 3), "y+", 8),
        ((1, 2, 3), "y-", 8),
        ((4,), "y+", 4),
        ((5,), "y-", 4),
    ),
}


ENDS = {
    "A": ((5, 7, 8, 9), (1, None, None)),
    "E": ((5, 6, 7, 8, 10, 11, 12), (1, None, None)),
    "D": ((6, 7), (None, None, 2)),
    "C": ((6, 7), (None, 2, None)),
}


def slot_of(kind, m):
    ends = ENDS[kind][0]
    return 0 if m in ends else 1 + [k for k in range(len(TREES[kind])) if k not in ends].index(m)


def needs_of(kind, m, turn):
    need = TREES[kind][m][0]
    if isinstance(need, str):
        first, second = int(need[1]), int(need[2])
        return (first if (turn > 0) == (need[0] == "s") else second,)
    return need


def link_of(kind, m, turn):
    name = TREES[kind][m][1]
    sign = {"+": 1, "-": -1, "s": turn, "o": -turn}[name[1]]
    return name[0], sign


RATE, HOP, AHEAD = 46.5, 2.2, 1.5
ORDER = (
    ("mix", 4, "D", -1),
    ("pj", 1, "D", -1),
    ("mix", 0, "A", 1),
    ("gu", 8, "E", -1),
    ("dn", 3, "A", 1),
    ("mix", 2, "D", 1),
    ("mix", 3, "A", 1),
    ("mix", 1, "E", -1),
    ("mix", 5, "A", -1),
    ("pj", 0, "D", 1),
    ("gu", 5, "A", -1),
    ("gu", 1, "D", 1),
    ("gu", 4, "A", 1),
    ("gu", 7, "D", 1),
    ("gu", 3, "E", -1),
    ("gu", 2, "A", -1),
    ("gu", 9, "D", -1),
    ("dn", 1, "E", 1),
    ("gu", 6, "E", -1),
    ("dn", 0, "D", 1),
    ("gu", 0, "A", -1),
    ("dn", 2, "E", 1),
    ("gu", 10, "E", 1),
    ("dn", 5, "D", -1),
    ("dn", 4, "E", 1),
)
LEAD = {("A", 6): 7.5, ("C", 4): 2.5, ("D", 2): 0.5, ("D", 3): 8.0, ("D", 1): 9.5, ("D", 5): 3, ("D", 6): 12, ("A", 0): 2.5, ("D", 7): 10.0, ("D", 0): 4.0, ("A", 7): 12, ("C", 1): 6.0, ("C", 6): 0.5, ("A", 1): -1.0, ("A", 9): -2.5, ("A", 4): 1.5, ("A", 2): 12, ("A", 3): 6.0, ("C", 0): 7.5, ("D", 4): 6.0, ("C", 5): 8.5, ("C", 7): -2.0, ("C", 3): -2.5, ("A", 5): 1, ("C", 2): 5.0, ("A", 8): 12, ("E", 7): 8, ("E", 11): -2, ("E", 8): -1.5, ("E", 0): -0.5, ("E", 2): -2.5, ("E", 9): 3.0, ("E", 3): 12, ("E", 5): 0.5, ("E", 4): -3, ("E", 1): -3, ("E", 12): 2.5, ("E", 6): 12}


def plan(chunks, comps, own_after, rate=RATE, hop=HOP, issue=0.04, ahead=AHEAD):
    links = {(a, s): 0.0 for a in "xyz" for s in (1, -1)}
    arrive, waited, sent, ops, done, t = {}, set(), set(), [], {}, 0.0
    every = [(c, m) for c in range(len(chunks)) for m in range(len(TREES[chunks[c][0]]))]
    every.sort(key=lambda e: (e[0] - LEAD.get((chunks[e[0]][0], e[1]), 0.0), e[1]))
    log = []

    def wait(pairs):
        for pair in pairs:
            if pair not in waited:
                waited.add(pair)
                ops.append(("wait", *pair))

    while True:
        best = None
        for c, m in every:
            kind, turn, size = chunks[c]
            if (c, m) in sent:
                continue
            needs = [(c, k) for k in needs_of(kind, m, turn)]
            link = link_of(kind, m, turn)
            here = bool(needs) or c not in own_after or own_after[c] in done
            if here and all(arrive.get(k, 1e9) <= t for k in needs) and links[link] <= t + ahead:
                best = (c, m, needs, link, size * TREES[kind][m][2])
                break
        if best is not None:
            c, m, needs, link, size = best
            wait(needs)
            ops.append(("send", c, m))
            sent.add((c, m))
            t += issue
            links[link] = max(t, links[link]) + size / rate / 1000.0
            arrive[c, m] = links[link] + hop
            continue
        soon = []
        for k, (us, of_chunks, of_comps) in enumerate(comps):
            if k in done:
                continue
            pairs = [(c, m) for c, m in every if c in of_chunks]
            ready = max([arrive.get(q, 1e9) for q in pairs] + [done.get(b, 1e9) + lag for b, lag in of_comps] + [0.0])
            if ready <= t:
                wait(pairs)
                ops.append(("comp", k))
                log.append((round(t, 1), k))
                t += us
                done[k] = t
                break
            if ready < 1e8:
                soon.append(ready)
        else:
            later = [a for a in arrive.values() if a > t] + [b - ahead for b in links.values() if b - ahead > t] + soon
            if not later:
                break
            t = min(later) + 1e-6
    wait(every)
    return ops, t, log, arrive


def list_of_chunks():
    chunks, where = [("A", 1, 4096)], [("sc", 0, 128)]
    for name, i, kind, turn in ORDER:
        width = UNIT // 2 if (name, i) == LAST else UNIT
        chunks.append((kind, turn, 64 * width * 2))
        where.append((name, i, width))
    return chunks, where


LAST = ("dn", 5)
CHUNKS, WHERE = list_of_chunks()
CHUNK_OF = {(name, i): c for c, (name, i, _) in enumerate(WHERE)}
ROWS = 256
DOWN = ((0, 2), (2, 2))
PASSED = 4


def list_of_blocks():
    names, comps, number = [], [], {}

    def add(name, us, chunks=(), after=()):
        number[name] = len(names)
        names.append(name)
        comps.append((us, {CHUNK_OF[c] for c in chunks}, [(number[b], lag) for b, lag in after]))

    add(("cast", "gu"), 0.5)
    add(("cast", "rest"), 0.4)
    add(("norm",), 1.3)
    add(("scales",), 0.3, [("sc", 0)])
    for k in range(6):
        add(("mix", k), 1.25, [("mix", k)], [(("norm",), 4.0), (("scales",), 0.0)])
    for g in range(2):
        add(("conv", g), 1.3, [], [(("mix", 3 * g + i), 0.0) for i in range(3)] + [(("conv", 0), 0.0)] * g)
    add(("proj", 0), 1.3, [("pj", 0), ("pj", 1)], [(("conv", 0), 0.0), (("conv", 1), 0.0)])
    add(("proj", 1), 1.3, [], [(("proj", 0), 0.0)])
    add(("first",), 2.8, [], [(("proj", 1), 0.0), (("proj", 0), 2.0)])
    for k in range(11):
        add(("gu", k), 1.75, [("gu", k)], [(("first",), 2.2)])
    for j, (first, count) in enumerate(DOWN):
        units = range(first, first + count)
        before = [(("gu", k), 0.0) for u in units for k in (2 * u, 2 * u + 1)] + [(("down", j - 1), 0.0)] * (j > 0)
        add(("down", j), 2.4, [("dn", u) for u in units], before)
    add(("give",), 0.3, [], [(("down", len(DOWN) - 1), 0.0)])
    add(("base",), 0.9, [], [(("give",), 4.2)])
    add(("near", 4), 1.7, [("dn", 4)], [(("base",), 0.0), (("gu", 8), 2.0), (("gu", 9), 2.0)])
    add(("near", 5), 1.9, [("dn", 5)], [(("near", 4), 0.0), (("gu", 10), 2.0)])
    own_after = {}
    for (name, _), c in CHUNK_OF.items():
        if name in ("gu", "pj", "dn"):
            own_after[c] = number["cast", "gu" if name == "gu" else "rest"]
    return names, comps, own_after


def place():
    rep, fs = lax.axis_index("rep"), lax.axis_index("fs")
    tp = lax.axis_index("tp")
    x, y, zl = lax.rem(fs, 4), lax.rem(fs // 4, 4), fs // 16
    z = rep * 2 + zl
    xs = {n: lax.rem(x + 4 + n, 4) for n in (-1, 1, 2)} | {0: x}
    ys = {n: lax.rem(y + 4 + n, 4) for n in (-1, 1, 2)} | {0: y}
    near = {}
    for sign in (1, -1):
        near["x", sign] = (rep, zl * 16 + y * 4 + xs[sign], tp)
        near["y", sign] = (rep, zl * 16 + ys[sign] * 4 + x, tp)
        zn = lax.rem(z + 4 + sign, 4)
        near["z", sign] = (zn // 2, lax.rem(zn, 2) * 16 + y * 4 + x, tp)
    return xs, ys, {0: zl, 1: 1 - zl}, near, (rep, fs, 1 - tp), tp


def carried(kind, m, turn, arriving):
    sent = {
        "A": (
            (0, 0, 0),
            (0, 0, 0),
            (0, 0, -turn),
            (0, 0, None),
            (0, 0, None),
            (0, 0, None),
            (0, -turn, None),
            (0, -turn, None),
            (0, turn, None),
            (0, 2, None),
        ),
        "D": (
            (0, 0, 0),
            (None, 0, 0),
            (None, 0, 0),
            (None, -turn, 0),
            (None, None, 0),
            (None, None, 0),
            ("plane0", None, -1),
            ("plane1", None, 1),
        ),
        "E": (
            (0, 0, 0),
            (0, 0, 0),
            (0, 0, -turn),
            (0, 0, None),
            (0, 0, None),
            (0, 0, 0),
            (0, 0, -1),
            (0, 0, 1),
            (0, 0, 2),
            (0, -turn, None),
            (0, -turn, None),
            (0, turn, None),
            (0, 2, None),
        ),
        "C": (
            (0, 0, 0),
            (None, 0, 0),
            (None, 0, 0),
            (None, 0, -turn),
            (None, 0, None),
            (None, 0, None),
            ("plane0", -1, None),
            ("plane1", 1, None),
        ),
    }[kind][m]
    if not arriving:
        return sent
    link, sign = link_of(kind, m, turn)
    z, y, x = sent

    def back(v, n):
        v = v - n
        return v + 4 if v < -1 else v - 4 if v > 2 else v

    if link == "x":
        x = back(x, sign)
    elif link == "y":
        y = back(y, sign)
    else:
        z = 1 - z
    return z, y, x


def mega_kernel(
    ops, names, tokens, in_w, val_w, out_w, gate_w, up_w, pj_w, dn_w, *rest,
):
    small_in, out, small = rest[:15], rest[15], rest[16:31]
    run_kernel(ops, names, tokens, in_w, val_w, out_w, gate_w, up_w, pj_w, dn_w, small_in, small, out, *rest[31:])


def run_kernel(
    ops, names, tokens, in_w, val_w, out_w, gate_w, up_w, pj_w, dn_w, small_in, small, out, mix, pj, gu, dn, sc, tok, rows, gates, conv, square, acc, hidden, psend, precv, sqrecv, sv_mix,
    sv_gu, sv_pj, sv_dn, hidden_other, dn_other, own_sem, send_sem, recv_sem, side_send, side_recv,
):
    f32, bf16 = jnp.float32, jnp.bfloat16
    (in_s, val_s, out_s, gate_s, up_s, pj_s, dn_s, mix_gain, ffn_gain, mix_taps, conv_gain, gate_taps, up_taps, gate_bias,
     up_bias) = small
    xs, ys, zs, near, other, tp = place()
    bufs = {"mix": mix, "pj": pj, "gu": gu, "dn": dn, "sc": sc}
    x, y, zl = xs[0], ys[0], zs[0]
    mine = pl.multiple_of(tp * 512, 512)
    yours = pl.multiple_of((1 - tp) * 512, 512)
    mix_f32 = [acc.at[64 * i : 64 * i + 64, 0:512] for i in range(3)]
    gu_f32 = [acc.at[192 + 64 * i : 256 + 64 * i, 0:1408] for i in range(2)]
    pj_f32, dn_f32 = acc.at[320:384, 0:512], acc.at[384:448, 0:1408]
    own = [
        pltpu.make_async_copy(src, dst, own_sem.at[i])
        for i, (src, dst) in enumerate(
            zip(
                (in_w, val_w, out_w, gate_w, up_w, pj_w, dn_w, tokens),
                (*mix_f32, *gu_f32, pj_f32, dn_f32, tok),
            )
        )
    ]
    small_copies = [pltpu.make_async_copy(src, dst, own_sem.at[8 + i]) for i, (src, dst) in enumerate(zip(small_in, small))]
    for copy in own[:3] + small_copies[:7] + own[3:] + small_copies[7:]:
        copy.start()
    barrier = pltpu.get_barrier_semaphore()
    for device in [*near.values(), other]:
        pl.semaphore_signal(barrier, inc=1, device_id=device, device_id_type=MESH)
    sc[zl, y, x] = jnp.zeros((8, 128), f32)
    for copy in small_copies[:7]:
        copy.wait()
    for i, ref in enumerate((in_s, val_s, out_s, gate_s, up_s, pj_s, dn_s)):
        sc[zl, y, x, i : i + 1, : ref.shape[0]] = ref[...].reshape(1, -1)
    for i in range(3):
        own[i].wait()
        for g in range(2):
            mix[3 * g + i, zl, y, x] = mix_f32[i][:, 256 * g : 256 * g + 256].astype(bf16)
    pl.semaphore_wait(barrier, 7)

    def block_cast(which):
        if which == "gu":
            for i in range(2):
                own[3 + i].wait()
                for k in range(11):
                    gu[k, zl, y, x, :, 128 * i : 128 * i + 128] = gu_f32[i][:, 128 * k : 128 * k + 128].astype(bf16)
        else:
            own[5].wait()
            pj[zl, y, x] = pj_f32[...].astype(bf16)
            own[6].wait()
            dn[zl, y, x] = dn_f32[...].astype(bf16)
            for unit in passed:
                pass_on(unit, (0, 0, 0))

    def part(c, at):
        name, i, width = WHERE[c]
        z, y, x = at
        z = slice(None) if z is None else int(z[-1]) if isinstance(z, str) else zs[z]
        y = slice(None) if y is None else ys[y]
        x = slice(None) if x is None else xs[x]
        ref = bufs[name]
        if name in ("mix", "gu"):
            return ref.at[i, z, y, x]
        if name == "sc":
            return ref.at[z, y, x]
        return ref.at[z, y, x, :, i * UNIT : i * UNIT + width]

    def all_of(c, m):
        kind, turn, _ = CHUNKS[c]
        ends, region = ENDS[kind]
        return region if m in ends else carried(kind, m, turn, True)

    def copy_of(c, m, arriving):
        kind, turn, _ = CHUNKS[c]
        ref = part(c, all_of(c, m) if arriving else carried(kind, m, turn, False))
        return pltpu.make_async_remote_copy(
            src_ref=ref,
            dst_ref=ref,
            send_sem=send_sem.at[c],
            recv_sem=recv_sem.at[c, slot_of(kind, m)],
            device_id=near[link_of(kind, m, turn)],
            device_id_type=MESH,
        )

    def to_other(src, dst, i):
        return pltpu.make_async_remote_copy(
            src_ref=src, dst_ref=dst, send_sem=side_send.at[i], recv_sem=side_recv.at[i], device_id=other, device_id_type=MESH
        )

    def normed(values, gain):
        return (values * lax.rsqrt(jnp.mean(values * values, axis=1, keepdims=True) + epsilon) * gain[...].reshape(1, -1)).astype(bf16)

    def shifted(values, before):
        both = jnp.concatenate([before, values], axis=0)
        return pltpu.roll(both, 1, 0)[8:], pltpu.roll(both, 2, 0)[8:]

    def dot_nt(left, right):
        return lax.dot_general(left, right, (((1,), (1,)), ((), ())), preferred_element_type=f32)

    def spread(row, width, group):
        total = jnp.zeros((1, 128), f32)
        lane = lax.broadcasted_iota(jnp.int32, (1, 128), 1)
        for s in range(group * 128 // width, min(31, (group * 128 + 127) // width) + 1):
            at = s * width - group * 128
            line = sc[s // 16, s // 4 % 4, s % 4, row : row + 1, :]
            if at % 128:
                line = pltpu.roll(line, at % 128, 1)
            total = jnp.where((lane >= at) & (lane < at + width), line, total)
        return total

    def rows_copy(to_send, first, count, i):
        at = pl.ds((mine if to_send else yours) + first, count)
        return to_other(rows.at[at], rows.at[at], i)

    send_rows, recv_rows = (rows_copy(b, 0, 512, 0) for b in (True, False))
    send_again, recv_again = ([rows_copy(b, 128 * q, 128, 9 + q) for q in range(4)] for b in (True, False))
    send_parts = [to_other(psend.at[pl.ds(256 * q, 256)], precv.at[pl.ds(256 * q, 256)], (1, 3)[q]) for q in range(2)]
    send_sums = to_other(psend, precv, 4)
    send_square = to_other(square.at[pl.ds(yours, 512)], sqrecv, 2)
    def lanes_of(unit):
        return slice(UNIT * unit, min(UNIT * unit + UNIT, 1408)), slice(UNIT * (unit - PASSED), min(UNIT * unit + UNIT, 1408) - UNIT * PASSED)

    send_hidden = {}
    for unit in (4, 5):
        here, there = lanes_of(unit)
        send_hidden[unit] = to_other(hidden.at[pl.ds(yours, 512), here], hidden_other.at[:, there], 1 + unit)
    passed = {}
    for unit in (4, 5):
        here, there = lanes_of(unit)
        passed[unit] = to_other(dn.at[:, :, :, :, here], dn_other.at[:, :, :, :, there], 3 + unit)
    seen = set()

    def pass_on(unit, at):
        z, y, x = at
        z = slice(None) if z is None else int(z[-1]) if isinstance(z, str) else zs[z]
        y = slice(None) if y is None else ys[y]
        x = slice(None) if x is None else xs[x]
        ref = dn_other.at[z, y, x, :, lanes_of(unit)[1]]
        to_other(part(CHUNK_OF["dn", unit], at), ref, 3 + unit).start()

    def block_norm():
        own[7].wait()
        for copy in small_copies[7:]:
            copy.wait()

        @pl.loop(0, 512, step=64)
        def _(r):
            at = pl.multiple_of(r, 64)
            rows[pl.ds(mine + at, 64), :] = normed(tok[pl.ds(at, 64), :].astype(f32), mix_gain)

        send_rows.start()

    def block_scales():
        for k in range(6):
            for i in range(2):
                sv_mix[k, :, 128 * i : 128 * i + 128] = spread(k % 3, 16, k // 3 * 2 + i)
        for k in range(11):
            sv_gu[k, :, :128] = spread(3, 44, k)
            sv_gu[k, :, 128:] = spread(4, 44, k)
        for k in range(16):
            sv_pj[k // 2, :, 128 * (k % 2) : 128 * (k % 2) + 128] = spread(5, 64, k)
            sv_dn[k // 2, :, 128 * (k % 2) : 128 * (k % 2) + 128] = spread(6, 64, k)

    def block_mix(k):
        if "rows" not in seen:
            seen.add("rows")
            recv_rows.wait_recv()

        for r in range(0, 1024, ROWS):
            at = pl.ds(r, ROWS)
            weight = mix[k].reshape(2048, 256)
            gates[k, at, :] = (jnp.dot(rows[at, :], weight, preferred_element_type=f32) * sv_mix[k]).astype(bf16)

    def block_conv(g):
        cols = slice(256 * g, 256 * g + 256)
        taps, gain = mix_taps[:, cols], conv_gain[cols].reshape(1, 256)

        def body(i, before):
            at = pl.ds(pl.multiple_of(i * 128, 128), 128)
            value = gates[3 * g, at, :].astype(f32) * gates[3 * g + 1, at, :].astype(f32)
            one, two = shifted(value, before)
            total = taps[0:1] * two + taps[1:2] * one + taps[2:3] * value
            done = (gates[3 * g + 2, at, :].astype(f32) * total).astype(bf16).astype(f32)
            conv[at, cols] = (done * gain).astype(bf16)
            squares = jnp.broadcast_to(jnp.sum(done * done, axis=1, keepdims=True), (128, 128))
            square[at, :] = squares if g == 0 else square[at, :] + squares
            return value[-8:]

        lax.fori_loop(0, 8, body, jnp.zeros((8, 256), f32))
        if g == 1:
            send_square.start()

    def block_proj(half):
        for q in range(2):
            here = pl.ds(256 * q, 256)
            rows_at = pl.ds((yours if half == 0 else mine) + 256 * q, 256)
            for n in range(8):
                weight = pj[n // 4, n % 4].reshape(256, 512)
                part_sum = dot_nt(conv[rows_at, :], weight) * sv_pj[n]
                cols = slice(n * 256, n * 256 + 256)
                if half == 0:
                    psend[here, cols] = part_sum.astype(bf16)
                else:
                    acc[rows_at, cols] = part_sum
            if half == 0:
                send_parts[q].start()

    def block_first():
        send_square.wait_recv()
        send_rows.wait_send()
        for q in range(4):
            if q % 2 == 0:
                send_parts[q // 2].wait_recv()

            @pl.loop(128 * q, 128 * q + 128, step=64)
            def _(r):
                at = pl.ds(pl.multiple_of(r, 64), 64)
                there = pl.ds(pl.multiple_of(mine + r, 64), 64)
                squares = square[there, :1] + sqrecv[at, :1]
                summed = (acc[there, :] + precv[at, :].astype(f32)) * lax.rsqrt(squares / 1024 + epsilon)
                first = (tok[at, :].astype(f32) + summed).astype(bf16)
                tok[at, :] = first
                rows[there, :] = normed(first.astype(f32), ffn_gain)

            send_again[q].start()

    def block_gu(k):
        if "rows2" not in seen:
            seen.add("rows2")
            for copy in recv_again:
                copy.wait_recv()
        cols = slice(128 * k, 128 * k + 128)

        def body(i, before):
            at = pl.ds(i * ROWS, ROWS)
            weight = gu[k].reshape(2048, 256)
            pre = (jnp.dot(rows[at, :], weight, preferred_element_type=f32) * sv_gu[k]).astype(bf16).astype(f32)
            one, two = shifted(pre, before)
            acts = []
            for j, (taps, bias) in enumerate(((gate_taps, gate_bias), (up_taps, up_bias))):
                half, t = slice(128 * j, 128 * j + 128), taps[:, cols]
                acts.append(t[0:1] * two[:, half] + t[1:2] * one[:, half] + t[2:3] * pre[:, half] + bias[cols].reshape(1, 128))
            half = 0.5 * acts[0]
            hidden[at, cols] = ((half + half * jnp.tanh(half)) * acts[1]).astype(bf16)
            return pre[-8:]

        before = jnp.zeros((8, 256), f32)
        for i in range(1024 // ROWS):
            before = body(i, before)
        seen.add(k)
        if k == 10:
            send_hidden[5].start()
        elif k in (8, 9) and {8, 9} <= seen:
            send_hidden[4].start()

    def block_down(j):
        first, count = DOWN[j]
        width = sum(WHERE[CHUNK_OF["dn", u]][2] for u in range(first, first + count))
        lanes = slice(UNIT * first, UNIT * first + width)

        def product(start, count, n):
            weight = dn[n // 4, n % 4, :, :, lanes].reshape(256, width)
            return dot_nt(hidden[pl.ds(start, count), lanes], weight)

        def sweep(start, count, store):
            for n in range(8):
                store(n, slice(n * 256, n * 256 + 256), pl.ds(start, count), product(start, count, n))

        def store(n, cols, at, value):
            acc[at, cols] = value if j == 0 else acc[at, cols] + value

        sweep(0, 1024, store)


    def block_give():
        for copy in send_parts:
            copy.wait_send()

        @pl.loop(0, 512, step=64)
        def _(r):
            at, there = pl.ds(pl.multiple_of(r, 64), 64), pl.ds(pl.multiple_of(yours + r, 64), 64)
            for n in range(8):
                cols = slice(256 * n, 256 * n + 256)
                psend[at, cols] = (acc[there, cols] * sv_dn[n]).astype(bf16)

        send_sums.start()

    def block_base():
        send_sums.wait_recv()

        @pl.loop(0, 512, step=64)
        def _(r):
            at, there = pl.ds(pl.multiple_of(r, 64), 64), pl.ds(pl.multiple_of(mine + r, 64), 64)
            for n in range(8):
                cols = slice(256 * n, 256 * n + 256)
                summed = acc[there, cols] * sv_dn[n] + precv[at, cols].astype(f32)
                acc[there, cols] = tok[at, cols].astype(f32) + summed

    def block_near(unit):
        send_hidden[unit].wait_recv()
        passed[unit].wait_recv()
        here, there = lanes_of(unit)
        width = here.stop - here.start
        at = pl.ds(mine, 512)
        left = jnp.concatenate([hidden[at, here], hidden_other[:, there]], axis=1)
        for n in range(8):
            cols = slice(256 * n, 256 * n + 256)
            weights = [ref[n // 4, n % 4, :, :, lanes].reshape(256, width) for ref, lanes in ((dn, here), (dn_other, there))]
            value = acc[at, cols] + dot_nt(left, jnp.concatenate(weights, axis=1)) * sv_dn[n]
            if unit == 5:
                out[:, cols] = value.astype(bf16)
            else:
                acc[at, cols] = value

    blocks = {
        "cast": block_cast,
        "norm": block_norm, "scales": block_scales, "mix": block_mix, "conv": block_conv, "proj": block_proj,
        "first": block_first, "gu": block_gu, "down": block_down, "give": block_give, "base": block_base,
        "near": block_near,
    }
    gone, met = set(), set()

    def sent_by(end):
        for c, (kind, _, _) in enumerate(CHUNKS):
            entries = range(len(TREES[kind]))
            if c not in gone and all(("send", c, m) in ops[:end] for m in entries):
                gone.add(c)
                for m in entries:
                    copy_of(c, m, False).wait_send()

    for step, op in enumerate(ops):
        if op[0] == "send":
            copy_of(op[1], op[2], False).start()
        elif op[0] == "wait":
            c, m = op[1:]
            if (c, slot_of(CHUNKS[c][0], m)) in met:
                continue
            met.add((c, slot_of(CHUNKS[c][0], m)))
            copy_of(c, m, True).wait_recv()
            name, unit, _ = WHERE[c]
            if name == "dn" and unit in passed:
                pass_on(unit, all_of(c, m))
        else:
            name, *index = names[op[1]]
            if name == "base":
                sent_by(step - 30)
            blocks[name](*index)
    sent_by(len(ops))
    send_square.wait_send()
    send_sums.wait_send()
    for copy in send_again:
        copy.wait_send()
    for unit in passed:
        send_hidden[unit].wait_send()
        passed[unit].wait_send()


def mega(*args):
    names, comps, own_after = list_of_blocks()
    ops, _, _, _ = plan(CHUNKS, comps, own_after)
    f32, bf16 = jnp.float32, jnp.bfloat16
    hbm, vmem = pl.BlockSpec(memory_space=pl.ANY), pl.BlockSpec(memory_space=pltpu.VMEM)
    dma = pltpu.SemaphoreType.DMA
    return pl.pallas_call(
        lambda *refs: mega_kernel(ops, names, *refs),
        out_shape=pltpu.VMEM((512, 2048), bf16),
        in_specs=[hbm] * 23,
        out_specs=vmem,
        scratch_shapes=[pltpu.VMEM(a.shape, f32) for a in args[8:]] + [
            pltpu.VMEM((6, 2, 4, 4, 64, 256), bf16),
            pltpu.VMEM((2, 4, 4, 64, 512), bf16),
            pltpu.VMEM((11, 2, 4, 4, 64, 256), bf16),
            pltpu.VMEM((2, 4, 4, 64, 1408), bf16),
            pltpu.VMEM((2, 4, 4, 8, 128), f32),
            pltpu.VMEM((512, 2048), bf16),
            pltpu.VMEM((1024, 2048), bf16),
            pltpu.VMEM((6, 1024, 256), bf16),
            pltpu.VMEM((1024, 512), bf16),
            pltpu.VMEM((1024, 128), f32),
            pltpu.VMEM((1024, 2048), f32),
            pltpu.VMEM((1024, 1408), bf16),
            pltpu.VMEM((512, 2048), bf16),
            pltpu.VMEM((512, 2048), bf16),
            pltpu.VMEM((512, 128), f32),
            pltpu.VMEM((6, 1, 256), f32),
            pltpu.VMEM((11, 1, 256), f32),
            pltpu.VMEM((8, 1, 256), f32),
            pltpu.VMEM((8, 1, 256), f32),
            pltpu.VMEM((512, 384), bf16),
            pltpu.VMEM((2, 4, 4, 64, 384), bf16),
            dma((23,)),
            dma((len(CHUNKS),)),
            dma((len(CHUNKS), 7)),
            dma((13,)),
            dma((13,)),
        ],
        compiler_params=pltpu.CompilerParams(collective_id=0, has_side_effects=True, vmem_limit_bytes=58 * 1024 * 1024),
    )(*args)


def to_hbm(values):
    def kernel(src, dst, sem):
        copies = [
            pltpu.make_async_copy(src.at[128 * q : 128 * q + 128], dst.at[128 * q : 128 * q + 128], sem.at[q])
            for q in range(4)
        ]
        for copy in copies:
            copy.start()
        for copy in copies:
            copy.wait()

    return pl.pallas_call(
        kernel,
        out_shape=jax.ShapeDtypeStruct(values.shape, values.dtype),
        in_specs=[pl.BlockSpec(memory_space=pltpu.VMEM)],
        out_specs=pl.BlockSpec(memory_space=pl.ANY),
        scratch_shapes=[pltpu.SemaphoreType.DMA((4,))],
        compiler_params=pltpu.CompilerParams(vmem_limit_bytes=4 * 1024 * 1024),
    )(values)


def local(
    tokens, mix_gain, out_gate_w, in_gate_w, value_w, out_gate_scale, in_gate_scale, value_scale, mix_taps, conv_gain,
    out_proj_w, proj_scale, ffn_gain, gate_w, up_w, gate_scale, up_scale, gate_taps, up_taps, gate_bias, up_bias, down_w,
    down_scale,
):
    return to_hbm(mega(
        tokens[0], in_gate_w, value_w, out_gate_w, gate_w, up_w, out_proj_w.T, down_w.T, in_gate_scale, value_scale,
        out_gate_scale, gate_scale, up_scale, proj_scale, down_scale, mix_gain, ffn_gain, mix_taps, conv_gain, gate_taps,
        up_taps, gate_bias, up_bias,
    ))[None]


def solution(mesh):
    placed = (
        P(("rep", "fs"), "tp", None), P(), P("fs", "tp"), P("fs", "tp"), P("fs", "tp"), P(("tp", "fs")), P(("tp", "fs")),
        P(("tp", "fs")), P(None, "tp"), P("tp"), P("tp", "fs"), P("fs"), P(), P("fs", "tp"), P("fs", "tp"), P(("tp", "fs")),
        P(("tp", "fs")), P(None, "tp"), P(None, "tp"), P("tp"), P("tp"), P("tp", "fs"), P("fs"),
    )
    return jax.shard_map(
        local, mesh=mesh, in_specs=placed, out_specs=P(("rep", "fs"), "tp", None), check_vma=False
    )
```

```python
import jax
import jax.numpy as jnp
from jax import lax
from jax.experimental import pallas as pl
from jax.experimental.pallas import tpu as pltpu
from jax.sharding import PartitionSpec as P

epsilon = 1e-06
MESH = pl.DeviceIdType.MESH
UNIT = 256
TURNED = "so"

TREES = {
    "A": (
        ((), "x+", 1),
        ((), "x-", 1),
        ("s01", "xs", 1),
        ((0, 1, 2), "y+", 4),
        ((0, 1, 2), "y-", 4),
        ((0, 1, 2), "zs", 4),
        ("s34", "ys", 4),
        ("s34", "zo", 4),
        ("o34", "zo", 4),
        ((6,), "zs", 4),
    ),
    "D": (
        ((), "zs", 1),
        ((0,), "y+", 2),
        ((0,), "y-", 2),
        ("s12", "ys", 2),
        ((1, 2, 3), "x+", 8),
        ((1, 2, 3), "x-", 8),
        ((4,), "x+", 4),
        ((5,), "x-", 4),
    ),
    "E": (
        ((), "x+", 1),
        ((), "x-", 1),
        ("s01", "xs", 1),
        ((0, 1, 2), "y+", 4),
        ((0, 1, 2), "y-", 4),
        ((), "zs", 1),
        ((0,), "zs", 1),
        ((1,), "zs", 1),
        ((2,), "zs", 1),
        ("s34", "ys", 4),
        ("s34", "zo", 4),
        ("o34", "zo", 4),
        ((9,), "zs", 4),
    ),
    "C": (
        ((), "zs", 1),
        ((0,), "x+", 2),
        ((0,), "x-", 2),
        ("s12", "xs", 2),
        ((1, 2, 3), "y+", 8),
        ((1, 2, 3), "y-", 8),
        ((4,), "y+", 4),
        ((5,), "y-", 4),
    ),
}


ENDS = {
    "A": ((5, 7, 8, 9), (1, None, None)),
    "E": ((5, 6, 7, 8, 10, 11, 12), (1, None, None)),
    "D": ((6, 7), (None, None, 2)),
    "C": ((6, 7), (None, 2, None)),
}


def slot_of(kind, m):
    ends = ENDS[kind][0]
    return 0 if m in ends else 1 + [k for k in range(len(TREES[kind])) if k not in ends].index(m)


def needs_of(kind, m, turn):
    need = TREES[kind][m][0]
    if isinstance(need, str):
        first, second = int(need[1]), int(need[2])
        return (first if (turn > 0) == (need[0] == "s") else second,)
    return need


def link_of(kind, m, turn):
    name = TREES[kind][m][1]
    sign = {"+": 1, "-": -1, "s": turn, "o": -turn}[name[1]]
    return name[0], sign


RATE, HOP, AHEAD = 46.5, 2.2, 1.5
ORDER = (
    ("mix", 4, "D", -1),
    ("pj", 1, "D", -1),
    ("mix", 0, "A", 1),
    ("gu", 8, "E", -1),
    ("dn", 3, "A", 1),
    ("mix", 2, "D", 1),
    ("mix", 3, "A", 1),
    ("mix", 1, "E", -1),
    ("mix", 5, "A", -1),
    ("pj", 0, "D", 1),
    ("gu", 5, "A", -1),
    ("gu", 1, "D", 1),
    ("gu", 4, "A", 1),
    ("gu", 7, "D", 1),
    ("gu", 3, "E", -1),
    ("gu", 2, "A", -1),
    ("gu", 9, "D", -1),
    ("dn", 1, "E", 1),
    ("gu", 6, "E", -1),
    ("dn", 0, "D", 1),
    ("gu", 0, "A", -1),
    ("dn", 2, "E", 1),
    ("gu", 10, "E", 1),
    ("dn", 5, "D", -1),
    ("dn", 4, "E", 1),
)
LEAD = {("A", 6): 7.5, ("C", 4): 2.5, ("D", 2): 0.5, ("D", 3): 8.0, ("D", 1): 9.5, ("D", 5): 3, ("D", 6): 12, ("A", 0): 2.5, ("D", 7): 10.0, ("D", 0): 4.0, ("A", 7): 12, ("C", 1): 6.0, ("C", 6): 0.5, ("A", 1): -1.0, ("A", 9): -2.5, ("A", 4): 1.5, ("A", 2): 12, ("A", 3): 6.0, ("C", 0): 7.5, ("D", 4): 6.0, ("C", 5): 8.5, ("C", 7): -2.0, ("C", 3): -2.5, ("A", 5): 1, ("C", 2): 5.0, ("A", 8): 12, ("E", 7): 8, ("E", 11): -2, ("E", 8): -1.5, ("E", 0): -0.5, ("E", 2): -2.5, ("E", 9): 3.0, ("E", 3): 12, ("E", 5): 0.5, ("E", 4): -3, ("E", 1): -3, ("E", 12): 2.5, ("E", 6): 12}


def plan(chunks, comps, own_after, rate=RATE, hop=HOP, issue=0.04, ahead=AHEAD):
    links = {(a, s): 0.0 for a in "xyz" for s in (1, -1)}
    arrive, waited, sent, ops, done, t = {}, set(), set(), [], {}, 0.0
    every = [(c, m) for c in range(len(chunks)) for m in range(len(TREES[chunks[c][0]]))]
    every.sort(key=lambda e: (e[0] - LEAD.get((chunks[e[0]][0], e[1]), 0.0), e[1]))
    log = []

    def wait(pairs):
        for pair in pairs:
            if pair not in waited:
                waited.add(pair)
                ops.append(("wait", *pair))

    while True:
        best = None
        for c, m in every:
            kind, turn, size = chunks[c]
            if (c, m) in sent:
                continue
            needs = [(c, k) for k in needs_of(kind, m, turn)]
            link = link_of(kind, m, turn)
            here = bool(needs) or c not in own_after or own_after[c] in done
            if here and all(arrive.get(k, 1e9) <= t for k in needs) and links[link] <= t + ahead:
                best = (c, m, needs, link, size * TREES[kind][m][2])
                break
        if best is not None:
            c, m, needs, link, size = best
            wait(needs)
            ops.append(("send", c, m))
            sent.add((c, m))
            t += issue
            links[link] = max(t, links[link]) + size / rate / 1000.0
            arrive[c, m] = links[link] + hop
            continue
        soon = []
        for k, (us, of_chunks, of_comps) in enumerate(comps):
            if k in done:
                continue
            pairs = [(c, m) for c, m in every if c in of_chunks]
            ready = max([arrive.get(q, 1e9) for q in pairs] + [done.get(b, 1e9) + lag for b, lag in of_comps] + [0.0])
            if ready <= t:
                wait(pairs)
                ops.append(("comp", k))
                log.append((round(t, 1), k))
                t += us
                done[k] = t
                break
            if ready < 1e8:
                soon.append(ready)
        else:
            later = [a for a in arrive.values() if a > t] + [b - ahead for b in links.values() if b - ahead > t] + soon
            if not later:
                break
            t = min(later) + 1e-6
    wait(every)
    return ops, t, log, arrive


def list_of_chunks():
    chunks, where = [("A", 1, 4096)], [("sc", 0, 128)]
    for name, i, kind, turn in ORDER:
        width = UNIT // 2 if (name, i) == LAST else UNIT
        chunks.append((kind, turn, 64 * width * 2))
        where.append((name, i, width))
    return chunks, where


LAST = ("dn", 5)
CHUNKS, WHERE = list_of_chunks()
CHUNK_OF = {(name, i): c for c, (name, i, _) in enumerate(WHERE)}
ROWS = 256
DOWN = ((0, 2), (2, 2))
PASSED = 4


def list_of_blocks():
    names, comps, number = [], [], {}

    def add(name, us, chunks=(), after=()):
        number[name] = len(names)
        names.append(name)
        comps.append((us, {CHUNK_OF[c] for c in chunks}, [(number[b], lag) for b, lag in after]))

    add(("cast", "gu"), 0.5)
    add(("cast", "rest"), 0.4)
    add(("norm",), 1.3)
    add(("scales",), 0.3, [("sc", 0)])
    for k in range(6):
        add(("mix", k), 1.25, [("mix", k)], [(("norm",), 4.0), (("scales",), 0.0)])
    for g in range(2):
        add(("conv", g), 1.3, [], [(("mix", 3 * g + i), 0.0) for i in range(3)] + [(("conv", 0), 0.0)] * g)
    add(("proj", 0), 1.3, [("pj", 0), ("pj", 1)], [(("conv", 0), 0.0), (("conv", 1), 0.0)])
    add(("proj", 1), 1.3, [], [(("proj", 0), 0.0)])
    add(("first",), 2.8, [], [(("proj", 1), 0.0), (("proj", 0), 2.0)])
    for k in range(11):
        add(("gu", k), 1.75, [("gu", k)], [(("first",), 2.2)])
    for j, (first, count) in enumerate(DOWN):
        units = range(first, first + count)
        before = [(("gu", k), 0.0) for u in units for k in (2 * u, 2 * u + 1)] + [(("down", j - 1), 0.0)] * (j > 0)
        add(("down", j), 2.4, [("dn", u) for u in units], before)
    add(("give",), 0.3, [], [(("down", len(DOWN) - 1), 0.0)])
    add(("base",), 0.9, [], [(("give",), 4.2)])
    add(("near", 4), 1.7, [("dn", 4), ("dn", 5)], [(("base",), 0.0), (("gu", 8), 2.0), (("gu", 9), 2.0)])
    add(("near", 5), 1.9, [("dn", 5)], [(("near", 4), 0.0), (("gu", 10), 2.0)])
    own_after = {}
    for (name, _), c in CHUNK_OF.items():
        if name in ("gu", "pj", "dn"):
            own_after[c] = number["cast", "gu" if name == "gu" else "rest"]
    return names, comps, own_after


def place():
    rep, fs = lax.axis_index("rep"), lax.axis_index("fs")
    tp = lax.axis_index("tp")
    x, y, zl = lax.rem(fs, 4), lax.rem(fs // 4, 4), fs // 16
    z = rep * 2 + zl
    xs = {n: lax.rem(x + 4 + n, 4) for n in (-1, 1, 2)} | {0: x}
    ys = {n: lax.rem(y + 4 + n, 4) for n in (-1, 1, 2)} | {0: y}
    near = {}
    for sign in (1, -1):
        near["x", sign] = (rep, zl * 16 + y * 4 + xs[sign], tp)
        near["y", sign] = (rep, zl * 16 + ys[sign] * 4 + x, tp)
        zn = lax.rem(z + 4 + sign, 4)
        near["z", sign] = (zn // 2, lax.rem(zn, 2) * 16 + y * 4 + x, tp)
    return xs, ys, {0: zl, 1: 1 - zl}, near, (rep, fs, 1 - tp), tp


def carried(kind, m, turn, arriving):
    sent = {
        "A": (
            (0, 0, 0),
            (0, 0, 0),
            (0, 0, -turn),
            (0, 0, None),
            (0, 0, None),
            (0, 0, None),
            (0, -turn, None),
            (0, -turn, None),
            (0, turn, None),
            (0, 2, None),
        ),
        "D": (
            (0, 0, 0),
            (None, 0, 0),
            (None, 0, 0),
            (None, -turn, 0),
            (None, None, 0),
            (None, None, 0),
            ("plane0", None, -1),
            ("plane1", None, 1),
        ),
        "E": (
            (0, 0, 0),
            (0, 0, 0),
            (0, 0, -turn),
            (0, 0, None),
            (0, 0, None),
            (0, 0, 0),
            (0, 0, -1),
            (0, 0, 1),
            (0, 0, 2),
            (0, -turn, None),
            (0, -turn, None),
            (0, turn, None),
            (0, 2, None),
        ),
        "C": (
            (0, 0, 0),
            (None, 0, 0),
            (None, 0, 0),
            (None, 0, -turn),
            (None, 0, None),
            (None, 0, None),
            ("plane0", -1, None),
            ("plane1", 1, None),
        ),
    }[kind][m]
    if not arriving:
        return sent
    link, sign = link_of(kind, m, turn)
    z, y, x = sent

    def back(v, n):
        v = v - n
        return v + 4 if v < -1 else v - 4 if v > 2 else v

    if link == "x":
        x = back(x, sign)
    elif link == "y":
        y = back(y, sign)
    else:
        z = 1 - z
    return z, y, x


def mega_kernel(
    ops, names, tokens, in_w, val_w, out_w, gate_w, up_w, pj_w, dn_w, *rest,
):
    small_in, out, small = rest[:15], rest[15], rest[16:31]
    run_kernel(ops, names, tokens, in_w, val_w, out_w, gate_w, up_w, pj_w, dn_w, small_in, small, out, *rest[31:])


def run_kernel(
    ops, names, tokens, in_w, val_w, out_w, gate_w, up_w, pj_w, dn_w, small_in, small, out, mix, pj, gu, dn, sc, tok, rows, gates, conv, square, acc, hidden, psend, precv, sqrecv, sv_mix,
    sv_gu, sv_pj, sv_dn, hidden_other, dn_other, own_sem, send_sem, recv_sem, side_send, side_recv,
):
    f32, bf16 = jnp.float32, jnp.bfloat16
    (in_s, val_s, out_s, gate_s, up_s, pj_s, dn_s, mix_gain, ffn_gain, mix_taps, conv_gain, gate_taps, up_taps, gate_bias,
     up_bias) = small
    xs, ys, zs, near, other, tp = place()
    bufs = {"mix": mix, "pj": pj, "gu": gu, "dn": dn, "sc": sc}
    x, y, zl = xs[0], ys[0], zs[0]
    mine = pl.multiple_of(tp * 512, 512)
    yours = pl.multiple_of((1 - tp) * 512, 512)
    mix_f32 = [acc.at[64 * i : 64 * i + 64, 0:512] for i in range(3)]
    gu_f32 = [acc.at[192 + 64 * i : 256 + 64 * i, 0:1408] for i in range(2)]
    pj_f32, dn_f32 = acc.at[320:384, 0:512], acc.at[384:448, 0:1408]
    own = [
        pltpu.make_async_copy(src, dst, own_sem.at[i])
        for i, (src, dst) in enumerate(
            zip(
                (in_w, val_w, out_w, gate_w, up_w, pj_w, dn_w, tokens),
                (*mix_f32, *gu_f32, pj_f32, dn_f32, tok),
            )
        )
    ]
    small_copies = [pltpu.make_async_copy(src, dst, own_sem.at[8 + i]) for i, (src, dst) in enumerate(zip(small_in, small))]
    for copy in own[:3] + small_copies[:7] + own[3:] + small_copies[7:]:
        copy.start()
    barrier = pltpu.get_barrier_semaphore()
    for device in [*near.values(), other]:
        pl.semaphore_signal(barrier, inc=1, device_id=device, device_id_type=MESH)
    sc[zl, y, x] = jnp.zeros((8, 128), f32)
    for copy in small_copies[:7]:
        copy.wait()
    for i, ref in enumerate((in_s, val_s, out_s, gate_s, up_s, pj_s, dn_s)):
        sc[zl, y, x, i : i + 1, : ref.shape[0]] = ref[...].reshape(1, -1)
    for i in range(3):
        own[i].wait()
        for g in range(2):
            mix[3 * g + i, zl, y, x] = mix_f32[i][:, 256 * g : 256 * g + 256].astype(bf16)
    pl.semaphore_wait(barrier, 7)

    def block_cast(which):
        if which == "gu":
            for i in range(2):
                own[3 + i].wait()
                for k in range(11):
                    gu[k, zl, y, x, :, 128 * i : 128 * i + 128] = gu_f32[i][:, 128 * k : 128 * k + 128].astype(bf16)
        else:
            own[5].wait()
            pj[zl, y, x] = pj_f32[...].astype(bf16)
            own[6].wait()
            dn[zl, y, x] = dn_f32[...].astype(bf16)
            for unit in passed:
                pass_on(unit, (0, 0, 0))

    def part(c, at):
        name, i, width = WHERE[c]
        z, y, x = at
        z = slice(None) if z is None else int(z[-1]) if isinstance(z, str) else zs[z]
        y = slice(None) if y is None else ys[y]
        x = slice(None) if x is None else xs[x]
        ref = bufs[name]
        if name in ("mix", "gu"):
            return ref.at[i, z, y, x]
        if name == "sc":
            return ref.at[z, y, x]
        return ref.at[z, y, x, :, i * UNIT : i * UNIT + width]

    def all_of(c, m):
        kind, turn, _ = CHUNKS[c]
        ends, region = ENDS[kind]
        return region if m in ends else carried(kind, m, turn, True)

    def copy_of(c, m, arriving):
        kind, turn, _ = CHUNKS[c]
        ref = part(c, all_of(c, m) if arriving else carried(kind, m, turn, False))
        return pltpu.make_async_remote_copy(
            src_ref=ref,
            dst_ref=ref,
            send_sem=send_sem.at[c],
            recv_sem=recv_sem.at[c, slot_of(kind, m)],
            device_id=near[link_of(kind, m, turn)],
            device_id_type=MESH,
        )

    def to_other(src, dst, i):
        return pltpu.make_async_remote_copy(
            src_ref=src, dst_ref=dst, send_sem=side_send.at[i], recv_sem=side_recv.at[i], device_id=other, device_id_type=MESH
        )

    def normed(values, gain):
        return (values * lax.rsqrt(jnp.mean(values * values, axis=1, keepdims=True) + epsilon) * gain[...].reshape(1, -1)).astype(bf16)

    def shifted(values, before):
        both = jnp.concatenate([before, values], axis=0)
        return pltpu.roll(both, 1, 0)[8:], pltpu.roll(both, 2, 0)[8:]

    def dot_nt(left, right):
        return lax.dot_general(left, right, (((1,), (1,)), ((), ())), preferred_element_type=f32)

    def spread(row, width, group):
        total = jnp.zeros((1, 128), f32)
        lane = lax.broadcasted_iota(jnp.int32, (1, 128), 1)
        for s in range(group * 128 // width, min(31, (group * 128 + 127) // width) + 1):
            at = s * width - group * 128
            line = sc[s // 16, s // 4 % 4, s % 4, row : row + 1, :]
            if at % 128:
                line = pltpu.roll(line, at % 128, 1)
            total = jnp.where((lane >= at) & (lane < at + width), line, total)
        return total

    def rows_copy(to_send, first, count, i):
        at = pl.ds((mine if to_send else yours) + first, count)
        return to_other(rows.at[at], rows.at[at], i)

    send_rows, recv_rows = (rows_copy(b, 0, 512, 0) for b in (True, False))
    send_again, recv_again = ([rows_copy(b, 128 * q, 128, 9 + q) for q in range(4)] for b in (True, False))
    send_parts = [to_other(psend.at[pl.ds(256 * q, 256)], precv.at[pl.ds(256 * q, 256)], (1, 3)[q]) for q in range(2)]
    send_sums = to_other(psend, precv, 4)
    send_square = to_other(square.at[pl.ds(yours, 512)], sqrecv, 2)
    def lanes_of(unit):
        return slice(UNIT * unit, min(UNIT * unit + UNIT, 1408)), slice(UNIT * (unit - PASSED), min(UNIT * unit + UNIT, 1408) - UNIT * PASSED)

    send_hidden = {}
    for unit in (4, 5):
        here, there = lanes_of(unit)
        send_hidden[unit] = to_other(hidden.at[pl.ds(yours, 512), here], hidden_other.at[:, there], 1 + unit)
    passed = {}
    for unit in (4, 5):
        here, there = lanes_of(unit)
        passed[unit] = to_other(dn.at[:, :, :, :, here], dn_other.at[:, :, :, :, there], 3 + unit)
    seen = set()

    def pass_on(unit, at):
        z, y, x = at
        z = slice(None) if z is None else int(z[-1]) if isinstance(z, str) else zs[z]
        y = slice(None) if y is None else ys[y]
        x = slice(None) if x is None else xs[x]
        ref = dn_other.at[z, y, x, :, lanes_of(unit)[1]]
        to_other(part(CHUNK_OF["dn", unit], at), ref, 3 + unit).start()

    def block_norm():
        own[7].wait()
        for copy in small_copies[7:]:
            copy.wait()

        @pl.loop(0, 512, step=64)
        def _(r):
            at = pl.multiple_of(r, 64)
            rows[pl.ds(mine + at, 64), :] = normed(tok[pl.ds(at, 64), :].astype(f32), mix_gain)

        send_rows.start()

    def block_scales():
        for k in range(6):
            for i in range(2):
                sv_mix[k, :, 128 * i : 128 * i + 128] = spread(k % 3, 16, k // 3 * 2 + i)
        for k in range(11):
            sv_gu[k, :, :128] = spread(3, 44, k)
            sv_gu[k, :, 128:] = spread(4, 44, k)
        for k in range(16):
            sv_pj[k // 2, :, 128 * (k % 2) : 128 * (k % 2) + 128] = spread(5, 64, k)
            sv_dn[k // 2, :, 128 * (k % 2) : 128 * (k % 2) + 128] = spread(6, 64, k)

    def block_mix(k):
        if "rows" not in seen:
            seen.add("rows")
            recv_rows.wait_recv()

        for r in range(0, 1024, ROWS):
            at = pl.ds(r, ROWS)
            weight = mix[k].reshape(2048, 256)
            gates[k, at, :] = (jnp.dot(rows[at, :], weight, preferred_element_type=f32) * sv_mix[k]).astype(bf16)

    def block_conv(g):
        cols = slice(256 * g, 256 * g + 256)
        taps, gain = mix_taps[:, cols], conv_gain[cols].reshape(1, 256)

        def body(i, before):
            at = pl.ds(pl.multiple_of(i * 128, 128), 128)
            value = gates[3 * g, at, :].astype(f32) * gates[3 * g + 1, at, :].astype(f32)
            one, two = shifted(value, before)
            total = taps[0:1] * two + taps[1:2] * one + taps[2:3] * value
            done = (gates[3 * g + 2, at, :].astype(f32) * total).astype(bf16).astype(f32)
            conv[at, cols] = (done * gain).astype(bf16)
            squares = jnp.broadcast_to(jnp.sum(done * done, axis=1, keepdims=True), (128, 128))
            square[at, :] = squares if g == 0 else square[at, :] + squares
            return value[-8:]

        lax.fori_loop(0, 8, body, jnp.zeros((8, 256), f32))
        if g == 1:
            send_square.start()

    def block_proj(half):
        for q in range(2):
            here = pl.ds(256 * q, 256)
            rows_at = pl.ds((yours if half == 0 else mine) + 256 * q, 256)
            for n in range(8):
                weight = pj[n // 4, n % 4].reshape(256, 512)
                part_sum = dot_nt(conv[rows_at, :], weight) * sv_pj[n]
                cols = slice(n * 256, n * 256 + 256)
                if half == 0:
                    psend[here, cols] = part_sum.astype(bf16)
                else:
                    acc[rows_at, cols] = part_sum
            if half == 0:
                send_parts[q].start()

    def block_first():
        send_square.wait_recv()
        send_rows.wait_send()
        for q in range(4):
            if q % 2 == 0:
                send_parts[q // 2].wait_recv()

            @pl.loop(128 * q, 128 * q + 128, step=64)
            def _(r):
                at = pl.ds(pl.multiple_of(r, 64), 64)
                there = pl.ds(pl.multiple_of(mine + r, 64), 64)
                squares = square[there, :1] + sqrecv[at, :1]
                summed = (acc[there, :] + precv[at, :].astype(f32)) * lax.rsqrt(squares / 1024 + epsilon)
                first = (tok[at, :].astype(f32) + summed).astype(bf16)
                tok[at, :] = first
                rows[there, :] = normed(first.astype(f32), ffn_gain)

            send_again[q].start()

    def block_gu(k):
        if "rows2" not in seen:
            seen.add("rows2")
            for copy in recv_again:
                copy.wait_recv()
        cols = slice(128 * k, 128 * k + 128)

        def body(i, before):
            at = pl.ds(i * ROWS, ROWS)
            weight = gu[k].reshape(2048, 256)
            pre = (jnp.dot(rows[at, :], weight, preferred_element_type=f32) * sv_gu[k]).astype(bf16).astype(f32)
            one, two = shifted(pre, before)
            acts = []
            for j, (taps, bias) in enumerate(((gate_taps, gate_bias), (up_taps, up_bias))):
                half, t = slice(128 * j, 128 * j + 128), taps[:, cols]
                acts.append(t[0:1] * two[:, half] + t[1:2] * one[:, half] + t[2:3] * pre[:, half] + bias[cols].reshape(1, 128))
            half = 0.5 * acts[0]
            hidden[at, cols] = ((half + half * jnp.tanh(half)) * acts[1]).astype(bf16)
            return pre[-8:]

        before = jnp.zeros((8, 256), f32)
        for i in range(1024 // ROWS):
            before = body(i, before)
        seen.add(k)
        if k == 10:
            send_hidden[5].start()
        elif k in (8, 9) and {8, 9} <= seen:
            send_hidden[4].start()

    def block_down(j):
        first, count = DOWN[j]
        width = sum(WHERE[CHUNK_OF["dn", u]][2] for u in range(first, first + count))
        lanes = slice(UNIT * first, UNIT * first + width)

        def product(start, count, n):
            weight = dn[n // 4, n % 4, :, :, lanes].reshape(256, width)
            return dot_nt(hidden[pl.ds(start, count), lanes], weight)

        def sweep(start, count, store):
            for n in range(8):
                store(n, slice(n * 256, n * 256 + 256), pl.ds(start, count), product(start, count, n))

        def store(n, cols, at, value):
            acc[at, cols] = value if j == 0 else acc[at, cols] + value

        sweep(0, 1024, store)


    def block_give():
        for copy in send_parts:
            copy.wait_send()

        @pl.loop(0, 512, step=64)
        def _(r):
            at, there = pl.ds(pl.multiple_of(r, 64), 64), pl.ds(pl.multiple_of(yours + r, 64), 64)
            for n in range(8):
                cols = slice(256 * n, 256 * n + 256)
                psend[at, cols] = (acc[there, cols] * sv_dn[n]).astype(bf16)

        send_sums.start()

    def block_base():
        send_sums.wait_recv()

        @pl.loop(0, 512, step=64)
        def _(r):
            at, there = pl.ds(pl.multiple_of(r, 64), 64), pl.ds(pl.multiple_of(mine + r, 64), 64)
            for n in range(8):
                cols = slice(256 * n, 256 * n + 256)
                summed = acc[there, cols] * sv_dn[n] + precv[at, cols].astype(f32)
                acc[there, cols] = tok[at, cols].astype(f32) + summed

    def block_near(unit):
        here, there = lanes_of(unit)
        width = here.stop - here.start
        at = pl.ds(mine, 512)

        def weight(ref, n, lanes):
            return ref[n // 4, n % 4, :, :, lanes].reshape(256, width)

        if unit == 4:
            for n in range(8):
                cols = slice(256 * n, 256 * n + 256)
                acc[at, cols] = acc[at, cols] + dot_nt(hidden[at, here], weight(dn, n, here)) * sv_dn[n]
        send_hidden[unit].wait_recv()
        passed[unit].wait_recv()
        for n in range(8):
            cols = slice(256 * n, 256 * n + 256)
            if unit == 4:
                acc[at, cols] = acc[at, cols] + dot_nt(hidden_other[:, there], weight(dn_other, n, there)) * sv_dn[n]
            else:
                left = jnp.concatenate([hidden[at, here], hidden_other[:, there]], axis=1)
                right = jnp.concatenate([weight(dn, n, here), weight(dn_other, n, there)], axis=1)
                out[:, cols] = (acc[at, cols] + dot_nt(left, right) * sv_dn[n]).astype(bf16)

    blocks = {
        "cast": block_cast,
        "norm": block_norm, "scales": block_scales, "mix": block_mix, "conv": block_conv, "proj": block_proj,
        "first": block_first, "gu": block_gu, "down": block_down, "give": block_give, "base": block_base,
        "near": block_near,
    }
    gone, met = set(), set()

    def sent_by(end):
        for c, (kind, _, _) in enumerate(CHUNKS):
            entries = range(len(TREES[kind]))
            if c not in gone and all(("send", c, m) in ops[:end] for m in entries):
                gone.add(c)
                for m in entries:
                    copy_of(c, m, False).wait_send()

    for step, op in enumerate(ops):
        if op[0] == "send":
            copy_of(op[1], op[2], False).start()
        elif op[0] == "wait":
            c, m = op[1:]
            if (c, slot_of(CHUNKS[c][0], m)) in met:
                continue
            met.add((c, slot_of(CHUNKS[c][0], m)))
            copy_of(c, m, True).wait_recv()
            name, unit, _ = WHERE[c]
            if name == "dn" and unit in passed:
                pass_on(unit, all_of(c, m))
        else:
            name, *index = names[op[1]]
            if name == "base":
                sent_by(step - 30)
            blocks[name](*index)
    sent_by(len(ops))
    send_square.wait_send()
    send_sums.wait_send()
    for copy in send_again:
        copy.wait_send()
    for unit in passed:
        send_hidden[unit].wait_send()
        passed[unit].wait_send()


def mega(*args):
    names, comps, own_after = list_of_blocks()
    ops, _, _, _ = plan(CHUNKS, comps, own_after)
    f32, bf16 = jnp.float32, jnp.bfloat16
    hbm, vmem = pl.BlockSpec(memory_space=pl.ANY), pl.BlockSpec(memory_space=pltpu.VMEM)
    dma = pltpu.SemaphoreType.DMA
    return pl.pallas_call(
        lambda *refs: mega_kernel(ops, names, *refs),
        out_shape=pltpu.VMEM((512, 2048), bf16),
        in_specs=[hbm] * 23,
        out_specs=vmem,
        scratch_shapes=[pltpu.VMEM(a.shape, f32) for a in args[8:]] + [
            pltpu.VMEM((6, 2, 4, 4, 64, 256), bf16),
            pltpu.VMEM((2, 4, 4, 64, 512), bf16),
            pltpu.VMEM((11, 2, 4, 4, 64, 256), bf16),
            pltpu.VMEM((2, 4, 4, 64, 1408), bf16),
            pltpu.VMEM((2, 4, 4, 8, 128), f32),
            pltpu.VMEM((512, 2048), bf16),
            pltpu.VMEM((1024, 2048), bf16),
            pltpu.VMEM((6, 1024, 256), bf16),
            pltpu.VMEM((1024, 512), bf16),
            pltpu.VMEM((1024, 128), f32),
            pltpu.VMEM((1024, 2048), f32),
            pltpu.VMEM((1024, 1408), bf16),
            pltpu.VMEM((512, 2048), bf16),
            pltpu.VMEM((512, 2048), bf16),
            pltpu.VMEM((512, 128), f32),
            pltpu.VMEM((6, 1, 256), f32),
            pltpu.VMEM((11, 1, 256), f32),
            pltpu.VMEM((8, 1, 256), f32),
            pltpu.VMEM((8, 1, 256), f32),
            pltpu.VMEM((512, 384), bf16),
            pltpu.VMEM((2, 4, 4, 64, 384), bf16),
            dma((23,)),
            dma((len(CHUNKS),)),
            dma((len(CHUNKS), 7)),
            dma((13,)),
            dma((13,)),
        ],
        compiler_params=pltpu.CompilerParams(collective_id=0, has_side_effects=True, vmem_limit_bytes=58 * 1024 * 1024),
    )(*args)


def to_hbm(values):
    def kernel(src, dst, sem):
        copies = [
            pltpu.make_async_copy(src.at[128 * q : 128 * q + 128], dst.at[128 * q : 128 * q + 128], sem.at[q])
            for q in range(4)
        ]
        for copy in copies:
            copy.start()
        for copy in copies:
            copy.wait()

    return pl.pallas_call(
        kernel,
        out_shape=jax.ShapeDtypeStruct(values.shape, values.dtype),
        in_specs=[pl.BlockSpec(memory_space=pltpu.VMEM)],
        out_specs=pl.BlockSpec(memory_space=pl.ANY),
        scratch_shapes=[pltpu.SemaphoreType.DMA((4,))],
        compiler_params=pltpu.CompilerParams(vmem_limit_bytes=4 * 1024 * 1024),
    )(values)


def local(
    tokens, mix_gain, out_gate_w, in_gate_w, value_w, out_gate_scale, in_gate_scale, value_scale, mix_taps, conv_gain,
    out_proj_w, proj_scale, ffn_gain, gate_w, up_w, gate_scale, up_scale, gate_taps, up_taps, gate_bias, up_bias, down_w,
    down_scale,
):
    return to_hbm(mega(
        tokens[0], in_gate_w, value_w, out_gate_w, gate_w, up_w, out_proj_w.T, down_w.T, in_gate_scale, value_scale,
        out_gate_scale, gate_scale, up_scale, proj_scale, down_scale, mix_gain, ffn_gain, mix_taps, conv_gain, gate_taps,
        up_taps, gate_bias, up_bias,
    ))[None]


def solution(mesh):
    placed = (
        P(("rep", "fs"), "tp", None), P(), P("fs", "tp"), P("fs", "tp"), P("fs", "tp"), P(("tp", "fs")), P(("tp", "fs")),
        P(("tp", "fs")), P(None, "tp"), P("tp"), P("tp", "fs"), P("fs"), P(), P("fs", "tp"), P("fs", "tp"), P(("tp", "fs")),
        P(("tp", "fs")), P(None, "tp"), P(None, "tp"), P("tp"), P("tp"), P("tp", "fs"), P("fs"),
    )
    return jax.shard_map(
        local, mesh=mesh, in_specs=placed, out_specs=P(("rep", "fs"), "tp", None), check_vma=False
    )
```
